256 devices in a mesh: grp: 2 (over y), sp: 32 (over z, core), tp: 4 (over x).
Axes of the slice: x: 4, y: 2, z: 16, core: 2. Of those that a mesh axis runs over, the one named last changes fastest.
The devices are a block of a 4x16x16 slice.
Arguments:
- carryover_vector: bfloat16 [16384, 2048], P(('grp', 'sp', 'tp')), parts along dimension 0, may hold values from -6 to 6
- channel_source_entries: bfloat16 [16384, 1024], P(('grp', 'sp'), 'tp'), parts along dimension 0, may hold values from -6 to 6
- final_modulation_vector: bfloat16 [16384, 1024], P(('grp', 'sp'), 'tp'), parts along dimension 0, may hold values from -54 to 54
- entering_basis_matrix: bfloat16 [16384, 512], P(('grp', 'sp'), 'tp'), parts along dimension 0, may hold values from -6 to 6
- readout_basis_matrix: bfloat16 [16384, 512], P(('grp', 'sp'), 'tp'), parts along dimension 0, may hold values from -6 to 6
- raw_stride_amount: float32 [16384, 16], P(('grp', 'sp'), 'tp'), parts along dimension 0, may hold values from -6 to 5
- extra_log_attenuation: float32 [16384, 16], P(('grp', 'sp'), 'tp'), parts along dimension 0, may hold values from -1.4 to 0
- channel_fading_rate: float32 [16], P('tp'), may hold values from 0 to 0.1, as said below
- channel_source_kernel: float32 [4, 1024], P(None, 'tp'), may hold values from -3 to 3
- entering_basis_kernel: float32 [4, 512], P(None, 'tp'), may hold values from -3 to 3
- readout_basis_kernel: float32 [4, 512], P(None, 'tp'), may hold values from -3 to 3
- modulated_rescaling_vector: float32 [1024], replicated, may hold values from 0.1 to 1.9
- blender_final_matrix: bfloat16 [1024, 2048], replicated, may hold values from -0.1875 to 0.1875
- specialist_rescaling_vector: float32 [2048], replicated, may hold values from 0.1 to 1.9
- specialist_gating_matrices: bfloat16 [64, 2048, 1024], P('sp', None, 'tp'), may hold values from -0.125 to 0.125
- widening_matrices: bfloat16 [64, 2048, 1024], P('sp', None, 'tp'), may hold values from -0.125 to 0.125
- contracting_matrices: bfloat16 [64, 1024, 2048], P('sp', 'tp'), may hold values from -0.1875 to 0.1875
- assigned_specialist_ids: int32 [16384, 2], P(('grp', 'sp')), parts along dimension 0, may hold values from 0 to 63, as said below
- specialist_choice_affinity: float32 [16384, 2], P(('grp', 'sp', 'tp')), parts along dimension 0, may hold values from -6 to 6
- cluster_chance: float32 [16384], P(('grp', 'sp', 'tp')), parts along dimension 0, may hold values from 0.25 to 1
Outputs:
- layer_out: bfloat16 [16384, 2048], P(('grp', 'sp', 'tp')), parts along dimension 0
The draws below stay inside these ranges and needn't reach their ends.
There are 2 independent parts, one for each index of `grp`. The reference program is written for one: setup_inputs(seed, part) draws one part's arguments, and reference() takes and returns one part's arrays. A program takes and returns all parts, laid end to end along the dimension named above; an argument that names none is the same for every part. Nothing has to cross between parts.
Inputs may be any that keep to these rules, and one draw needn't show every extreme that they name: `assigned_specialist_ids`: each row names 2 different experts of one group: the experts g * 16 to (g + 1) * 16 - 1 for one g below 4. In each aligned block of 64 rows (the rows of one device) no expert is named by more than 4 rows, and every expert of one group, the same group in all blocks, is named by exactly 4 rows of every block. `channel_fading_rate`: positive.
All inputs are finite; a program needn't handle non-finite values.
Results may differ from the reference program's by a relative error of at most 0.015.
Values may be sent and summed in bfloat16 or wider, within the bound.
A program may use at most 64 MiB of HBM per device.

```python
import jax
import jax.numpy as jnp
from jax import lax

D = 2048
HEADS = 16
HEAD_DIM = 64
GROUPS_BC = 4
STATE = 128
CONV = 4
BLOCK = 64
FF = 1024
EGROUPS = 4
TOPK = 2
SEG_TOK = 256
D_SSD = 1024
ROWS = 64
TOKENS = 8192
EXPERTS = 64
CAP = 4
N_TP = 4


def draw_final_modulation_vector(key, part):
    row_key, column_key, base_key = jax.random.split(jax.random.fold_in(key, 7), 3)
    row_scale = jnp.exp(jax.random.uniform(row_key, (TOKENS, 1), jnp.float32, jnp.log(0.3), jnp.log(3.0)))
    column = jnp.arange(D_SSD, dtype=jnp.float32)[None, :] / D_SSD
    jitter = jnp.exp(jax.random.uniform(column_key, (1, D_SSD), jnp.float32, jnp.log(0.6), jnp.log(1.5)))
    base = jnp.clip(jax.random.normal(base_key, (TOKENS, D_SSD), jnp.float32), -4.0, 4.0)
    column_scale = jnp.exp(column * jnp.log(3.0)) * jitter
    return (base * row_scale * column_scale).astype(jnp.bfloat16)


def draw_raw_stride_amount(key, part):
    jitter_key, level_key = jax.random.split(jax.random.fold_in(key, 11))
    segments = TOKENS // SEG_TOK
    levels = jax.random.uniform(level_key, (segments, 1, 1), jnp.float32, -1.5, 1.0)
    jitter = jnp.clip(jax.random.normal(jitter_key, (segments, SEG_TOK, HEADS), jnp.float32), -4.5, 4.0)
    return (jitter + levels).reshape(TOKENS, HEADS)


def draw_channel_fading_rate(key, part):
    pick_key, slow_key, fast_key = jax.random.split(jax.random.fold_in(key, 13), 3)
    slow_share = 0.5
    is_slow = jax.random.uniform(pick_key, (HEADS,), jnp.float32) < slow_share
    slow_rates = jnp.exp(jax.random.uniform(slow_key, (HEADS,), jnp.float32, jnp.log(0.1 / TOKENS), jnp.log(1.0 / TOKENS)))
    fast_rates = jnp.exp(jax.random.uniform(fast_key, (HEADS,), jnp.float32, jnp.log(0.03), jnp.log(0.1)))
    return jnp.where(is_slow, slow_rates, fast_rates)


def draw_extra_log_attenuation(key, part):
    place_key, strength_key = jax.random.split(jax.random.fold_in(key, 17))
    places = jax.random.randint(place_key, (2, 1, HEADS), 0, TOKENS)
    strengths = jax.random.uniform(strength_key, (2, 1, HEADS), jnp.float32, 0.22, 0.69)
    positions = jnp.arange(TOKENS, dtype=jnp.int32)[None, :, None]
    return -jnp.sum(jnp.where(positions == places, strengths, 0.0), axis=0)


def draw_assigned_specialist_ids(key, part):
    blocks = TOKENS // ROWS
    per_group = EXPERTS // EGROUPS
    busy_rows = CAP * per_group // TOPK
    busy_key, other_key, order_key, deal_key = jax.random.split(jax.random.fold_in(key, 19), 4)
    busy_group = jax.random.randint(busy_key, (), 0, EGROUPS)
    others = jax.random.randint(other_key, (blocks, ROWS - busy_rows), 0, EGROUPS - 1)
    others = others + (others >= busy_group).astype(jnp.int32)
    groups = jnp.concatenate([jnp.full((blocks, busy_rows), busy_group, jnp.int32), others], axis=1)
    orders = jax.vmap(lambda subkey: jax.random.permutation(subkey, ROWS))(jax.random.split(order_key, blocks))
    groups = jnp.take_along_axis(groups, orders, axis=1)
    member = (groups[..., None] == jnp.arange(EGROUPS, dtype=jnp.int32)).astype(jnp.int32)
    ranking = jnp.sum((jnp.cumsum(member, axis=1) - member) * member, axis=2)
    dealing = jax.vmap(lambda subkey: jax.random.permutation(subkey, per_group))(jax.random.split(deal_key, blocks * EGROUPS)).reshape(blocks, EGROUPS, per_group)
    chosen = dealing[jnp.arange(blocks)[:, None], groups]
    first_place = TOPK * ranking % per_group
    first_pick = jnp.take_along_axis(chosen, first_place[..., None], axis=2)[..., 0]
    second_pick = jnp.take_along_axis(chosen, (first_place + 1)[..., None], axis=2)[..., 0]
    group_base = groups * per_group
    picked = jnp.stack([group_base + first_pick, group_base + second_pick], axis=-1)
    return picked.reshape(TOKENS, TOPK).astype(jnp.int32)


def block_levels(own_key, extent, cuts, low, top_value):
    def one(position, parts):
        steps = jax.random.uniform(jax.random.fold_in(jax.random.fold_in(own_key, 6), position), (parts,), jnp.float32, low / len(cuts), top_value / len(cuts))
        return jnp.repeat(jnp.exp(steps), extent[position] // parts).reshape((-1,) + (1,) * (len(extent) - position - 1))

    level = one(*cuts[0])
    for cut in cuts[1:]:
        level = level * one(*cut)
    return level


def centred(own_key, shape, width, limit, shards=(), kind=jnp.bfloat16):
    values = jax.random.normal(own_key, shape, jnp.float32) * width
    if len(shards) > 0:
        values = block_levels(own_key, shape, shards, -0.22, 0.18) * values
    return jnp.clip(values, min=-limit, max=limit).astype(kind)


def setup_inputs(seed: int = 0, part: int = 0) -> dict:
    streams_of = jax.random.split(jax.random.key(seed), 21)
    own_keys = jax.random.split(jax.random.fold_in(streams_of[20], part), 21)
    carryover_vector = centred(own_keys[0], (TOKENS, D), 1.0, 6.0, ((0, 128),))
    channel_source_entries = centred(own_keys[1], (TOKENS, D_SSD), 1.0, 6.0, ((0, 32), (1, 4)))
    final_modulation_vector = draw_final_modulation_vector(jax.random.fold_in(jax.random.fold_in(streams_of[20], part), 71), part)
    entering_basis_matrix = centred(own_keys[3], (TOKENS, GROUPS_BC * STATE), 1.0, 6.0, ((0, 32), (1, 4)))
    readout_basis_matrix = centred(own_keys[4], (TOKENS, GROUPS_BC * STATE), 1.0, 6.0, ((0, 32), (1, 4)))
    raw_stride_amount = draw_raw_stride_amount(jax.random.fold_in(jax.random.fold_in(streams_of[20], part), 71), part)
    extra_log_attenuation = draw_extra_log_attenuation(jax.random.fold_in(jax.random.fold_in(streams_of[20], part), 71), part)
    channel_fading_rate = draw_channel_fading_rate(jax.random.fold_in(streams_of[20], 71), part)
    channel_source_kernel = centred(streams_of[8], (CONV, D_SSD), CONV ** -0.5, 3.0, ((1, 4),), jnp.float32)
    entering_basis_kernel = centred(streams_of[9], (CONV, GROUPS_BC * STATE), CONV ** -0.5, 3.0, ((1, 4),), jnp.float32)
    readout_basis_kernel = centred(streams_of[10], (CONV, GROUPS_BC * STATE), CONV ** -0.5, 3.0, ((1, 4),), jnp.float32)
    modulated_rescaling_vector = jnp.clip(1.0 + 0.18 * jax.random.normal(streams_of[11], (D_SSD,), jnp.float32), 0.1, 1.9)
    blender_final_matrix = centred(streams_of[12], (D_SSD, D), D_SSD ** -0.5, 0.1875)
    specialist_rescaling_vector = jnp.clip(1.0 + 0.18 * jax.random.normal(streams_of[13], (D,), jnp.float32), 0.1, 1.9)
    specialist_gating_matrices = centred(streams_of[14], (EXPERTS, D, FF), D ** -0.5, 0.125, ((0, 32), (2, 4)))
    widening_matrices = centred(streams_of[15], (EXPERTS, D, FF), D ** -0.5, 0.125, ((0, 32), (2, 4)))
    contracting_matrices = centred(streams_of[16], (EXPERTS, FF, D), FF ** -0.5, 0.1875, ((0, 32), (1, 4)))
    assigned_specialist_ids = draw_assigned_specialist_ids(jax.random.fold_in(jax.random.fold_in(streams_of[20], part), 71), part)
    specialist_choice_affinity = centred(own_keys[18], (TOKENS, TOPK), 1.5, 6.0, ((0, 128),), jnp.float32)
    cluster_chance = jnp.clip(0.25 + 0.75 * jax.random.uniform(own_keys[19], (TOKENS,), jnp.float32) ** block_levels(own_keys[19], (TOKENS,), ((0, 128),), -0.2, 0.2), 0.25, 1.0)
    return dict(carryover_vector=carryover_vector, channel_source_entries=channel_source_entries, final_modulation_vector=final_modulation_vector, entering_basis_matrix=entering_basis_matrix, readout_basis_matrix=readout_basis_matrix, raw_stride_amount=raw_stride_amount, extra_log_attenuation=extra_log_attenuation, channel_fading_rate=channel_fading_rate, channel_source_kernel=channel_source_kernel, entering_basis_kernel=entering_basis_kernel, readout_basis_kernel=readout_basis_kernel, modulated_rescaling_vector=modulated_rescaling_vector, blender_final_matrix=blender_final_matrix, specialist_rescaling_vector=specialist_rescaling_vector, specialist_gating_matrices=specialist_gating_matrices, widening_matrices=widening_matrices, contracting_matrices=contracting_matrices, assigned_specialist_ids=assigned_specialist_ids, specialist_choice_affinity=specialist_choice_affinity, cluster_chance=cluster_chance)


EPS = 1e-06
HIGHEST = lax.Precision.HIGHEST

def causal_conv(signal, weights):
    kernel_len = weights.shape[0]
    length = signal.shape[0]
    padded = jnp.pad(signal.astype(jnp.float32), ((kernel_len - 1, 0), (0, 0)))
    accumulated = jnp.zeros((length, signal.shape[1]), jnp.float32)
    for offset in range(kernel_len):
        accumulated = accumulated + weights[offset][None, :] * padded[offset:offset + length]
    return jax.nn.silu(accumulated)

def state_space(scaled_in, log_attenuation, keys_b, queries_c):
    blocks = scaled_in.shape[0] // BLOCK
    per_group = HEADS // GROUPS_BC
    scaled_in = scaled_in.reshape(blocks, BLOCK, GROUPS_BC, per_group, HEAD_DIM)
    log_attenuation = log_attenuation.reshape(blocks, BLOCK, GROUPS_BC, per_group)
    keys_b = keys_b.reshape(blocks, BLOCK, GROUPS_BC, STATE)
    queries_c = queries_c.reshape(blocks, BLOCK, GROUPS_BC, STATE)
    lower_mask = jnp.tril(jnp.ones((BLOCK, BLOCK), dtype=bool))

    def advance(carried, pieces):
        block_in, block_log, block_b, block_c = pieces
        running = jnp.cumsum(block_log, axis=0)
        between = running[:, None] - running[None, :]
        decays = jnp.exp(jnp.where(lower_mask[:, :, None, None], between, -jnp.inf))
        scores = jnp.einsum('lgn,sgn->lsg', block_c, block_b, precision=HIGHEST)
        inside = jnp.einsum('lsg,lsgr,sgrp->lgrp', scores, decays, block_in, precision=HIGHEST)
        outside = jnp.einsum('lgn,grpn,lgr->lgrp', block_c, carried, jnp.exp(running), precision=HIGHEST)
        remain = jnp.exp(running[-1][None] - running)
        updated = carried * jnp.exp(running[-1])[:, :, None, None] + jnp.einsum('sgn,sgr,sgrp->grpn', block_b, remain, block_in, precision=HIGHEST)
        return (updated, inside + outside)
    initial = jnp.zeros((GROUPS_BC, per_group, HEAD_DIM, STATE), jnp.float32)
    _, outputs = lax.scan(advance, initial, (scaled_in, log_attenuation, keys_b, queries_c))
    return outputs.reshape(blocks * BLOCK, HEADS, HEAD_DIM)

def reference(carryover_vector, channel_source_entries, final_modulation_vector, entering_basis_matrix, readout_basis_matrix, raw_stride_amount, extra_log_attenuation, channel_fading_rate, channel_source_kernel, entering_basis_kernel, readout_basis_kernel, modulated_rescaling_vector, blender_final_matrix, specialist_rescaling_vector, specialist_gating_matrices, widening_matrices, contracting_matrices, assigned_specialist_ids, specialist_choice_affinity, cluster_chance):
    length = carryover_vector.shape[0]
    inputs_x = causal_conv(channel_source_entries, channel_source_kernel)
    keys_b = causal_conv(entering_basis_matrix, entering_basis_kernel)
    queries_c = causal_conv(readout_basis_matrix, readout_basis_kernel)
    channel_stride_amount = jax.nn.softplus(raw_stride_amount)
    log_attenuation = extra_log_attenuation - channel_fading_rate[None, :] * channel_stride_amount
    heads_x = inputs_x.reshape(length, HEADS, HEAD_DIM)
    mixed = state_space(heads_x * channel_stride_amount[:, :, None], log_attenuation, keys_b, queries_c)
    gated = mixed.reshape(length, D_SSD) * jax.nn.silu(final_modulation_vector.astype(jnp.float32))
    normed = (gated * lax.rsqrt(lax.optimization_barrier(jnp.mean(gated * gated, axis=1, keepdims=True)) + EPS) * modulated_rescaling_vector[None, :]).astype(jnp.bfloat16)
    middle = (carryover_vector.astype(jnp.float32) + jnp.dot(normed, blender_final_matrix, preferred_element_type=jnp.float32)).astype(jnp.bfloat16)
    middle_wide = middle.astype(jnp.float32)
    expert_input = (middle_wide * lax.rsqrt(lax.optimization_barrier(jnp.mean(middle_wide * middle_wide, axis=1, keepdims=True)) + EPS) * specialist_rescaling_vector[None, :]).astype(jnp.bfloat16)
    assigned = assigned_specialist_ids.reshape(-1)
    count_all = assigned.shape[0]
    member = (assigned[:, None] == jnp.arange(EXPERTS, dtype=jnp.int32)[None, :]).astype(jnp.int32)
    ranking = lax.optimization_barrier(jnp.sum((jnp.cumsum(member, axis=0) - member) * member, axis=1))
    slot_count = length // ROWS * CAP
    table = jnp.full((EXPERTS, slot_count), -1, jnp.int32).at[assigned, ranking].set(jnp.arange(count_all, dtype=jnp.int32))
    lifted = jnp.exp(specialist_choice_affinity)
    shares = (cluster_chance[:, None] * lifted / lax.optimization_barrier(jnp.sum(lifted, axis=1, keepdims=True))).reshape(-1)
    quarter = FF // N_TP

    def expert_pass(combined, expert_index):
        slot_ids = table[expert_index]
        is_live = slot_ids >= 0
        safe_ids = jnp.maximum(slot_ids, 0)
        token_ids = safe_ids // TOPK
        chosen = jnp.take(expert_input, token_ids, axis=0)
        gate_value = jnp.dot(chosen, specialist_gating_matrices[expert_index], preferred_element_type=jnp.float32)
        up_value = jnp.dot(chosen, widening_matrices[expert_index], preferred_element_type=jnp.float32)
        hidden = (jax.nn.silu(gate_value) * up_value).astype(jnp.bfloat16)
        down_rows = contracting_matrices[expert_index]
        summed = jnp.zeros((slot_count, D), jnp.float32)
        for part_index in range(N_TP):
            piece_sum = jnp.dot(hidden[:, part_index * quarter:(part_index + 1) * quarter], down_rows[part_index * quarter:(part_index + 1) * quarter], preferred_element_type=jnp.float32).astype(jnp.bfloat16)
            summed = summed + lax.optimization_barrier(piece_sum).astype(jnp.float32)
        result = lax.optimization_barrier(summed.astype(jnp.bfloat16)).astype(jnp.float32)
        weight_column = jnp.where(is_live, shares[safe_ids], 0.0)
        return (combined.at[token_ids].add(weight_column[:, None] * result), None)
    combined, _ = lax.scan(expert_pass, jnp.zeros((length, D), jnp.float32), jnp.arange(EXPERTS, dtype=jnp.int32))
    return (middle_wide + combined).astype(jnp.bfloat16)
```

```python
import functools

import jax
import jax.numpy as jnp
from jax import lax
from jax.experimental import pallas as pl
from jax.experimental.pallas import tpu as pltpu
from jax.sharding import Mesh
from jax.sharding import PartitionSpec as P

HEAD_DIM = 64
STATE = 128
BLOCK = 64
SP = ("sp_0", "sp_1")
GRP_SP_TP = ("grp", "sp_0", "sp_1", "tp")
GRP_SP = ("grp", "sp_0", "sp_1")


EPS = 1e-06


def filled_with(x, identity):
    return jax.tree.map(
        lambda part, zero: jnp.zeros_like(part) + jnp.asarray(zero, part.dtype), x, identity
    )


def carried_in(x, axes, combine, identity):
    before = start = filled_with(x, identity)
    subtotal = x
    for axis in reversed(axes):
        size, index = (lax.axis_size(axis), lax.axis_index(axis))
        pieces = jax.tree.map(
            lambda part, kind: lax.all_gather(part.astype(kind), axis),
            subtotal,
            (jnp.bfloat16, jnp.bfloat16),
        )
        inside, subtotal = (start, start)
        for k in range(size):
            passed = k < index
            subtotal = combine(
                subtotal, jax.tree.map(lambda part, own: part[k].astype(own.dtype), pieces, x)
            )
            inside = jax.tree.map(lambda new, old: jnp.where(passed, new, old), subtotal, inside)
        before = combine(inside, before)
    return before


def from_behind(x, axis, by):
    size = lax.axis_size(axis)
    pairs = [(i, i + by) for i in range(size) if 0 <= i + by < size]
    return lax.ppermute(x, axis, pairs)


def for_sending(x):
    return jax.tree.map(lambda a: a.astype(jnp.bfloat16) if a.dtype == jnp.float32 else a, x)


def split_up(x, dim, size):
    shape = x.shape
    blocks = x.reshape(*shape[:dim], size, shape[dim] // size, *shape[dim + 1 :])
    return jnp.moveaxis(blocks, dim, 0)


def summed_on_arrival(x, axis, dim):
    size = lax.axis_size(axis)
    blocks = lax.all_to_all(split_up(x, dim, size), axis, 0, 0, tiled=True)
    return jnp.sum(blocks.astype(jnp.float32), axis=0)


def causal_conv(signal, earlier, weights):
    kernel_len = weights.shape[0]
    length = signal.shape[0]
    joined = jnp.concatenate([earlier, signal], axis=0).astype(jnp.float32)
    accumulated = jnp.zeros((length, signal.shape[1]), jnp.float32)
    for offset in range(kernel_len):
        accumulated = accumulated + weights[offset][None, :] * joined[offset : offset + length]
    return jax.nn.silu(accumulated)


def link_states(earlier, later):
    return (earlier[0] * later[0], earlier[1] * later[0][..., None, None] + later[1])


def device_states(scaled_in, log_attenuation, keys_b, queries_c, groups_here):
    length = scaled_in.shape[0]
    blocks = length // BLOCK
    per_group = scaled_in.shape[1] // groups_here
    scaled_in = scaled_in.reshape(blocks, BLOCK, groups_here, per_group, HEAD_DIM)
    log_attenuation = log_attenuation.reshape(blocks, BLOCK, groups_here, per_group)
    keys_b = keys_b.reshape(blocks, BLOCK, groups_here, STATE)
    queries_c = queries_c.reshape(blocks, BLOCK, groups_here, STATE)
    running = jnp.cumsum(log_attenuation, axis=1)
    lower_mask = jnp.tril(jnp.ones((BLOCK, BLOCK), dtype=bool))
    between = running[:, :, None] - running[:, None, :]
    decays = jnp.exp(jnp.where(lower_mask[None, :, :, None, None], between, -jnp.inf))
    scores = jnp.einsum("blgn,bsgn->blsg", queries_c, keys_b)
    inside = jnp.einsum("blsg,blsgr,bsgrp->blgrp", scores, decays, scaled_in)
    totals = running[:, -1]
    remain = jnp.exp(totals[:, None] - running)
    block_states = jnp.einsum("bsgn,bsgr,bsgrp->bgrpn", keys_b, remain, scaled_in)

    def advance(carried, pieces):
        return (carried * jnp.exp(pieces[1])[..., None, None] + pieces[0], carried)

    initial = jnp.zeros(block_states.shape[1:], jnp.float32)
    own_state, entering = lax.scan(advance, initial, (block_states, totals))
    own_decay = jnp.exp(jnp.sum(totals, axis=0))
    _, incoming = carried_in(
        (own_decay, own_state),
        SP,
        link_states,
        (jnp.ones_like(own_decay), jnp.zeros_like(own_state)),
    )
    preceding = jnp.exp(jnp.cumsum(totals, axis=0) - totals)
    entering = entering + preceding[..., None, None] * incoming[None]
    outside = jnp.einsum("blgn,bgrpn,blgr->blgrp", queries_c, entering, jnp.exp(running))
    return (inside + outside).reshape(length, -1)


def hop(step):
    half = (step + 1) // 2
    return jnp.where(step % 2 == 1, half, -half)


def greet(nz, nx):
    z, x = lax.axis_index("sp_0"), lax.axis_index("tp")
    barrier = pltpu.get_barrier_semaphore()

    def signal(k, carry):
        pl.semaphore_signal(barrier, inc=1, device_id={"sp_0": lax.rem(z + k, nz)})
        return carry

    lax.fori_loop(1, nz, signal, 0)
    pl.semaphore_signal(barrier, inc=1, device_id={"tp": lax.rem(x + 1, nx)})
    pl.semaphore_signal(barrier, inc=1, device_id={"tp": lax.rem(x + nx - 1, nx)})
    pl.semaphore_wait(barrier, nz + 1)


def dispatch_kernel(nz, nx, src, dst, zs, zr, xs, xr, fs, fr, here):
    z, x = lax.axis_index("sp_0"), lax.axis_index("tp")
    xp, xm = lax.rem(x + 1, nx), lax.rem(x + nx - 1, nx)
    x2 = lax.rem(x + 2, nx)
    greet(nz, nx)

    def along_z(i):
        to = lax.rem(z + hop(i) + nz, nz)
        return pltpu.make_async_remote_copy(
            src.at[:, to], dst.at[:, x, z], zs.at[i], zr.at[i], device_id={"sp_0": to}
        )

    def origin(i):
        return lax.rem(z - hop(i) + nz, nz)

    def along_x(i, way):
        chunk = dst.at[:, x, origin(i)]
        to = xp if way == 0 else xm
        return pltpu.make_async_remote_copy(
            chunk, chunk, xs.at[way, i], xr.at[way, i], device_id={"tp": to}
        )

    def further(i):
        way = i % 2
        chunk = dst.at[:, jnp.where(way == 0, xm, xp), origin(i)]
        to = jnp.where(way == 0, xp, xm)
        return pltpu.make_async_remote_copy(
            chunk, chunk, fs.at[i], fr.at[i], device_id={"tp": to}
        )

    def arrived_x(i, way):
        chunk = dst.at[:, jnp.where(way == 0, xm, xp), origin(i)]
        return pltpu.make_async_remote_copy(
            chunk, chunk, xs.at[way, i], xr.at[way, i], device_id={"tp": xp}
        )

    def arrived_far(i):
        chunk = dst.at[:, x2, origin(i)]
        return pltpu.make_async_remote_copy(
            chunk, chunk, fs.at[i], fr.at[i], device_id={"tp": xp}
        )

    def send_z(i, carry):
        along_z(i).start()
        return carry

    lax.fori_loop(1, nz, send_z, 0)
    own = pltpu.make_async_copy(src.at[:, z], dst.at[:, x, z], here)
    own.start()
    own.wait()
    along_x(0, 0).start()
    along_x(0, 1).start()

    def spread(i, carry):
        pltpu.make_async_remote_copy(
            src.at[:, z], dst.at[:, x, origin(i)], zs.at[i], zr.at[i], device_id={"tp": xp}
        ).wait_recv()
        along_x(i, 0).start()
        along_x(i, 1).start()
        arrived_x(i - 1, (i - 1) % 2).wait_recv()
        further(i - 1).start()
        return carry

    lax.fori_loop(1, nz, spread, 0)
    arrived_x(nz - 1, (nz - 1) % 2).wait_recv()
    further(nz - 1).start()

    def finish(i, carry):
        arrived_x(i, (i + 1) % 2).wait_recv()
        arrived_far(i).wait_recv()
        along_x(i, 0).wait_send()
        along_x(i, 1).wait_send()
        further(i).wait_send()
        return carry

    lax.fori_loop(0, nz, finish, 0)

    def sent(i, carry):
        along_z(i).wait_send()
        return carry

    lax.fori_loop(1, nz, sent, 0)


def dispatch(outgoing, nz, nx):
    experts, _, rows, width = outgoing.shape
    return pl.pallas_call(
        functools.partial(dispatch_kernel, nz, nx),
        out_shape=jax.ShapeDtypeStruct((experts, nx, nz, rows, width), outgoing.dtype),
        in_specs=[pl.BlockSpec(memory_space=pltpu.VMEM)],
        out_specs=pl.BlockSpec(memory_space=pltpu.VMEM),
        scratch_shapes=[
            pltpu.SemaphoreType.DMA((nz,)),
            pltpu.SemaphoreType.DMA((nz,)),
            pltpu.SemaphoreType.DMA((2, nz)),
            pltpu.SemaphoreType.DMA((2, nz)),
            pltpu.SemaphoreType.DMA((nz,)),
            pltpu.SemaphoreType.DMA((nz,)),
            pltpu.SemaphoreType.DMA,
        ],
        compiler_params=pltpu.CompilerParams(collective_id=1, has_side_effects=True),
        name="dispatch",
    )(outgoing)


def collect_kernel(nz, nx, part, out, far, near, both, mine, total, fs, fr, ns, nr, bs, br, zs, zr, here):
    z, x = lax.axis_index("sp_0"), lax.axis_index("tp")
    xp, xm = lax.rem(x + 1, nx), lax.rem(x + nx - 1, nx)
    x2 = lax.rem(x + 2, nx)
    greet(nz, nx)

    def step_of(s):
        return nz - 1 - s

    def goal(i):
        return lax.rem(z + hop(i) + nz, nz)

    def ahead(i):
        return jnp.where(i % 2 == 0, xp, xm)

    def behind(i):
        return jnp.where(i % 2 == 0, xm, xp)

    def send_far(i):
        return pltpu.make_async_remote_copy(
            part.at[:, x2, goal(i)], far.at[i], fs.at[i], fr.at[i], device_id={"tp": ahead(i)}
        )

    def send_near(i):
        return pltpu.make_async_remote_copy(
            part.at[:, behind(i), goal(i)], near.at[i], ns.at[i], nr.at[i], device_id={"tp": behind(i)}
        )

    def send_both(i):
        return pltpu.make_async_remote_copy(
            mine.at[i], both.at[i], bs.at[i], br.at[i], device_id={"tp": ahead(i)}
        )

    def send_z(i):
        return pltpu.make_async_remote_copy(
            total.at[i], out.at[:, z], zs.at[i], zr.at[i], device_id={"sp_0": goal(i)}
        )

    def first(i):
        send_far(i).start()
        send_near(i).start()

    def second(i):
        send_far(i).wait_recv()
        mine[i] = (
            part[:, ahead(i), goal(i)].astype(jnp.float32) + far[i].astype(jnp.float32)
        ).astype(mine.dtype)
        send_both(i).start()

    def third(i):
        send_near(i).wait_recv()
        send_both(i).wait_recv()
        total[i] = (
            part[:, x, goal(i)].astype(jnp.float32)
            + near[i].astype(jnp.float32)
            + both[i].astype(jnp.float32)
        ).astype(total.dtype)

    first(step_of(0))
    first(step_of(1))
    second(step_of(0))

    def turn(s, carry):
        first(step_of(s))
        second(step_of(s - 1))
        third(step_of(s - 2))
        send_z(step_of(s - 2)).start()
        return carry

    lax.fori_loop(2, nz, turn, 0)
    second(step_of(nz - 1))
    third(step_of(nz - 2))
    send_z(step_of(nz - 2)).start()
    third(step_of(nz - 1))
    own = pltpu.make_async_copy(total.at[0], out.at[:, z], here)
    own.start()
    own.wait()

    def finish(i, carry):
        send_far(i).wait_send()
        send_near(i).wait_send()
        send_both(i).wait_send()
        return carry

    lax.fori_loop(0, nz, finish, 0)

    def sent(i, carry):
        send_z(i).wait_send()
        pltpu.make_async_remote_copy(
            total.at[i], out.at[:, lax.rem(z - hop(i) + nz, nz)], zs.at[i], zr.at[i], device_id={"tp": xp}
        ).wait_recv()
        return carry

    lax.fori_loop(1, nz, sent, 0)


def collect(part, nz, nx):
    experts, _, _, rows, width = part.shape
    slots = pltpu.VMEM((nz, experts, rows, width), part.dtype)
    return pl.pallas_call(
        functools.partial(collect_kernel, nz, nx),
        out_shape=jax.ShapeDtypeStruct((experts, nz, rows, width), part.dtype),
        in_specs=[pl.BlockSpec(memory_space=pltpu.VMEM)],
        out_specs=pl.BlockSpec(memory_space=pltpu.VMEM),
        scratch_shapes=[slots] * 5
        + [pltpu.SemaphoreType.DMA((nz,))] * 8
        + [pltpu.SemaphoreType.DMA],
        compiler_params=pltpu.CompilerParams(collective_id=2, has_side_effects=True),
        name="collect",
    )(part)


def per_device(
    carryover_vector,
    channel_source_entries,
    final_modulation_vector,
    entering_basis_matrix,
    readout_basis_matrix,
    raw_stride_amount,
    extra_log_attenuation,
    channel_fading_rate,
    channel_source_kernel,
    entering_basis_kernel,
    readout_basis_kernel,
    modulated_rescaling_vector,
    blender_final_matrix,
    specialist_rescaling_vector,
    specialist_gating_matrices,
    widening_matrices,
    contracting_matrices,
    assigned_specialist_ids,
    specialist_choice_affinity,
    cluster_chance,
):
    length = channel_source_entries.shape[0]
    row_count = carryover_vector.shape[0]
    model_width = carryover_vector.shape[1]
    heads_here = channel_fading_rate.shape[0]
    groups_here = entering_basis_matrix.shape[1] // STATE
    tp_index = lax.axis_index("tp")
    rim_rows = channel_source_kernel.shape[0] - 1
    neighbours = from_behind(
        (
            channel_source_entries[length - rim_rows :],
            entering_basis_matrix[length - rim_rows :],
            readout_basis_matrix[length - rim_rows :],
        ),
        SP,
        1,
    )
    inputs_x = causal_conv(channel_source_entries, neighbours[0], channel_source_kernel)
    keys_b = causal_conv(entering_basis_matrix, neighbours[1], entering_basis_kernel)
    queries_c = causal_conv(readout_basis_matrix, neighbours[2], readout_basis_kernel)
    channel_stride_amount = jax.nn.softplus(raw_stride_amount)
    log_attenuation = extra_log_attenuation - channel_fading_rate[None, :] * channel_stride_amount
    heads_x = inputs_x.reshape(length, heads_here, HEAD_DIM)
    mixed = device_states(
        heads_x * channel_stride_amount[:, :, None], log_attenuation, keys_b, queries_c, groups_here
    )
    gated = mixed * jax.nn.silu(final_modulation_vector.astype(jnp.float32))
    own_rows = lax.all_to_all(
        for_sending(gated), "tp", split_axis=0, concat_axis=1, tiled=True
    ).astype(gated.dtype)
    normed = (
        own_rows
        * lax.rsqrt(jnp.mean(own_rows * own_rows, axis=1, keepdims=True) + EPS)
        * modulated_rescaling_vector[None, :]
    ).astype(jnp.bfloat16)
    middle = (
        carryover_vector.astype(jnp.float32)
        + jnp.dot(normed, blender_final_matrix, preferred_element_type=jnp.float32)
    ).astype(jnp.bfloat16)
    middle_wide = middle.astype(jnp.float32)
    expert_input = (
        middle_wide
        * lax.rsqrt(jnp.mean(middle_wide * middle_wide, axis=1, keepdims=True) + EPS)
        * specialist_rescaling_vector[None, :]
    ).astype(jnp.bfloat16)
    nz, cores, nx = lax.axis_size("sp_0"), lax.axis_size("sp_1"), lax.axis_size("tp")
    core = lax.axis_index("sp_1")
    local_experts = specialist_gating_matrices.shape[0]
    experts = nz * cores * local_experts
    picks = assigned_specialist_ids.shape[1]
    capacity = 2 * row_count * picks // experts
    own_ids = lax.dynamic_slice_in_dim(assigned_specialist_ids, tp_index * row_count, row_count, 0)
    flat_ids = own_ids.reshape(-1)
    member = (flat_ids[:, None] == jnp.arange(experts, dtype=jnp.int32)).astype(jnp.bfloat16)
    earlier = jnp.tril(jnp.ones((flat_ids.shape[0],) * 2, jnp.bfloat16), -1)
    before = jnp.dot(earlier, member, preferred_element_type=jnp.float32)
    position = jnp.sum(before * member.astype(jnp.float32), axis=1).reshape(row_count, picks)
    lifted = jnp.exp(specialist_choice_affinity)
    shares = cluster_chance[:, None] * lifted / jnp.sum(lifted, axis=1, keepdims=True)
    facts = jnp.concatenate([own_ids.astype(jnp.float32), position, shares], axis=1)
    facts = lax.all_gather(facts, "sp_1")
    pair_ids = facts[..., :picks].astype(jnp.int32)
    pair_places = facts[..., picks : 2 * picks].astype(jnp.int32)
    pair_shares = facts[..., 2 * picks :]
    per_core = cores * capacity
    side = jnp.arange(cores, dtype=jnp.int32)[:, None, None]
    holder = pair_ids // local_experts
    slot = (
        (pair_ids % local_experts * nz + holder // cores) * per_core + side * capacity + pair_places
    )
    slot = jnp.where(holder % cores == core, slot, -1).reshape(cores * row_count, picks)
    pair_shares = pair_shares.reshape(cores * row_count, picks)
    slot_count = local_experts * nz * per_core
    slot_axis = jnp.arange(slot_count, dtype=jnp.int32)
    pick_of = jnp.sum((slot[:, :, None] == slot_axis).astype(jnp.float32), axis=1)
    weight_of = jnp.sum(
        jnp.where(slot[:, :, None] == slot_axis, pair_shares[:, :, None], 0.0), axis=1
    )
    pair_rows = lax.all_gather(expert_input, "sp_1", axis=0, tiled=True)
    outgoing = lax.dot_general(
        pick_of.astype(jnp.bfloat16),
        pair_rows,
        (((0,), (0,)), ((), ())),
        preferred_element_type=jnp.float32,
    ).astype(jnp.bfloat16)
    outgoing = outgoing.reshape(local_experts, nz, per_core, model_width)
    arrived = dispatch(outgoing, nz, nx).reshape(local_experts, -1, model_width)
    gate_value = jnp.einsum(
        "lrd,ldf->lrf", arrived, specialist_gating_matrices, preferred_element_type=jnp.float32
    )
    up_value = jnp.einsum(
        "lrd,ldf->lrf", arrived, widening_matrices, preferred_element_type=jnp.float32
    )
    hidden = (jax.nn.silu(gate_value) * up_value).astype(jnp.bfloat16)
    partial_value = jnp.einsum(
        "lrf,lfd->lrd", hidden, contracting_matrices, preferred_element_type=jnp.float32
    ).astype(jnp.bfloat16)
    answers = collect(
        partial_value.reshape(local_experts, nx, nz, per_core, model_width), nz, nx
    ).reshape(slot_count, model_width)
    weight_high = weight_of.astype(jnp.bfloat16)
    weight_low = (weight_of - weight_high.astype(jnp.float32)).astype(jnp.bfloat16)
    gathered = jnp.dot(weight_high, answers, preferred_element_type=jnp.float32) + jnp.dot(
        weight_low, answers, preferred_element_type=jnp.float32
    )
    gathered = gathered.reshape(cores, row_count, model_width)
    kept = lax.dynamic_index_in_dim(gathered, core, 0, keepdims=False)
    given = lax.dynamic_index_in_dim(gathered, cores - 1 - core, 0, keepdims=False)
    taken = lax.ppermute(given, "sp_1", [(0, 1), (1, 0)])
    return (middle_wide + (kept + taken)).astype(jnp.bfloat16)


def solution(mesh):
    finer = Mesh(
        mesh.devices.reshape(mesh.shape["grp"], mesh.shape["sp"] // 2, 2, mesh.shape["tp"]),
        ("grp", "sp_0", "sp_1", "tp"),
    )
    return jax.shard_map(
        per_device,
        mesh=finer,
        in_specs=(
            P(GRP_SP_TP, None),
            P(GRP_SP, "tp"),
            P(GRP_SP, "tp"),
            P(GRP_SP, "tp"),
            P(GRP_SP, "tp"),
            P(GRP_SP, "tp"),
            P(GRP_SP, "tp"),
            P("tp"),
            P(None, "tp"),
            P(None, "tp"),
            P(None, "tp"),
            P(),
            P(),
            P(),
            P(SP, None, "tp"),
            P(SP, None, "tp"),
            P(SP, "tp", None),
            P(GRP_SP, None),
            P(GRP_SP_TP, None),
            P(GRP_SP_TP),
        ),
        out_specs=P(GRP_SP_TP, None),
        check_vma=False,
    )
```

```python
import functools

import jax
import jax.numpy as jnp
from jax import lax
from jax.experimental import pallas as pl
from jax.experimental.pallas import tpu as pltpu
from jax.sharding import Mesh
from jax.sharding import PartitionSpec as P

SP = ("sp_0", "sp_1")
GRP_SP_TP = ("grp", "sp_0", "sp_1", "tp")
GRP_SP = ("grp", "sp_0", "sp_1")


EPS = 1e-06


def hop(step):
    half = (step + 1) // 2
    return jnp.where(step % 2 == 1, half, -half)


def greet(nz, nx):
    z, x = lax.axis_index("sp_0"), lax.axis_index("tp")
    barrier = pltpu.get_barrier_semaphore()

    def signal(k, carry):
        pl.semaphore_signal(barrier, inc=1, device_id={"sp_0": lax.rem(z + k, nz)})
        return carry

    lax.fori_loop(1, nz, signal, 0)
    pl.semaphore_signal(barrier, inc=1, device_id={"tp": lax.rem(x + 1, nx)})
    pl.semaphore_signal(barrier, inc=1, device_id={"tp": lax.rem(x + nx - 1, nx)})
    pl.semaphore_wait(barrier, nz + 1)


def dispatch_kernel(nz, nx, src, dst, zs, zr, xs, xr, fs, fr, here):
    z, x = lax.axis_index("sp_0"), lax.axis_index("tp")
    xp, xm = lax.rem(x + 1, nx), lax.rem(x + nx - 1, nx)
    x2 = lax.rem(x + 2, nx)
    greet(nz, nx)

    def along_z(i):
        to = lax.rem(z + hop(i) + nz, nz)
        return pltpu.make_async_remote_copy(
            src.at[:, to], dst.at[:, x, z], zs.at[i], zr.at[i], device_id={"sp_0": to}
        )

    def origin(i):
        return lax.rem(z - hop(i) + nz, nz)

    def along_x(i, way):
        chunk = dst.at[:, x, origin(i)]
        to = xp if way == 0 else xm
        return pltpu.make_async_remote_copy(
            chunk, chunk, xs.at[way, i], xr.at[way, i], device_id={"tp": to}
        )

    def further(i):
        way = i % 2
        chunk = dst.at[:, jnp.where(way == 0, xm, xp), origin(i)]
        to = jnp.where(way == 0, xp, xm)
        return pltpu.make_async_remote_copy(
            chunk, chunk, fs.at[i], fr.at[i], device_id={"tp": to}
        )

    def arrived_x(i, way):
        chunk = dst.at[:, jnp.where(way == 0, xm, xp), origin(i)]
        return pltpu.make_async_remote_copy(
            chunk, chunk, xs.at[way, i], xr.at[way, i], device_id={"tp": xp}
        )

    def arrived_far(i):
        chunk = dst.at[:, x2, origin(i)]
        return pltpu.make_async_remote_copy(
            chunk, chunk, fs.at[i], fr.at[i], device_id={"tp": xp}
        )

    def send_z(i, carry):
        along_z(i).start()
        return carry

    lax.fori_loop(1, nz, send_z, 0)
    own = pltpu.make_async_copy(src.at[:, z], dst.at[:, x, z], here)
    own.start()
    own.wait()
    along_x(0, 0).start()
    along_x(0, 1).start()

    def spread(i, carry):
        pltpu.make_async_remote_copy(
            src.at[:, z], dst.at[:, x, origin(i)], zs.at[i], zr.at[i], device_id={"tp": xp}
        ).wait_recv()
        along_x(i, 0).start()
        along_x(i, 1).start()
        arrived_x(i - 1, (i - 1) % 2).wait_recv()
        further(i - 1).start()
        return carry

    lax.fori_loop(1, nz, spread, 0)
    arrived_x(nz - 1, (nz - 1) % 2).wait_recv()
    further(nz - 1).start()

    def finish(i, carry):
        arrived_x(i, (i + 1) % 2).wait_recv()
        arrived_far(i).wait_recv()
        along_x(i, 0).wait_send()
        along_x(i, 1).wait_send()
        further(i).wait_send()
        return carry

    lax.fori_loop(0, nz, finish, 0)

    def sent(i, carry):
        along_z(i).wait_send()
        return carry

    lax.fori_loop(1, nz, sent, 0)


def dispatch(outgoing, nz, nx):
    experts, _, rows, width = outgoing.shape
    return pl.pallas_call(
        functools.partial(dispatch_kernel, nz, nx),
        out_shape=jax.ShapeDtypeStruct((experts, nx, nz, rows, width), outgoing.dtype),
        in_specs=[pl.BlockSpec(memory_space=pltpu.VMEM)],
        out_specs=pl.BlockSpec(memory_space=pltpu.VMEM),
        scratch_shapes=[
            pltpu.SemaphoreType.DMA((nz,)),
            pltpu.SemaphoreType.DMA((nz,)),
            pltpu.SemaphoreType.DMA((2, nz)),
            pltpu.SemaphoreType.DMA((2, nz)),
            pltpu.SemaphoreType.DMA((nz,)),
            pltpu.SemaphoreType.DMA((nz,)),
            pltpu.SemaphoreType.DMA,
        ],
        compiler_params=pltpu.CompilerParams(collective_id=1, has_side_effects=True),
        name="dispatch",
    )(outgoing)


def collect_kernel(nz, nx, part, out, far, near, both, mine, total, fs, fr, ns, nr, bs, br, zs, zr, here):
    z, x = lax.axis_index("sp_0"), lax.axis_index("tp")
    xp, xm = lax.rem(x + 1, nx), lax.rem(x + nx - 1, nx)
    x2 = lax.rem(x + 2, nx)
    greet(nz, nx)

    def step_of(s):
        return nz - 1 - s

    def goal(i):
        return lax.rem(z + hop(i) + nz, nz)

    def ahead(i):
        return jnp.where(i % 2 == 0, xp, xm)

    def behind(i):
        return jnp.where(i % 2 == 0, xm, xp)

    def send_far(i):
        return pltpu.make_async_remote_copy(
            part.at[:, x2, goal(i)], far.at[i], fs.at[i], fr.at[i], device_id={"tp": ahead(i)}
        )

    def send_near(i):
        return pltpu.make_async_remote_copy(
            part.at[:, behind(i), goal(i)], near.at[i], ns.at[i], nr.at[i], device_id={"tp": behind(i)}
        )

    def send_both(i):
        return pltpu.make_async_remote_copy(
            mine.at[i], both.at[i], bs.at[i], br.at[i], device_id={"tp": ahead(i)}
        )

    def send_z(i):
        return pltpu.make_async_remote_copy(
            total.at[i], out.at[:, z], zs.at[i], zr.at[i], device_id={"sp_0": goal(i)}
        )

    def first(i):
        send_far(i).start()
        send_near(i).start()

    def second(i):
        send_far(i).wait_recv()
        mine[i] = (
            part[:, ahead(i), goal(i)].astype(jnp.float32) + far[i].astype(jnp.float32)
        ).astype(mine.dtype)
        send_both(i).start()

    def third(i):
        send_near(i).wait_recv()
        send_both(i).wait_recv()
        total[i] = (
            part[:, x, goal(i)].astype(jnp.float32)
            + near[i].astype(jnp.float32)
            + both[i].astype(jnp.float32)
        ).astype(total.dtype)

    first(step_of(0))
    first(step_of(1))
    second(step_of(0))

    def turn(s, carry):
        first(step_of(s))
        second(step_of(s - 1))
        third(step_of(s - 2))
        send_z(step_of(s - 2)).start()
        return carry

    lax.fori_loop(2, nz, turn, 0)
    second(step_of(nz - 1))
    third(step_of(nz - 2))
    send_z(step_of(nz - 2)).start()
    third(step_of(nz - 1))
    own = pltpu.make_async_copy(total.at[0], out.at[:, z], here)
    own.start()
    own.wait()

    def finish(i, carry):
        send_far(i).wait_send()
        send_near(i).wait_send()
        send_both(i).wait_send()
        return carry

    lax.fori_loop(0, nz, finish, 0)

    def sent(i, carry):
        send_z(i).wait_send()
        pltpu.make_async_remote_copy(
            total.at[i], out.at[:, lax.rem(z - hop(i) + nz, nz)], zs.at[i], zr.at[i], device_id={"tp": xp}
        ).wait_recv()
        return carry

    lax.fori_loop(1, nz, sent, 0)


def collect(part, nz, nx):
    experts, _, _, rows, width = part.shape
    slots = pltpu.VMEM((nz, experts, rows, width), part.dtype)
    return pl.pallas_call(
        functools.partial(collect_kernel, nz, nx),
        out_shape=jax.ShapeDtypeStruct((experts, nz, rows, width), part.dtype),
        in_specs=[pl.BlockSpec(memory_space=pltpu.VMEM)],
        out_specs=pl.BlockSpec(memory_space=pltpu.VMEM),
        scratch_shapes=[slots] * 5
        + [pltpu.SemaphoreType.DMA((nz,))] * 8
        + [pltpu.SemaphoreType.DMA],
        compiler_params=pltpu.CompilerParams(collective_id=2, has_side_effects=True),
        name="collect",
    )(part)


QUAD = 4
TAIL = 16


def greet_all(nz, nx):
    z, c, x = lax.axis_index("sp_0"), lax.axis_index("sp_1"), lax.axis_index("tp")
    barrier = pltpu.get_barrier_semaphore()

    def along_z(k, carry):
        pl.semaphore_signal(barrier, inc=1, device_id={"sp_0": lax.rem(z + k, nz)})
        return carry

    def along_x(k, carry):
        pl.semaphore_signal(barrier, inc=1, device_id={"tp": lax.rem(x + k, nx)})
        return carry

    lax.fori_loop(1, nz, along_z, 0)
    lax.fori_loop(1, nx, along_x, 0)
    pl.semaphore_signal(barrier, inc=1, device_id={"sp_1": 1 - c})
    pl.semaphore_signal(
        barrier, inc=1, device_id={"sp_0": lax.rem(z + nz - 1 + 2 * c, nz), "sp_1": 1 - c}
    )
    pl.semaphore_wait(barrier, nz + nx)


def silu(v):
    return v * jax.nn.sigmoid(v)


def exact_dot(a, b):
    return jnp.dot(a, b, preferred_element_type=jnp.float32, precision=lax.Precision.HIGHEST)


def packed(state, decays):
    lanes = state.shape[1]
    row = lax.broadcasted_iota(jnp.int32, (TAIL, lanes), 0)
    tail = jnp.zeros((TAIL, lanes), jnp.float32)
    for h, decay in enumerate(decays):
        wide = jnp.broadcast_to(decay, (TAIL, lanes))
        high = wide.astype(jnp.bfloat16).astype(jnp.float32)
        tail = jnp.where(row == h, high, tail)
        tail = jnp.where(row == TAIL // 2 + h, wide - high, tail)
    return jnp.concatenate([state.astype(jnp.bfloat16), tail.astype(jnp.bfloat16)], axis=0)


def unpacked(message, heads):
    rows = message.shape[0] - TAIL
    state = message[:rows].astype(jnp.float32)
    tail = message[rows:].astype(jnp.float32)
    half = TAIL // 2
    return state, [tail[h : h + 1, 0:1] + tail[half + h : half + h + 1, 0:1] for h in range(heads)]


def per_row(decays, rows, lanes):
    each = rows // len(decays)
    return jnp.concatenate([jnp.broadcast_to(d, (each, lanes)) for d in decays], axis=0)


def followed(earlier, later):
    (state_a, decay_a), (state_b, decay_b) = earlier, later
    state = state_a * per_row(decay_b, *state_a.shape) + state_b
    return state, [a * b for a, b in zip(decay_a, decay_b)]


def chosen(flag, one, other):
    return jnp.where(flag, one[0], other[0]), [
        jnp.where(flag, a, b) for a, b in zip(one[1], other[1])
    ]


def front_kernel(
    nz,
    nx,
    capacity,
    xs_ref,
    gate_ref,
    keys_ref,
    queries_ref,
    raw_ref,
    extra_ref,
    rate_ref,
    taps_ref,
    gain_ref,
    blend_hbm,
    carry_ref,
    gain2_ref,
    ids_ref,
    affinity_ref,
    chance_ref,
    outgoing_ref,
    middle_ref,
    weight_ref,
    halo,
    joined,
    pair_out,
    pair_in,
    quad_out,
    quad_in,
    far_out,
    far_in,
    half_out,
    half_in,
    gated_out,
    gated_in,
    facts,
    rows,
    blend,
    blend_sem,
    halo_s,
    halo_r,
    pair_s,
    pair_r,
    quad_s,
    quad_r,
    far_s,
    far_r,
    gated_s,
    gated_r,
):
    z, c, x = lax.axis_index("sp_0"), lax.axis_index("sp_1"), lax.axis_index("tp")
    length, width_x = xs_ref.shape
    state_width = keys_ref.shape[1]
    heads = raw_ref.shape[1]
    head_dim = width_x // heads
    half_heads = heads // 2
    half_rows = width_x // 2
    place, quad = lax.rem(z, QUAD), z // QUAD
    quads = nz // QUAD
    f32, bf16 = jnp.float32, jnp.bfloat16
    partner = {"sp_1": 1 - c}
    load = pltpu.make_async_copy(blend_hbm, blend, blend_sem)
    load.start()

    count, picks = ids_ref.shape[0] // nx, ids_ref.shape[1]
    local_experts = outgoing_ref.shape[0]
    experts = nz * 2 * local_experts
    ids = ids_ref[pl.ds(pl.multiple_of(x * count, count), count), :]
    expert_axis = lax.broadcasted_iota(jnp.int32, (count, experts), 1)
    member = [(ids[:, k : k + 1] == expert_axis).astype(f32) for k in range(picks)]
    row_axis = lax.broadcasted_iota(jnp.int32, (count, count), 0)
    column_axis = lax.broadcasted_iota(jnp.int32, (count, count), 1)
    earlier = (row_axis > column_axis).astype(bf16)
    before = jnp.dot(earlier, sum(member).astype(bf16), preferred_element_type=f32)
    lifted = jnp.exp(affinity_ref[...])
    shares = chance_ref[...] * lifted / jnp.sum(lifted, axis=1, keepdims=True)
    lane = lax.broadcasted_iota(jnp.int32, (count, facts.shape[2]), 1)
    noted = jnp.zeros((count, facts.shape[2]), f32)
    for k in range(picks):
        position = jnp.sum(before * member[k], axis=1, keepdims=True)
        expert = ids[:, k : k + 1]
        holder = lax.div(expert, local_experts)
        slot = (
            (lax.rem(expert, local_experts) * nz + lax.div(holder, 2)) * 2 + c
        ) * capacity + position.astype(jnp.int32)
        for core in range(2):
            there = jnp.where(lax.rem(holder, 2) == core, slot, -1).astype(f32)
            noted = jnp.where(lane == core * picks + k, there, noted)
        noted = jnp.where(lane == 2 * picks + k, shares[:, k : k + 1], noted)
    facts[c] = noted

    greet_all(nz, nx)
    rim = halo.shape[0]
    after = {"sp_0": lax.rem(z + c, nz), "sp_1": 1 - c}
    edges = []
    start = 0
    for n, ref in enumerate((xs_ref, keys_ref, queries_ref)):
        columns = pl.ds(start, ref.shape[1])
        edges.append(
            pltpu.make_async_remote_copy(
                ref.at[pl.ds(length - rim, rim)],
                halo.at[:, columns],
                halo_s.at[n],
                halo_r.at[n],
                device_id=after,
            )
        )
        start += ref.shape[1]
    for edge in edges:
        edge.start()
    facts_copy = pltpu.make_async_remote_copy(
        facts.at[c], facts.at[c], pair_s.at[0], pair_r.at[0], device_id=partner
    )
    facts_copy.start()

    stride = jnp.maximum(raw_ref[...], 0.0) + jnp.log1p(jnp.exp(-jnp.abs(raw_ref[...])))
    log_decay = extra_ref[...] - rate_ref[...] * stride
    lane = lax.broadcasted_iota(jnp.int32, (length, 128), 1)
    padded = jnp.zeros((length, 128), f32)
    for h in range(heads):
        padded = jnp.where(lane == h, log_decay[:, h : h + 1], padded)
    t_axis = lax.broadcasted_iota(jnp.int32, (length, length), 0)
    s_axis = lax.broadcasted_iota(jnp.int32, (length, length), 1)
    causal = t_axis >= s_axis
    running = exact_dot(causal.astype(f32), padded)
    running_row = running.T
    final = running[length - 1 : length, :]

    start = 0
    for ref in (xs_ref, keys_ref, queries_ref):
        joined[rim:, start : start + ref.shape[1]] = ref[...].astype(f32)
        start += ref.shape[1]
    for edge in edges:
        edge.wait_recv()
    joined[:rim, :] = jnp.where(z + c > 0, halo[...].astype(f32), 0.0)
    kernel_len = taps_ref.shape[0]
    convolved = taps_ref[0:1, :] * joined[rim - kernel_len + 1 : rim - kernel_len + 1 + length, :]
    for tap in range(1, kernel_len):
        first = rim - kernel_len + 1 + tap
        convolved = convolved + taps_ref[tap : tap + 1, :] * joined[first : first + length, :]
    convolved = silu(convolved)
    inputs_x = convolved[:, :width_x]
    keys_b = convolved[:, width_x : width_x + state_width].astype(bf16)
    queries_c = convolved[:, width_x + state_width :].astype(bf16)

    scaled = [
        inputs_x[:, h * head_dim : (h + 1) * head_dim] * stride[:, h : h + 1] for h in range(heads)
    ]
    remaining = jnp.concatenate(
        [scaled[h] * jnp.exp(final[:, h : h + 1] - running[:, h : h + 1]) for h in range(heads)],
        axis=1,
    ).astype(bf16)
    own_state = lax.dot_general(
        remaining, keys_b, (((0,), (0,)), ((), ())), preferred_element_type=f32
    )
    pair_out[...] = packed(own_state, [jnp.exp(final[:, h : h + 1]) for h in range(heads)])
    pair_copy = pltpu.make_async_remote_copy(
        pair_out, pair_in, pair_s.at[1], pair_r.at[1], device_id=partner
    )
    pair_copy.start()

    scores = lax.dot_general(
        queries_c, keys_b, (((1,), (1,)), ((), ())), preferred_element_type=f32
    )
    inside = []
    for h in range(heads):
        between = running[:, h : h + 1] - running_row[h : h + 1, :]
        decays = jnp.exp(jnp.where(causal, between, -1e30))
        inside.append(
            jnp.dot(
                (scores * decays).astype(bf16), scaled[h].astype(bf16), preferred_element_type=f32
            )
        )

    pair_copy.wait_recv()

    def half_of(ref):
        state, decays = unpacked(ref[...], heads)
        return (
            jnp.where(c == 0, state[:half_rows], state[half_rows:]),
            [jnp.where(c == 0, decays[j], decays[half_heads + j]) for j in range(half_heads)],
        )

    ours, theirs = half_of(pair_out), half_of(pair_in)
    lower, upper = chosen(c == 0, ours, theirs), chosen(c == 0, theirs, ours)
    chip = followed(lower, upper)
    quad_out[...] = packed(*chip)

    def quad_send(k):
        to = quad * QUAD + lax.rem(place + k, QUAD)
        return pltpu.make_async_remote_copy(
            quad_out, quad_in.at[place], quad_s.at[k], quad_r.at[k], device_id={"sp_0": to}
        )

    def quad_arrival(k):
        return pltpu.make_async_remote_copy(
            quad_out,
            quad_in.at[lax.rem(place + QUAD - k, QUAD)],
            quad_s.at[k],
            quad_r.at[k],
            device_id={"sp_0": lax.rem(z + 1, nz)},
        )

    for k in range(1, QUAD):
        quad_send(k).start()
    quad_in[place] = quad_out[...]
    for k in range(1, QUAD):
        quad_arrival(k).wait_recv()
    nothing = (jnp.zeros_like(chip[0]), [jnp.ones_like(d) for d in chip[1]])
    whole, inner = nothing, nothing
    for k in range(QUAD):
        inner = chosen(place == k, whole, inner)
        whole = followed(whole, unpacked(quad_in[k], half_heads))
    far_out[...] = packed(*whole)

    def far_send(k):
        return pltpu.make_async_remote_copy(
            far_out,
            far_in.at[k],
            far_s.at[k],
            far_r.at[k],
            device_id={"sp_0": lax.rem(z + k * QUAD, nz)},
        )

    for k in range(1, quads):

        @pl.when(quad + k < quads)
        def _(k=k):
            far_send(k).start()

    far_in[0] = jnp.zeros_like(far_out)
    for k in range(1, quads):

        @pl.when(quad >= k)
        def _(k=k):
            far_send(k).wait_recv()

        @pl.when(quad < k)
        def _(k=k):
            far_in[k] = jnp.zeros_like(far_out)

    incoming = nothing
    for k in reversed(range(1, quads)):
        incoming = followed(incoming, unpacked(far_in[k], half_heads))
    incoming = followed(incoming, inner)
    incoming_low = incoming[0]
    incoming_high = followed(incoming, lower)[0]
    half_out[...] = jnp.where(c == 0, incoming_high, incoming_low).astype(bf16)
    half_copy = pltpu.make_async_remote_copy(
        half_out, half_in, pair_s.at[2], pair_r.at[2], device_id=partner
    )
    half_copy.start()
    kept = jnp.where(c == 0, incoming_low, incoming_high).astype(bf16)
    modulation = silu(gate_ref[...].astype(f32))
    half_copy.wait_recv()
    sent_in = half_in[...]
    entering = jnp.concatenate(
        [jnp.where(c == 0, kept, sent_in), jnp.where(c == 0, sent_in, kept)], axis=0
    )
    outside = lax.dot_general(
        queries_c, entering, (((1,), (1,)), ((), ())), preferred_element_type=f32
    )
    mixed = jnp.concatenate(
        [
            inside[h]
            + outside[:, h * head_dim : (h + 1) * head_dim] * jnp.exp(running[:, h : h + 1])
            for h in range(heads)
        ],
        axis=1,
    )
    gated_out[...] = (mixed * modulation).astype(bf16).reshape(gated_out.shape)

    def gated_send(k):
        to = lax.rem(x + k, nx)
        return pltpu.make_async_remote_copy(
            gated_out.at[to], gated_in.at[x], gated_s.at[k], gated_r.at[k], device_id={"tp": to}
        )

    for k in range(1, nx):
        gated_send(k).start()
    gated_in[x] = gated_out[x]
    facts_arrival = pltpu.make_async_remote_copy(
        facts.at[1 - c], facts.at[1 - c], pair_s.at[0], pair_r.at[0], device_id=partner
    )
    facts_arrival.wait_recv()
    slot_count = weight_ref.shape[1]
    slot_axis = lax.broadcasted_iota(jnp.int32, (2 * count, slot_count), 1).astype(f32)
    known = jnp.concatenate([facts[0], facts[1]], axis=0)
    picked = jnp.zeros((2 * count, slot_count), f32)
    weight = jnp.zeros((2 * count, slot_count), f32)
    for k in range(picks):
        slot = jnp.where(c == 0, known[:, k : k + 1], known[:, picks + k : picks + k + 1])
        hit = slot == slot_axis
        picked = jnp.where(hit, 1.0, picked)
        weight = jnp.where(hit, known[:, 2 * picks + k : 2 * picks + k + 1], weight)
    weight_ref[...] = weight
    for k in range(1, nx):
        pltpu.make_async_remote_copy(
            gated_out.at[x],
            gated_in.at[lax.rem(x + nx - k, nx)],
            gated_s.at[k],
            gated_r.at[k],
            device_id={"tp": lax.rem(x + k, nx)},
        ).wait_recv()
    own_rows = jnp.concatenate([gated_in[k] for k in range(nx)], axis=1).astype(f32)
    normed = (
        own_rows
        * lax.rsqrt(jnp.mean(own_rows * own_rows, axis=1, keepdims=True) + EPS)
        * gain_ref[...]
    ).astype(bf16)
    load.wait()
    middle = (
        carry_ref[...].astype(f32) + jnp.dot(normed, blend[...], preferred_element_type=f32)
    ).astype(bf16)
    middle_ref[...] = middle
    wide = middle.astype(f32)
    rows[c] = (
        wide
        * lax.rsqrt(jnp.mean(wide * wide, axis=1, keepdims=True) + EPS)
        * gain2_ref[...]
    ).astype(bf16)
    rows_copy = pltpu.make_async_remote_copy(
        rows.at[c], rows.at[c], pair_s.at[3], pair_r.at[3], device_id=partner
    )
    rows_copy.start()
    pltpu.make_async_remote_copy(
        rows.at[1 - c], rows.at[1 - c], pair_s.at[3], pair_r.at[3], device_id=partner
    ).wait_recv()
    outgoing_ref[...] = (
        lax.dot_general(
            picked.astype(bf16),
            jnp.concatenate([rows[0], rows[1]], axis=0),
            (((0,), (0,)), ((), ())),
            preferred_element_type=f32,
        )
        .astype(bf16)
        .reshape(outgoing_ref.shape)
    )

    for edge in edges:
        edge.wait_send()
    facts_copy.wait_send()
    pair_copy.wait_send()
    half_copy.wait_send()
    rows_copy.wait_send()
    for k in range(1, QUAD):
        quad_send(k).wait_send()
    for k in range(1, quads):

        @pl.when(quad + k < quads)
        def _(k=k):
            far_send(k).wait_send()

    for k in range(1, nx):
        gated_send(k).wait_send()


def front(nz, nx, local_experts, capacity, *arrays):
    xs, _, keys, queries, raw = arrays[:5]
    blend, carry = arrays[9:11]
    count, width = carry.shape
    slots = local_experts * nz * 2 * capacity
    channels = xs.shape[1]
    total = channels + keys.shape[1] + queries.shape[1]
    rim = 8
    states = keys.shape[1]
    bf16 = jnp.bfloat16
    vmem = pl.BlockSpec(memory_space=pltpu.VMEM)
    half = channels // 2
    return pl.pallas_call(
        functools.partial(front_kernel, nz, nx, capacity),
        out_shape=(
            jax.ShapeDtypeStruct((local_experts, nz, 2 * capacity, width), bf16),
            jax.ShapeDtypeStruct((count, width), bf16),
            jax.ShapeDtypeStruct((2 * count, slots), jnp.float32),
        ),
        in_specs=[vmem] * 9 + [pl.BlockSpec(memory_space=pl.ANY)] + [vmem] * 5,
        out_specs=(vmem, vmem, vmem),
        scratch_shapes=[
            pltpu.VMEM((rim, total), bf16),
            pltpu.VMEM((rim + xs.shape[0], total), jnp.float32),
            pltpu.VMEM((channels + TAIL, states), bf16),
            pltpu.VMEM((channels + TAIL, states), bf16),
            pltpu.VMEM((half + TAIL, states), bf16),
            pltpu.VMEM((QUAD, half + TAIL, states), bf16),
            pltpu.VMEM((half + TAIL, states), bf16),
            pltpu.VMEM((nz // QUAD, half + TAIL, states), bf16),
            pltpu.VMEM((half, states), bf16),
            pltpu.VMEM((half, states), bf16),
            pltpu.VMEM((nx, count, channels), bf16),
            pltpu.VMEM((nx, count, channels), bf16),
            pltpu.VMEM((2, count, 128), jnp.float32),
            pltpu.VMEM((2, count, width), bf16),
            pltpu.VMEM(blend.shape, bf16),
            pltpu.SemaphoreType.DMA,
            pltpu.SemaphoreType.DMA((3,)),
            pltpu.SemaphoreType.DMA((3,)),
            pltpu.SemaphoreType.DMA((4,)),
            pltpu.SemaphoreType.DMA((4,)),
            pltpu.SemaphoreType.DMA((QUAD,)),
            pltpu.SemaphoreType.DMA((QUAD,)),
            pltpu.SemaphoreType.DMA((nz // QUAD,)),
            pltpu.SemaphoreType.DMA((nz // QUAD,)),
            pltpu.SemaphoreType.DMA((nx,)),
            pltpu.SemaphoreType.DMA((nx,)),
        ],
        compiler_params=pltpu.CompilerParams(collective_id=3, has_side_effects=True),
        name="front",
    )(*arrays)


def per_device(
    carryover_vector,
    channel_source_entries,
    final_modulation_vector,
    entering_basis_matrix,
    readout_basis_matrix,
    raw_stride_amount,
    extra_log_attenuation,
    channel_fading_rate,
    channel_source_kernel,
    entering_basis_kernel,
    readout_basis_kernel,
    modulated_rescaling_vector,
    blender_final_matrix,
    specialist_rescaling_vector,
    specialist_gating_matrices,
    widening_matrices,
    contracting_matrices,
    assigned_specialist_ids,
    specialist_choice_affinity,
    cluster_chance,
):
    nz, cores, nx = lax.axis_size("sp_0"), lax.axis_size("sp_1"), lax.axis_size("tp")
    core = lax.axis_index("sp_1")
    row_count, model_width = carryover_vector.shape
    local_experts = specialist_gating_matrices.shape[0]
    experts = nz * cores * local_experts
    picks = assigned_specialist_ids.shape[1]
    capacity = 2 * row_count * picks // experts
    per_core = cores * capacity
    taps = jnp.concatenate(
        [channel_source_kernel, entering_basis_kernel, readout_basis_kernel], axis=1
    )
    outgoing, middle, weight_of = front(
        nz,
        nx,
        local_experts,
        capacity,
        channel_source_entries,
        final_modulation_vector,
        entering_basis_matrix,
        readout_basis_matrix,
        raw_stride_amount,
        extra_log_attenuation,
        channel_fading_rate[None, :],
        taps,
        modulated_rescaling_vector[None, :],
        blender_final_matrix,
        carryover_vector,
        specialist_rescaling_vector[None, :],
        assigned_specialist_ids,
        specialist_choice_affinity,
        cluster_chance[:, None],
    )
    middle_wide = middle.astype(jnp.float32)
    slot_count = weight_of.shape[1]
    arrived = dispatch(outgoing, nz, nx).reshape(local_experts, -1, model_width)
    gate_value = jnp.einsum(
        "lrd,ldf->lrf", arrived, specialist_gating_matrices, preferred_element_type=jnp.float32
    )
    up_value = jnp.einsum(
        "lrd,ldf->lrf", arrived, widening_matrices, preferred_element_type=jnp.float32
    )
    hidden = (jax.nn.silu(gate_value) * up_value).astype(jnp.bfloat16)
    partial_value = jnp.einsum(
        "lrf,lfd->lrd", hidden, contracting_matrices, preferred_element_type=jnp.float32
    ).astype(jnp.bfloat16)
    answers = collect(
        partial_value.reshape(local_experts, nx, nz, per_core, model_width), nz, nx
    ).reshape(slot_count, model_width)
    weight_high = weight_of.astype(jnp.bfloat16)
    weight_low = (weight_of - weight_high.astype(jnp.float32)).astype(jnp.bfloat16)
    gathered = jnp.dot(weight_high, answers, preferred_element_type=jnp.float32) + jnp.dot(
        weight_low, answers, preferred_element_type=jnp.float32
    )
    gathered = gathered.reshape(cores, row_count, model_width)
    kept = lax.dynamic_index_in_dim(gathered, core, 0, keepdims=False)
    given = lax.dynamic_index_in_dim(gathered, cores - 1 - core, 0, keepdims=False)
    taken = lax.ppermute(given, "sp_1", [(0, 1), (1, 0)])
    return (middle_wide + (kept + taken)).astype(jnp.bfloat16)


def solution(mesh):
    finer = Mesh(
        mesh.devices.reshape(mesh.shape["grp"], mesh.shape["sp"] // 2, 2, mesh.shape["tp"]),
        ("grp", "sp_0", "sp_1", "tp"),
    )
    return jax.shard_map(
        per_device,
        mesh=finer,
        in_specs=(
            P(GRP_SP_TP, None),
            P(GRP_SP, "tp"),
            P(GRP_SP, "tp"),
            P(GRP_SP, "tp"),
            P(GRP_SP, "tp"),
            P(GRP_SP, "tp"),
            P(GRP_SP, "tp"),
            P("tp"),
            P(None, "tp"),
            P(None, "tp"),
            P(None, "tp"),
            P(),
            P(),
            P(),
            P(SP, None, "tp"),
            P(SP, None, "tp"),
            P(SP, "tp", None),
            P(GRP_SP, None),
            P(GRP_SP_TP, None),
            P(GRP_SP_TP),
        ),
        out_specs=P(GRP_SP_TP, None),
        check_vma=False,
    )
```

```python
import functools

import jax
import jax.numpy as jnp
from jax import lax
from jax.experimental import pallas as pl
from jax.experimental.pallas import tpu as pltpu
from jax.sharding import Mesh
from jax.sharding import PartitionSpec as P

SP = ("sp_0", "sp_1")
GRP_SP_TP = ("grp", "sp_0", "sp_1", "tp")
GRP_SP = ("grp", "sp_0", "sp_1")


EPS = 1e-06


def hop(step):
    half = (step + 1) // 2
    return jnp.where(step % 2 == 1, half, -half)


def greet(nz, nx):
    z, c, x = lax.axis_index("sp_0"), lax.axis_index("sp_1"), lax.axis_index("tp")
    barrier = pltpu.get_barrier_semaphore()

    def signal(k, carry):
        pl.semaphore_signal(barrier, inc=1, device_id={"sp_0": lax.rem(z + k, nz)})
        return carry

    lax.fori_loop(1, nz, signal, 0)
    pl.semaphore_signal(barrier, inc=1, device_id={"tp": lax.rem(x + 1, nx)})
    pl.semaphore_signal(barrier, inc=1, device_id={"tp": lax.rem(x + nx - 1, nx)})
    pl.semaphore_signal(barrier, inc=1, device_id={"sp_1": 1 - c})
    pl.semaphore_wait(barrier, nz + 2)


def experts_kernel(
    nz,
    nx,
    src,
    gates_hbm,
    ups_hbm,
    downs_hbm,
    middle_ref,
    weight_ref,
    out_ref,
    arrived,
    part,
    far,
    near,
    both,
    mine,
    total,
    answers,
    gates,
    ups,
    downs,
    given,
    taken,
    load_sem,
    here,
    zs,
    zr,
    xs,
    xr,
    os_,
    or_,
    fs,
    fr,
    ns,
    nr,
    bs,
    br,
    ts,
    tr,
    ps,
    pr,
):
    z, c, x = lax.axis_index("sp_0"), lax.axis_index("sp_1"), lax.axis_index("tp")
    xp, xm = lax.rem(x + 1, nx), lax.rem(x + nx - 1, nx)
    x2 = lax.rem(x + 2, nx)
    local_experts, _, rows, width = src.shape
    f32, bf16 = jnp.float32, jnp.bfloat16
    loads = [
        pltpu.make_async_copy(a, b, load_sem.at[n])
        for n, (a, b) in enumerate(((gates_hbm, gates), (ups_hbm, ups), (downs_hbm, downs)))
    ]
    for load in loads:
        load.start()
    greet(nz, nx)

    def goal(i):
        return lax.rem(z + hop(i) + nz, nz)

    def origin(i):
        return lax.rem(z - hop(i) + nz, nz)

    def ahead(i):
        return jnp.where(i % 2 == 0, xp, xm)

    def behind(i):
        return jnp.where(i % 2 == 0, xm, xp)

    def remote(a, b, sent, got, **to):
        return pltpu.make_async_remote_copy(a, b, sent, got, device_id=to)

    def along_z(i):
        return remote(src.at[:, goal(i)], arrived.at[i, :, x], zs.at[i], zr.at[i], sp_0=goal(i))

    def along_x(i, way):
        chunk = arrived.at[i, :, x]
        to = xp if way == 0 else xm
        return remote(chunk, chunk, xs.at[way, i], xr.at[way, i], tp=to)

    def from_x(i, way):
        chunk = arrived.at[i, :, jnp.where(way == 0, xm, xp)]
        return remote(chunk, chunk, xs.at[way, i], xr.at[way, i], tp=xp)

    def onward(i):
        chunk = arrived.at[i, :, behind(i)]
        return remote(chunk, chunk, os_.at[i], or_.at[i], tp=ahead(i))

    def from_far(i):
        chunk = arrived.at[i, :, x2]
        return remote(chunk, chunk, os_.at[i], or_.at[i], tp=xp)

    def send_far(i):
        return remote(part.at[i, :, x2], far.at[i], fs.at[i], fr.at[i], tp=ahead(i))

    def send_near(i):
        return remote(part.at[i, :, behind(i)], near.at[i], ns.at[i], nr.at[i], tp=behind(i))

    def send_both(i):
        return remote(mine.at[i], both.at[i], bs.at[i], br.at[i], tp=ahead(i))

    def send_back(i):
        return remote(total.at[i], answers.at[:, z], ts.at[i], tr.at[i], sp_0=origin(i))

    def send_z(i, carry):
        along_z(i).start()
        return carry

    lax.fori_loop(1, nz, send_z, 0)
    own = pltpu.make_async_copy(src.at[:, z], arrived.at[0, :, x], here.at[0])
    own.start()
    own.wait()

    def spread(i):
        along_x(i, 0).start()
        along_x(i, 1).start()

    def pass_on(i):
        from_x(i, i % 2).wait_recv()
        onward(i).start()

    def complete(i):
        from_x(i, (i + 1) % 2).wait_recv()
        from_far(i).wait_recv()

    def multiply(i):
        for e in range(local_experts):
            tokens = jnp.concatenate(
                [
                    arrived[i + k, e].astype(f32).reshape(nx * rows, width).astype(bf16)
                    for k in range(2)
                ],
                axis=0,
            )
            gate = jnp.dot(tokens, gates[e], preferred_element_type=f32)
            up = jnp.dot(tokens, ups[e], preferred_element_type=f32)
            hidden = (silu(gate) * up).astype(bf16)
            result = jnp.dot(hidden, downs[e], preferred_element_type=f32)
            for k in range(2):
                part[i + k, e] = (
                    result[k * nx * rows : (k + 1) * nx * rows].reshape(nx, rows, width).astype(bf16)
                )

    def first(i):
        send_far(i).start()
        send_near(i).start()

    def second(i):
        send_far(i).wait_recv()
        mine[i] = (part[i, :, ahead(i)].astype(f32) + far[i].astype(f32)).astype(bf16)
        send_both(i).start()

    def third(i):
        send_near(i).wait_recv()
        send_both(i).wait_recv()
        total[i] = (
            part[i, :, x].astype(f32) + near[i].astype(f32) + both[i].astype(f32)
        ).astype(bf16)

    pairs = nz // 2

    def turn(p, carry):
        i = 2 * p

        @pl.when(p == 0)
        def _():
            spread(0)

        @pl.when((p > 0) & (p < pairs))
        def _():
            remote(src.at[:, z], arrived.at[i, :, x], zs.at[i], zr.at[i], tp=xp).wait_recv()
            spread(i)

        @pl.when((p > 0) & (p <= pairs))
        def _():
            pass_on(i - 1)

        @pl.when(p < pairs)
        def _():
            remote(src.at[:, z], arrived.at[i + 1, :, x], zs.at[i + 1], zr.at[i + 1], tp=xp).wait_recv()
            spread(i + 1)
            pass_on(i)

        @pl.when(p == 1)
        def _():
            for load in loads:
                load.wait()

        @pl.when((p > 0) & (p <= pairs))
        def _():
            complete(i - 2)
            complete(i - 1)
            multiply(i - 2)
            first(i - 2)
            first(i - 1)

        @pl.when((p > 1) & (p <= pairs + 1))
        def _():
            second(i - 4)
            second(i - 3)

        @pl.when(p > 2)
        def _():
            third(i - 6)
            third(i - 5)

            @pl.when(p > 3)
            def _():
                send_back(i - 6).start()

            send_back(i - 5).start()

        return carry

    lax.fori_loop(0, pairs + 3, turn, 0)
    own_back = pltpu.make_async_copy(total.at[0], answers.at[:, z], here.at[1])
    own_back.start()
    own_back.wait()

    def sent(i, carry):
        along_x(i, 0).wait_send()
        along_x(i, 1).wait_send()
        onward(i).wait_send()
        send_far(i).wait_send()
        send_near(i).wait_send()
        send_both(i).wait_send()
        return carry

    lax.fori_loop(0, nz, sent, 0)

    def returned(i, carry):
        along_z(i).wait_send()
        send_back(i).wait_send()
        remote(total.at[i], answers.at[:, goal(i)], ts.at[i], tr.at[i], tp=xp).wait_recv()
        return carry

    lax.fori_loop(1, nz, returned, 0)

    count = out_ref.shape[0]
    slots = local_experts * nz * rows
    known = answers[...].astype(f32).reshape(slots, width).astype(bf16)

    def shared(start):
        weight = weight_ref[pl.ds(pl.multiple_of(start * count, count), count), :]
        high = weight.astype(bf16)
        low = (weight - high.astype(f32)).astype(bf16)
        return jnp.dot(high, known, preferred_element_type=f32) + jnp.dot(
            low, known, preferred_element_type=f32
        )

    given[...] = shared(1 - c)
    swap = remote(given, taken, ps, pr, sp_1=1 - c)
    swap.start()
    kept = middle_ref[...].astype(f32) + shared(c)
    swap.wait()
    out_ref[...] = (kept + taken[...]).astype(bf16)


def routed(outgoing, gates, ups, downs, middle, weight, nz, nx):
    experts, _, rows, width = outgoing.shape
    bf16 = jnp.bfloat16
    slots = pltpu.VMEM((nz, experts, rows, width), bf16)
    wide = pltpu.VMEM((nz, experts, nx, rows, width), bf16)
    count = middle.shape[0]
    vmem = pl.BlockSpec(memory_space=pltpu.VMEM)
    anywhere = pl.BlockSpec(memory_space=pl.ANY)
    line = pltpu.SemaphoreType.DMA((nz,))
    return pl.pallas_call(
        functools.partial(experts_kernel, nz, nx),
        out_shape=jax.ShapeDtypeStruct((count, width), bf16),
        in_specs=[vmem, anywhere, anywhere, anywhere, vmem, vmem],
        out_specs=vmem,
        scratch_shapes=[wide, wide, slots, slots, slots, slots, slots]
        + [pltpu.VMEM((experts, nz, rows, width), bf16)]
        + [pltpu.VMEM(w.shape, bf16) for w in (gates, ups, downs)]
        + [pltpu.VMEM((count, width), jnp.float32)] * 2
        + [pltpu.SemaphoreType.DMA((3,)), pltpu.SemaphoreType.DMA((2,))]
        + [line, line]
        + [pltpu.SemaphoreType.DMA((2, nz))] * 2
        + [line] * 10
        + [pltpu.SemaphoreType.DMA] * 2,
        compiler_params=pltpu.CompilerParams(
            collective_id=1, has_side_effects=True, vmem_limit_bytes=60 << 20
        ),
        name="experts",
    )(outgoing, gates, ups, downs, middle, weight)


QUAD = 4
TAIL = 16


def greet_all(nz, nx):
    z, c, x = lax.axis_index("sp_0"), lax.axis_index("sp_1"), lax.axis_index("tp")
    barrier = pltpu.get_barrier_semaphore()

    def along_z(k, carry):
        pl.semaphore_signal(barrier, inc=1, device_id={"sp_0": lax.rem(z + k, nz)})
        return carry

    def along_x(k, carry):
        pl.semaphore_signal(barrier, inc=1, device_id={"tp": lax.rem(x + k, nx)})
        return carry

    lax.fori_loop(1, nz, along_z, 0)
    lax.fori_loop(1, nx, along_x, 0)
    pl.semaphore_signal(barrier, inc=1, device_id={"sp_1": 1 - c})
    pl.semaphore_signal(
        barrier, inc=1, device_id={"sp_0": lax.rem(z + nz - 1 + 2 * c, nz), "sp_1": 1 - c}
    )
    pl.semaphore_wait(barrier, nz + nx)


def silu(v):
    return v * jax.nn.sigmoid(v)


def exact_dot(a, b):
    return jnp.dot(a, b, preferred_element_type=jnp.float32, precision=lax.Precision.HIGHEST)


def packed(state, decays):
    lanes = state.shape[1]
    row = lax.broadcasted_iota(jnp.int32, (TAIL, lanes), 0)
    tail = jnp.zeros((TAIL, lanes), jnp.float32)
    for h, decay in enumerate(decays):
        wide = jnp.broadcast_to(decay, (TAIL, lanes))
        high = wide.astype(jnp.bfloat16).astype(jnp.float32)
        tail = jnp.where(row == h, high, tail)
        tail = jnp.where(row == TAIL // 2 + h, wide - high, tail)
    return jnp.concatenate([state.astype(jnp.bfloat16), tail.astype(jnp.bfloat16)], axis=0)


def unpacked(message, heads):
    rows = message.shape[0] - TAIL
    state = message[:rows].astype(jnp.float32)
    tail = message[rows:].astype(jnp.float32)
    half = TAIL // 2
    return state, [tail[h : h + 1, 0:1] + tail[half + h : half + h + 1, 0:1] for h in range(heads)]


def per_row(decays, rows, lanes):
    each = rows // len(decays)
    return jnp.concatenate([jnp.broadcast_to(d, (each, lanes)) for d in decays], axis=0)


def followed(earlier, later):
    (state_a, decay_a), (state_b, decay_b) = earlier, later
    state = state_a * per_row(decay_b, *state_a.shape) + state_b
    return state, [a * b for a, b in zip(decay_a, decay_b)]


def chosen(flag, one, other):
    return jnp.where(flag, one[0], other[0]), [
        jnp.where(flag, a, b) for a, b in zip(one[1], other[1])
    ]


def front_kernel(
    nz,
    nx,
    capacity,
    xs_ref,
    gate_ref,
    keys_ref,
    queries_ref,
    raw_ref,
    extra_ref,
    rate_ref,
    taps_x_ref,
    taps_k_ref,
    taps_q_ref,
    gain_ref,
    blend_hbm,
    carry_ref,
    gain2_ref,
    ids_ref,
    affinity_ref,
    chance_ref,
    outgoing_ref,
    middle_ref,
    weight_ref,
    halo,
    joined,
    pair_out,
    pair_in,
    quad_out,
    quad_in,
    far_out,
    far_in,
    half_out,
    half_in,
    gated_out,
    gated_in,
    facts,
    rows,
    blend,
    turned,
    blend_sem,
    halo_s,
    halo_r,
    pair_s,
    pair_r,
    quad_s,
    quad_r,
    far_s,
    far_r,
    gated_s,
    gated_r,
):
    z, c, x = lax.axis_index("sp_0"), lax.axis_index("sp_1"), lax.axis_index("tp")
    length, width_x = xs_ref.shape
    state_width = keys_ref.shape[1]
    heads = raw_ref.shape[0]
    head_dim = width_x // heads
    half_heads = heads // 2
    half_rows = width_x // 2
    place, quad = lax.rem(z, QUAD), z // QUAD
    quads = nz // QUAD
    f32, bf16 = jnp.float32, jnp.bfloat16
    partner = {"sp_1": 1 - c}
    load = pltpu.make_async_copy(blend_hbm, blend, blend_sem)
    load.start()

    stride_row = jnp.maximum(raw_ref[...], 0.0) + jnp.log1p(jnp.exp(-jnp.abs(raw_ref[...])))
    diagonal = lax.broadcasted_iota(jnp.int32, (heads, heads), 0) == lax.broadcasted_iota(
        jnp.int32, (heads, heads), 1
    )
    rate = jnp.sum(
        jnp.where(diagonal, jnp.broadcast_to(rate_ref[...], (heads, heads)), 0.0),
        axis=1,
        keepdims=True,
    )
    log_row = extra_ref[...] - rate * stride_row
    t_axis = lax.broadcasted_iota(jnp.int32, (length, length), 0)
    s_axis = lax.broadcasted_iota(jnp.int32, (length, length), 1)
    causal = t_axis >= s_axis
    running_row = exact_dot(
        jnp.concatenate([log_row, jnp.zeros_like(log_row)], axis=0), (t_axis <= s_axis).astype(f32)
    )
    picks = ids_ref.shape[0]
    count = ids_ref.shape[1] // nx
    lanes = 128
    stacked = jnp.concatenate(
        [
            running_row[:heads],
            stride_row,
            ids_ref[...].astype(f32),
            jnp.zeros((lanes - 2 * heads - picks, length), f32),
        ],
        axis=0,
    )
    turned[...] = stacked.T
    running = turned[:, :heads]
    stride = turned[:, heads : 2 * heads]
    final = running[length - 1 : length, :]
    lifted = jnp.exp(affinity_ref[...])
    share_row = chance_ref[...] * lifted / jnp.sum(lifted, axis=0, keepdims=True)
    share_row = jnp.concatenate([share_row, jnp.zeros((lanes - picks, count), f32)], axis=0)
    share_row = jnp.concatenate([share_row, jnp.zeros((lanes, lanes - count), f32)], axis=1)
    shares = share_row.T[:count]
    local_experts = outgoing_ref.shape[0]
    experts = nz * 2 * local_experts
    ids = turned[pl.ds(pl.multiple_of(x * count, count), count), :]
    ids = ids[:, 2 * heads : 2 * heads + picks].astype(jnp.int32)
    expert_axis = lax.broadcasted_iota(jnp.int32, (count, experts), 1)
    member = [(ids[:, k : k + 1] == expert_axis).astype(f32) for k in range(picks)]
    row_axis = lax.broadcasted_iota(jnp.int32, (count, count), 0)
    column_axis = lax.broadcasted_iota(jnp.int32, (count, count), 1)
    earlier = (row_axis > column_axis).astype(bf16)
    before = jnp.dot(earlier, sum(member).astype(bf16), preferred_element_type=f32)
    lane = lax.broadcasted_iota(jnp.int32, (count, facts.shape[2]), 1)
    noted = jnp.zeros((count, facts.shape[2]), f32)
    for k in range(picks):
        position = jnp.sum(before * member[k], axis=1, keepdims=True)
        expert = ids[:, k : k + 1]
        holder = lax.div(expert, local_experts)
        slot = (
            (lax.rem(expert, local_experts) * nz + lax.div(holder, 2)) * 2 + c
        ) * capacity + position.astype(jnp.int32)
        for core in range(2):
            there = jnp.where(lax.rem(holder, 2) == core, slot, -1).astype(f32)
            noted = jnp.where(lane == core * picks + k, there, noted)
        noted = jnp.where(lane == 2 * picks + k, shares[:, k : k + 1], noted)
    facts[c] = noted

    greet_all(nz, nx)
    rim = halo.shape[0]
    after = {"sp_0": lax.rem(z + c, nz), "sp_1": 1 - c}
    edges = []
    start = 0
    for n, ref in enumerate((xs_ref, keys_ref, queries_ref)):
        columns = pl.ds(start, ref.shape[1])
        edges.append(
            pltpu.make_async_remote_copy(
                ref.at[pl.ds(length - rim, rim)],
                halo.at[:, columns],
                halo_s.at[n],
                halo_r.at[n],
                device_id=after,
            )
        )
        start += ref.shape[1]
    for edge in edges:
        edge.start()
    facts_copy = pltpu.make_async_remote_copy(
        facts.at[c], facts.at[c], pair_s.at[0], pair_r.at[0], device_id=partner
    )
    facts_copy.start()

    start = 0
    for ref in (xs_ref, keys_ref, queries_ref):
        joined[rim:, start : start + ref.shape[1]] = ref[...].astype(f32)
        start += ref.shape[1]
    for edge in edges:
        edge.wait_recv()
    joined[:rim, :] = jnp.where(z + c > 0, halo[...].astype(f32), 0.0)
    taps = jnp.concatenate([taps_x_ref[...], taps_k_ref[...], taps_q_ref[...]], axis=1)
    kernel_len = taps.shape[0]
    convolved = taps[0:1, :] * joined[rim - kernel_len + 1 : rim - kernel_len + 1 + length, :]
    for tap in range(1, kernel_len):
        first = rim - kernel_len + 1 + tap
        convolved = convolved + taps[tap : tap + 1, :] * joined[first : first + length, :]
    convolved = silu(convolved)
    inputs_x = convolved[:, :width_x]
    keys_b = convolved[:, width_x : width_x + state_width].astype(bf16)
    queries_c = convolved[:, width_x + state_width :].astype(bf16)

    scaled = [
        inputs_x[:, h * head_dim : (h + 1) * head_dim] * stride[:, h : h + 1] for h in range(heads)
    ]
    remaining = jnp.concatenate(
        [scaled[h] * jnp.exp(final[:, h : h + 1] - running[:, h : h + 1]) for h in range(heads)],
        axis=1,
    ).astype(bf16)
    own_state = lax.dot_general(
        remaining, keys_b, (((0,), (0,)), ((), ())), preferred_element_type=f32
    )
    pair_out[...] = packed(own_state, [jnp.exp(final[:, h : h + 1]) for h in range(heads)])
    pair_copy = pltpu.make_async_remote_copy(
        pair_out, pair_in, pair_s.at[1], pair_r.at[1], device_id=partner
    )
    pair_copy.start()

    scores = lax.dot_general(
        queries_c, keys_b, (((1,), (1,)), ((), ())), preferred_element_type=f32
    )
    inside = []
    for h in range(heads):
        between = running[:, h : h + 1] - running_row[h : h + 1, :]
        decays = jnp.exp(jnp.where(causal, between, -1e30))
        inside.append(
            jnp.dot(
                (scores * decays).astype(bf16), scaled[h].astype(bf16), preferred_element_type=f32
            )
        )

    pair_copy.wait_recv()

    def half_of(ref):
        state, decays = unpacked(ref[...], heads)
        return (
            jnp.where(c == 0, state[:half_rows], state[half_rows:]),
            [jnp.where(c == 0, decays[j], decays[half_heads + j]) for j in range(half_heads)],
        )

    ours, theirs = half_of(pair_out), half_of(pair_in)
    lower, upper = chosen(c == 0, ours, theirs), chosen(c == 0, theirs, ours)
    chip = followed(lower, upper)
    quad_out[...] = packed(*chip)

    def quad_send(k):
        to = quad * QUAD + lax.rem(place + k, QUAD)
        return pltpu.make_async_remote_copy(
            quad_out, quad_in.at[place], quad_s.at[k], quad_r.at[k], device_id={"sp_0": to}
        )

    def quad_arrival(k):
        return pltpu.make_async_remote_copy(
            quad_out,
            quad_in.at[lax.rem(place + QUAD - k, QUAD)],
            quad_s.at[k],
            quad_r.at[k],
            device_id={"sp_0": lax.rem(z + 1, nz)},
        )

    for k in range(1, QUAD):
        quad_send(k).start()
    quad_in[place] = quad_out[...]
    for k in range(1, QUAD):
        quad_arrival(k).wait_recv()
    nothing = (jnp.zeros_like(chip[0]), [jnp.ones_like(d) for d in chip[1]])
    whole, inner = nothing, nothing
    for k in range(QUAD):
        inner = chosen(place == k, whole, inner)
        whole = followed(whole, unpacked(quad_in[k], half_heads))
    far_out[...] = packed(*whole)

    def far_send(k):
        return pltpu.make_async_remote_copy(
            far_out,
            far_in.at[k],
            far_s.at[k],
            far_r.at[k],
            device_id={"sp_0": lax.rem(z + k * QUAD, nz)},
        )

    for k in range(1, quads):

        @pl.when(quad + k < quads)
        def _(k=k):
            far_send(k).start()

    far_in[0] = jnp.zeros_like(far_out)
    for k in range(1, quads):

        @pl.when(quad >= k)
        def _(k=k):
            far_send(k).wait_recv()

        @pl.when(quad < k)
        def _(k=k):
            far_in[k] = jnp.zeros_like(far_out)

    incoming = nothing
    for k in reversed(range(1, quads)):
        incoming = followed(incoming, unpacked(far_in[k], half_heads))
    incoming = followed(incoming, inner)
    incoming_low = incoming[0]
    incoming_high = followed(incoming, lower)[0]
    half_out[...] = jnp.where(c == 0, incoming_high, incoming_low).astype(bf16)
    half_copy = pltpu.make_async_remote_copy(
        half_out, half_in, pair_s.at[2], pair_r.at[2], device_id=partner
    )
    half_copy.start()
    kept = jnp.where(c == 0, incoming_low, incoming_high).astype(bf16)
    modulation = silu(gate_ref[...].astype(f32))
    half_copy.wait_recv()
    sent_in = half_in[...]
    entering = jnp.concatenate(
        [jnp.where(c == 0, kept, sent_in), jnp.where(c == 0, sent_in, kept)], axis=0
    )
    outside = lax.dot_general(
        queries_c, entering, (((1,), (1,)), ((), ())), preferred_element_type=f32
    )
    mixed = jnp.concatenate(
        [
            inside[h]
            + outside[:, h * head_dim : (h + 1) * head_dim] * jnp.exp(running[:, h : h + 1])
            for h in range(heads)
        ],
        axis=1,
    )
    gated_out[...] = (mixed * modulation).astype(bf16).reshape(gated_out.shape)

    def gated_send(k):
        to = lax.rem(x + k, nx)
        return pltpu.make_async_remote_copy(
            gated_out.at[to], gated_in.at[x], gated_s.at[k], gated_r.at[k], device_id={"tp": to}
        )

    for k in range(1, nx):
        gated_send(k).start()
    gated_in[x] = gated_out[x]
    facts_arrival = pltpu.make_async_remote_copy(
        facts.at[1 - c], facts.at[1 - c], pair_s.at[0], pair_r.at[0], device_id=partner
    )
    facts_arrival.wait_recv()
    slot_count = weight_ref.shape[1]
    slot_axis = lax.broadcasted_iota(jnp.int32, (2 * count, slot_count), 1).astype(f32)
    known = jnp.concatenate([facts[0], facts[1]], axis=0)
    picked = jnp.zeros((2 * count, slot_count), f32)
    weight = jnp.zeros((2 * count, slot_count), f32)
    for k in range(picks):
        slot = jnp.where(c == 0, known[:, k : k + 1], known[:, picks + k : picks + k + 1])
        hit = slot == slot_axis
        picked = jnp.where(hit, 1.0, picked)
        weight = jnp.where(hit, known[:, 2 * picks + k : 2 * picks + k + 1], weight)
    weight_ref[...] = weight
    for k in range(1, nx):
        pltpu.make_async_remote_copy(
            gated_out.at[x],
            gated_in.at[lax.rem(x + nx - k, nx)],
            gated_s.at[k],
            gated_r.at[k],
            device_id={"tp": lax.rem(x + k, nx)},
        ).wait_recv()
    own_rows = jnp.concatenate([gated_in[k] for k in range(nx)], axis=1).astype(f32)
    normed = (
        own_rows
        * lax.rsqrt(jnp.mean(own_rows * own_rows, axis=1, keepdims=True) + EPS)
        * gain_ref[...]
    ).astype(bf16)
    load.wait()
    middle = (
        carry_ref[...].astype(f32) + jnp.dot(normed, blend[...], preferred_element_type=f32)
    ).astype(bf16)
    middle_ref[...] = middle
    wide = middle.astype(f32)
    rows[c] = (
        wide
        * lax.rsqrt(jnp.mean(wide * wide, axis=1, keepdims=True) + EPS)
        * gain2_ref[...]
    ).astype(bf16)
    rows_copy = pltpu.make_async_remote_copy(
        rows.at[c], rows.at[c], pair_s.at[3], pair_r.at[3], device_id=partner
    )
    rows_copy.start()
    pltpu.make_async_remote_copy(
        rows.at[1 - c], rows.at[1 - c], pair_s.at[3], pair_r.at[3], device_id=partner
    ).wait_recv()
    outgoing_ref[...] = (
        lax.dot_general(
            picked.astype(bf16),
            jnp.concatenate([rows[0], rows[1]], axis=0),
            (((0,), (0,)), ((), ())),
            preferred_element_type=f32,
        )
        .astype(bf16)
        .reshape(outgoing_ref.shape)
    )

    for edge in edges:
        edge.wait_send()
    facts_copy.wait_send()
    pair_copy.wait_send()
    half_copy.wait_send()
    rows_copy.wait_send()
    for k in range(1, QUAD):
        quad_send(k).wait_send()
    for k in range(1, quads):

        @pl.when(quad + k < quads)
        def _(k=k):
            far_send(k).wait_send()

    for k in range(1, nx):
        gated_send(k).wait_send()


def front(nz, nx, local_experts, capacity, *arrays):
    xs, _, keys, queries, raw = arrays[:5]
    blend, carry = arrays[11:13]
    count, width = carry.shape
    slots = local_experts * nz * 2 * capacity
    channels = xs.shape[1]
    total = channels + keys.shape[1] + queries.shape[1]
    rim = 8
    states = keys.shape[1]
    bf16 = jnp.bfloat16
    vmem = pl.BlockSpec(memory_space=pltpu.VMEM)
    half = channels // 2
    return pl.pallas_call(
        functools.partial(front_kernel, nz, nx, capacity),
        out_shape=(
            jax.ShapeDtypeStruct((local_experts, nz, 2 * capacity, width), bf16),
            jax.ShapeDtypeStruct((count, width), bf16),
            jax.ShapeDtypeStruct((2 * count, slots), jnp.float32),
        ),
        in_specs=[vmem] * 11 + [pl.BlockSpec(memory_space=pl.ANY)] + [vmem] * 5,
        out_specs=(vmem, vmem, vmem),
        scratch_shapes=[
            pltpu.VMEM((rim, total), bf16),
            pltpu.VMEM((rim + xs.shape[0], total), jnp.float32),
            pltpu.VMEM((channels + TAIL, states), bf16),
            pltpu.VMEM((channels + TAIL, states), bf16),
            pltpu.VMEM((half + TAIL, states), bf16),
            pltpu.VMEM((QUAD, half + TAIL, states), bf16),
            pltpu.VMEM((half + TAIL, states), bf16),
            pltpu.VMEM((nz // QUAD, half + TAIL, states), bf16),
            pltpu.VMEM((half, states), bf16),
            pltpu.VMEM((half, states), bf16),
            pltpu.VMEM((nx, count, channels), bf16),
            pltpu.VMEM((nx, count, channels), bf16),
            pltpu.VMEM((2, count, 128), jnp.float32),
            pltpu.VMEM((2, count, width), bf16),
            pltpu.VMEM(blend.shape, bf16),
            pltpu.VMEM((xs.shape[0], 128), jnp.float32),
            pltpu.SemaphoreType.DMA,
            pltpu.SemaphoreType.DMA((3,)),
            pltpu.SemaphoreType.DMA((3,)),
            pltpu.SemaphoreType.DMA((4,)),
            pltpu.SemaphoreType.DMA((4,)),
            pltpu.SemaphoreType.DMA((QUAD,)),
            pltpu.SemaphoreType.DMA((QUAD,)),
            pltpu.SemaphoreType.DMA((nz // QUAD,)),
            pltpu.SemaphoreType.DMA((nz // QUAD,)),
            pltpu.SemaphoreType.DMA((nx,)),
            pltpu.SemaphoreType.DMA((nx,)),
        ],
        compiler_params=pltpu.CompilerParams(collective_id=3, has_side_effects=True),
        name="front",
    )(*arrays)


def per_device(
    carryover_vector,
    channel_source_entries,
    final_modulation_vector,
    entering_basis_matrix,
    readout_basis_matrix,
    raw_stride_amount,
    extra_log_attenuation,
    channel_fading_rate,
    channel_source_kernel,
    entering_basis_kernel,
    readout_basis_kernel,
    modulated_rescaling_vector,
    blender_final_matrix,
    specialist_rescaling_vector,
    specialist_gating_matrices,
    widening_matrices,
    contracting_matrices,
    assigned_specialist_ids,
    specialist_choice_affinity,
    cluster_chance,
):
    nz, cores, nx = lax.axis_size("sp_0"), lax.axis_size("sp_1"), lax.axis_size("tp")
    row_count, model_width = carryover_vector.shape
    local_experts = specialist_gating_matrices.shape[0]
    experts = nz * cores * local_experts
    picks = assigned_specialist_ids.shape[1]
    capacity = 2 * row_count * picks // experts
    outgoing, middle, weight_of = front(
        nz,
        nx,
        local_experts,
        capacity,
        channel_source_entries,
        final_modulation_vector,
        entering_basis_matrix,
        readout_basis_matrix,
        raw_stride_amount.T,
        extra_log_attenuation.T,
        channel_fading_rate[None, :],
        channel_source_kernel,
        entering_basis_kernel,
        readout_basis_kernel,
        modulated_rescaling_vector[None, :],
        blender_final_matrix,
        carryover_vector,
        specialist_rescaling_vector[None, :],
        assigned_specialist_ids.T,
        specialist_choice_affinity.T,
        cluster_chance[None, :],
    )
    return routed(
        outgoing,
        specialist_gating_matrices,
        widening_matrices,
        contracting_matrices,
        middle,
        weight_of,
        nz,
        nx,
    )


def solution(mesh):
    finer = Mesh(
        mesh.devices.reshape(mesh.shape["grp"], mesh.shape["sp"] // 2, 2, mesh.shape["tp"]),
        ("grp", "sp_0", "sp_1", "tp"),
    )
    return jax.shard_map(
        per_device,
        mesh=finer,
        in_specs=(
            P(GRP_SP_TP, None),
            P(GRP_SP, "tp"),
            P(GRP_SP, "tp"),
            P(GRP_SP, "tp"),
            P(GRP_SP, "tp"),
            P(GRP_SP, "tp"),
            P(GRP_SP, "tp"),
            P("tp"),
            P(None, "tp"),
            P(None, "tp"),
            P(None, "tp"),
            P(),
            P(),
            P(),
            P(SP, None, "tp"),
            P(SP, None, "tp"),
            P(SP, "tp", None),
            P(GRP_SP, None),
            P(GRP_SP_TP, None),
            P(GRP_SP_TP),
        ),
        out_specs=P(GRP_SP_TP, None),
        check_vma=False,
    )
```

```python
import functools

import jax
import jax.numpy as jnp
from jax import lax
from jax.experimental import pallas as pl
from jax.experimental.pallas import tpu as pltpu
from jax.sharding import Mesh
from jax.sharding import PartitionSpec as P

SP = ("sp_0", "sp_1")
GRP_SP_TP = ("grp", "sp_0", "sp_1", "tp")
GRP_SP = ("grp", "sp_0", "sp_1")


EPS = 1e-06


NEAR = 4


def hop(step, nz):
    step = jnp.where(step > NEAR, nz + NEAR - step, step)
    half = (step + 1) // 2
    return jnp.where(step % 2 == 1, half, -half)


def greet(nz, nx):
    z, c, x = lax.axis_index("sp_0"), lax.axis_index("sp_1"), lax.axis_index("tp")
    barrier = pltpu.get_barrier_semaphore()

    def signal(k, carry):
        pl.semaphore_signal(barrier, inc=1, device_id={"sp_0": lax.rem(z + k, nz)})
        return carry

    lax.fori_loop(1, nz, signal, 0)
    pl.semaphore_signal(barrier, inc=1, device_id={"tp": lax.rem(x + 1, nx)})
    pl.semaphore_signal(barrier, inc=1, device_id={"tp": lax.rem(x + nx - 1, nx)})
    pl.semaphore_signal(barrier, inc=1, device_id={"sp_1": 1 - c})
    pl.semaphore_wait(barrier, nz + 2)


def experts_kernel(
    nz,
    nx,
    src,
    gates_hbm,
    ups_hbm,
    downs_hbm,
    middle_ref,
    weight_ref,
    out_ref,
    arrived,
    part,
    far,
    near,
    both,
    mine,
    total,
    answers,
    gates,
    ups,
    downs,
    given,
    taken,
    load_sem,
    here,
    zs,
    zr,
    xs,
    xr,
    os_,
    or_,
    fs,
    fr,
    ns,
    nr,
    bs,
    br,
    ts,
    tr,
    ps,
    pr,
):
    z, c, x = lax.axis_index("sp_0"), lax.axis_index("sp_1"), lax.axis_index("tp")
    xp, xm = lax.rem(x + 1, nx), lax.rem(x + nx - 1, nx)
    x2 = lax.rem(x + 2, nx)
    local_experts, _, rows, width = src.shape
    f32, bf16 = jnp.float32, jnp.bfloat16
    loads = [
        pltpu.make_async_copy(a, b, load_sem.at[n])
        for n, (a, b) in enumerate(((gates_hbm, gates), (ups_hbm, ups), (downs_hbm, downs)))
    ]
    for load in loads:
        load.start()
    greet(nz, nx)

    def goal(i):
        return lax.rem(z + hop(i, nz) + nz, nz)

    def origin(i):
        return lax.rem(z - hop(i, nz) + nz, nz)

    def ahead(i):
        return jnp.where(i % 2 == 0, xp, xm)

    def behind(i):
        return jnp.where(i % 2 == 0, xm, xp)

    def remote(a, b, sent, got, **to):
        return pltpu.make_async_remote_copy(a, b, sent, got, device_id=to)

    def along_z(i):
        return remote(src.at[:, goal(i)], arrived.at[i, :, x], zs.at[i], zr.at[i], sp_0=goal(i))

    def along_x(i, way):
        chunk = arrived.at[i, :, x]
        to = xp if way == 0 else xm
        return remote(chunk, chunk, xs.at[way, i], xr.at[way, i], tp=to)

    def from_x(i, way):
        chunk = arrived.at[i, :, jnp.where(way == 0, xm, xp)]
        return remote(chunk, chunk, xs.at[way, i], xr.at[way, i], tp=xp)

    def onward(i):
        chunk = arrived.at[i, :, behind(i)]
        return remote(chunk, chunk, os_.at[i], or_.at[i], tp=ahead(i))

    def from_far(i):
        chunk = arrived.at[i, :, x2]
        return remote(chunk, chunk, os_.at[i], or_.at[i], tp=xp)

    def send_far(i):
        return remote(part.at[i, :, x2], far.at[i], fs.at[i], fr.at[i], tp=ahead(i))

    def send_near(i):
        return remote(part.at[i, :, behind(i)], near.at[i], ns.at[i], nr.at[i], tp=behind(i))

    def send_both(i):
        return remote(mine.at[i], both.at[i], bs.at[i], br.at[i], tp=ahead(i))

    def send_back(i):
        return remote(total.at[i], answers.at[:, z], ts.at[i], tr.at[i], sp_0=origin(i))

    def send_z(i, carry):
        along_z(i).start()
        return carry

    lax.fori_loop(1, nz, send_z, 0)
    own = pltpu.make_async_copy(src.at[:, z], arrived.at[0, :, x], here.at[0])
    own.start()
    own.wait()

    def spread(i):
        along_x(i, 0).start()
        along_x(i, 1).start()

    def pass_on(i):
        from_x(i, i % 2).wait_recv()
        onward(i).start()

    def complete(i):
        from_x(i, (i + 1) % 2).wait_recv()
        from_far(i).wait_recv()

    def multiply(i):
        for e in range(local_experts):
            tokens = jnp.concatenate(
                [
                    arrived[i + k, e].astype(f32).reshape(nx * rows, width).astype(bf16)
                    for k in range(2)
                ],
                axis=0,
            )
            gate = jnp.dot(tokens, gates[e], preferred_element_type=f32)
            up = jnp.dot(tokens, ups[e], preferred_element_type=f32)
            hidden = (silu(gate) * up).astype(bf16)
            result = jnp.dot(hidden, downs[e], preferred_element_type=f32)
            for k in range(2):
                part[i + k, e] = (
                    result[k * nx * rows : (k + 1) * nx * rows].reshape(nx, rows, width).astype(bf16)
                )

    def first(i):
        send_far(i).start()
        send_near(i).start()

    def second(i):
        send_far(i).wait_recv()
        mine[i] = (part[i, :, ahead(i)].astype(f32) + far[i].astype(f32)).astype(bf16)
        send_both(i).start()

    def third(i):
        send_near(i).wait_recv()
        send_both(i).wait_recv()
        total[i] = (
            part[i, :, x].astype(f32) + near[i].astype(f32) + both[i].astype(f32)
        ).astype(bf16)

    pairs = nz // 2

    def turn(p, carry):
        i = 2 * p

        @pl.when(p == 0)
        def _():
            spread(0)

        @pl.when((p > 0) & (p < pairs))
        def _():
            remote(src.at[:, z], arrived.at[i, :, x], zs.at[i], zr.at[i], tp=xp).wait_recv()
            spread(i)

        @pl.when((p > 0) & (p <= pairs))
        def _():
            pass_on(i - 1)

        @pl.when(p < pairs)
        def _():
            remote(src.at[:, z], arrived.at[i + 1, :, x], zs.at[i + 1], zr.at[i + 1], tp=xp).wait_recv()
            spread(i + 1)
            pass_on(i)

        @pl.when(p == 1)
        def _():
            for load in loads:
                load.wait()

        @pl.when((p > 0) & (p <= pairs))
        def _():
            complete(i - 2)
            complete(i - 1)
            multiply(i - 2)
            first(i - 2)
            first(i - 1)

        @pl.when((p > 1) & (p <= pairs + 1))
        def _():
            second(i - 4)
            second(i - 3)

        @pl.when(p > 2)
        def _():
            third(i - 6)
            third(i - 5)

            @pl.when(p > 3)
            def _():
                send_back(i - 6).start()

            send_back(i - 5).start()

        return carry

    lax.fori_loop(0, pairs + 3, turn, 0)
    own_back = pltpu.make_async_copy(total.at[0], answers.at[:, z], here.at[1])
    own_back.start()
    own_back.wait()

    def sent(i, carry):
        along_x(i, 0).wait_send()
        along_x(i, 1).wait_send()
        onward(i).wait_send()
        send_far(i).wait_send()
        send_near(i).wait_send()
        send_both(i).wait_send()
        return carry

    lax.fori_loop(0, nz, sent, 0)

    def returned(i, carry):
        along_z(i).wait_send()
        send_back(i).wait_send()
        remote(total.at[i], answers.at[:, goal(i)], ts.at[i], tr.at[i], tp=xp).wait_recv()
        return carry

    lax.fori_loop(1, nz, returned, 0)

    count = out_ref.shape[0]
    slots = local_experts * nz * rows
    known = answers[...].astype(f32).reshape(slots, width).astype(bf16)

    def shared(start):
        weight = weight_ref[pl.ds(pl.multiple_of(start * count, count), count), :]
        high = weight.astype(bf16)
        low = (weight - high.astype(f32)).astype(bf16)
        return jnp.dot(high, known, preferred_element_type=f32) + jnp.dot(
            low, known, preferred_element_type=f32
        )

    given[...] = shared(1 - c)
    swap = remote(given, taken, ps, pr, sp_1=1 - c)
    swap.start()
    kept = middle_ref[...].astype(f32) + shared(c)
    swap.wait()
    out_ref[...] = (kept + taken[...]).astype(bf16)


def routed(outgoing, gates, ups, downs, middle, weight, nz, nx):
    experts, _, rows, width = outgoing.shape
    bf16 = jnp.bfloat16
    slots = pltpu.VMEM((nz, experts, rows, width), bf16)
    wide = pltpu.VMEM((nz, experts, nx, rows, width), bf16)
    count = middle.shape[0]
    vmem = pl.BlockSpec(memory_space=pltpu.VMEM)
    anywhere = pl.BlockSpec(memory_space=pl.ANY)
    line = pltpu.SemaphoreType.DMA((nz,))
    return pl.pallas_call(
        functools.partial(experts_kernel, nz, nx),
        out_shape=jax.ShapeDtypeStruct((count, width), bf16),
        in_specs=[vmem, anywhere, anywhere, anywhere, vmem, vmem],
        out_specs=vmem,
        scratch_shapes=[wide, wide, slots, slots, slots, slots, slots]
        + [pltpu.VMEM((experts, nz, rows, width), bf16)]
        + [pltpu.VMEM(w.shape, bf16) for w in (gates, ups, downs)]
        + [pltpu.VMEM((count, width), jnp.float32)] * 2
        + [pltpu.SemaphoreType.DMA((3,)), pltpu.SemaphoreType.DMA((2,))]
        + [line, line]
        + [pltpu.SemaphoreType.DMA((2, nz))] * 2
        + [line] * 10
        + [pltpu.SemaphoreType.DMA] * 2,
        compiler_params=pltpu.CompilerParams(
            collective_id=1, has_side_effects=True, vmem_limit_bytes=60 << 20
        ),
        name="experts",
    )(outgoing, gates, ups, downs, middle, weight)


QUAD = 4
TAIL = 16


def greet_all(nz, nx):
    z, c, x = lax.axis_index("sp_0"), lax.axis_index("sp_1"), lax.axis_index("tp")
    barrier = pltpu.get_barrier_semaphore()

    def along_z(k, carry):
        pl.semaphore_signal(barrier, inc=1, device_id={"sp_0": lax.rem(z + k, nz)})
        return carry

    def along_x(k, carry):
        pl.semaphore_signal(barrier, inc=1, device_id={"tp": lax.rem(x + k, nx)})
        return carry

    lax.fori_loop(1, nz, along_z, 0)
    lax.fori_loop(1, nx, along_x, 0)
    pl.semaphore_signal(barrier, inc=1, device_id={"sp_1": 1 - c})
    pl.semaphore_signal(
        barrier, inc=1, device_id={"sp_0": lax.rem(z + nz - 1 + 2 * c, nz), "sp_1": 1 - c}
    )
    pl.semaphore_wait(barrier, nz + nx)


def silu(v):
    return v * jax.nn.sigmoid(v)


def exact_dot(a, b):
    return jnp.dot(a, b, preferred_element_type=jnp.float32, precision=lax.Precision.HIGHEST)


def packed(state, decays):
    lanes = state.shape[1]
    row = lax.broadcasted_iota(jnp.int32, (TAIL, lanes), 0)
    tail = jnp.zeros((TAIL, lanes), jnp.float32)
    for h, decay in enumerate(decays):
        wide = jnp.broadcast_to(decay, (TAIL, lanes))
        high = wide.astype(jnp.bfloat16).astype(jnp.float32)
        tail = jnp.where(row == h, high, tail)
        tail = jnp.where(row == TAIL // 2 + h, wide - high, tail)
    return jnp.concatenate([state.astype(jnp.bfloat16), tail.astype(jnp.bfloat16)], axis=0)


def unpacked(message, heads):
    rows = message.shape[0] - TAIL
    state = message[:rows].astype(jnp.float32)
    tail = message[rows:].astype(jnp.float32)
    half = TAIL // 2
    return state, [tail[h : h + 1, 0:1] + tail[half + h : half + h + 1, 0:1] for h in range(heads)]


def per_row(decays, rows, lanes):
    each = rows // len(decays)
    return jnp.concatenate([jnp.broadcast_to(d, (each, lanes)) for d in decays], axis=0)


def followed(earlier, later):
    (state_a, decay_a), (state_b, decay_b) = earlier, later
    state = state_a * per_row(decay_b, *state_a.shape) + state_b
    return state, [a * b for a, b in zip(decay_a, decay_b)]


def chosen(flag, one, other):
    return jnp.where(flag, one[0], other[0]), [
        jnp.where(flag, a, b) for a, b in zip(one[1], other[1])
    ]


def front_kernel(
    nz,
    nx,
    capacity,
    xs_ref,
    gate_ref,
    keys_ref,
    queries_ref,
    raw_ref,
    extra_ref,
    rate_ref,
    taps_x_ref,
    taps_k_ref,
    taps_q_ref,
    gain_ref,
    blend_hbm,
    carry_ref,
    gain2_ref,
    ids_ref,
    affinity_ref,
    chance_ref,
    outgoing_ref,
    middle_ref,
    weight_ref,
    halo,
    joined,
    pair_out,
    pair_in,
    quad_out,
    quad_in,
    far_out,
    far_in,
    half_out,
    half_in,
    gated_out,
    gated_in,
    facts,
    rows,
    blend,
    turned,
    blend_sem,
    halo_s,
    halo_r,
    pair_s,
    pair_r,
    quad_s,
    quad_r,
    far_s,
    far_r,
    gated_s,
    gated_r,
):
    z, c, x = lax.axis_index("sp_0"), lax.axis_index("sp_1"), lax.axis_index("tp")
    length, width_x = xs_ref.shape
    state_width = keys_ref.shape[1]
    heads = raw_ref.shape[0]
    head_dim = width_x // heads
    half_heads = heads // 2
    half_rows = width_x // 2
    place, quad = lax.rem(z, QUAD), z // QUAD
    quads = nz // QUAD
    f32, bf16 = jnp.float32, jnp.bfloat16
    partner = {"sp_1": 1 - c}
    load = pltpu.make_async_copy(blend_hbm, blend, blend_sem)
    load.start()

    stride_row = jnp.maximum(raw_ref[...], 0.0) + jnp.log1p(jnp.exp(-jnp.abs(raw_ref[...])))
    diagonal = lax.broadcasted_iota(jnp.int32, (heads, heads), 0) == lax.broadcasted_iota(
        jnp.int32, (heads, heads), 1
    )
    rate = jnp.sum(
        jnp.where(diagonal, jnp.broadcast_to(rate_ref[...], (heads, heads)), 0.0),
        axis=1,
        keepdims=True,
    )
    log_row = extra_ref[...] - rate * stride_row
    t_axis = lax.broadcasted_iota(jnp.int32, (length, length), 0)
    s_axis = lax.broadcasted_iota(jnp.int32, (length, length), 1)
    causal = t_axis >= s_axis
    running_row = exact_dot(
        jnp.concatenate([log_row, jnp.zeros_like(log_row)], axis=0), (t_axis <= s_axis).astype(f32)
    )
    picks = ids_ref.shape[0]
    count = ids_ref.shape[1] // nx
    lanes = 128
    stacked = jnp.concatenate(
        [
            running_row[:heads],
            stride_row,
            ids_ref[...].astype(f32),
            jnp.zeros((lanes - 2 * heads - picks, length), f32),
        ],
        axis=0,
    )
    turned[...] = stacked.T
    running = turned[:, :heads]
    stride = turned[:, heads : 2 * heads]
    final = running[length - 1 : length, :]
    lifted = jnp.exp(affinity_ref[...])
    share_row = chance_ref[...] * lifted / jnp.sum(lifted, axis=0, keepdims=True)
    share_row = jnp.concatenate([share_row, jnp.zeros((lanes - picks, count), f32)], axis=0)
    share_row = jnp.concatenate([share_row, jnp.zeros((lanes, lanes - count), f32)], axis=1)
    shares = share_row.T[:count]
    local_experts = outgoing_ref.shape[0]
    experts = nz * 2 * local_experts
    ids = turned[pl.ds(pl.multiple_of(x * count, count), count), :]
    ids = ids[:, 2 * heads : 2 * heads + picks].astype(jnp.int32)
    expert_axis = lax.broadcasted_iota(jnp.int32, (count, experts), 1)
    member = [(ids[:, k : k + 1] == expert_axis).astype(f32) for k in range(picks)]
    row_axis = lax.broadcasted_iota(jnp.int32, (count, count), 0)
    column_axis = lax.broadcasted_iota(jnp.int32, (count, count), 1)
    earlier = (row_axis > column_axis).astype(bf16)
    before = jnp.dot(earlier, sum(member).astype(bf16), preferred_element_type=f32)
    lane = lax.broadcasted_iota(jnp.int32, (count, facts.shape[2]), 1)
    noted = jnp.zeros((count, facts.shape[2]), f32)
    for k in range(picks):
        position = jnp.sum(before * member[k], axis=1, keepdims=True)
        expert = ids[:, k : k + 1]
        holder = lax.div(expert, local_experts)
        slot = (
            (lax.rem(expert, local_experts) * nz + lax.div(holder, 2)) * 2 + c
        ) * capacity + position.astype(jnp.int32)
        for core in range(2):
            there = jnp.where(lax.rem(holder, 2) == core, slot, -1).astype(f32)
            noted = jnp.where(lane == core * picks + k, there, noted)
        noted = jnp.where(lane == 2 * picks + k, shares[:, k : k + 1], noted)
    facts[c] = noted

    greet_all(nz, nx)
    rim = halo.shape[0]
    after = {"sp_0": lax.rem(z + c, nz), "sp_1": 1 - c}
    edges = []
    start = 0
    for n, ref in enumerate((xs_ref, keys_ref, queries_ref)):
        columns = pl.ds(start, ref.shape[1])
        edges.append(
            pltpu.make_async_remote_copy(
                ref.at[pl.ds(length - rim, rim)],
                halo.at[:, columns],
                halo_s.at[n],
                halo_r.at[n],
                device_id=after,
            )
        )
        start += ref.shape[1]
    for edge in edges:
        edge.start()
    facts_copy = pltpu.make_async_remote_copy(
        facts.at[c], facts.at[c], pair_s.at[0], pair_r.at[0], device_id=partner
    )
    facts_copy.start()

    start = 0
    for ref in (xs_ref, keys_ref, queries_ref):
        joined[rim:, start : start + ref.shape[1]] = ref[...].astype(f32)
        start += ref.shape[1]
    for edge in edges:
        edge.wait_recv()
    joined[:rim, :] = jnp.where(z + c > 0, halo[...].astype(f32), 0.0)
    taps = jnp.concatenate([taps_x_ref[...], taps_k_ref[...], taps_q_ref[...]], axis=1)
    kernel_len = taps.shape[0]
    convolved = taps[0:1, :] * joined[rim - kernel_len + 1 : rim - kernel_len + 1 + length, :]
    for tap in range(1, kernel_len):
        first = rim - kernel_len + 1 + tap
        convolved = convolved + taps[tap : tap + 1, :] * joined[first : first + length, :]
    convolved = silu(convolved)
    inputs_x = convolved[:, :width_x]
    keys_b = convolved[:, width_x : width_x + state_width].astype(bf16)
    queries_c = convolved[:, width_x + state_width :].astype(bf16)

    scaled = [
        inputs_x[:, h * head_dim : (h + 1) * head_dim] * stride[:, h : h + 1] for h in range(heads)
    ]
    remaining = jnp.concatenate(
        [scaled[h] * jnp.exp(final[:, h : h + 1] - running[:, h : h + 1]) for h in range(heads)],
        axis=1,
    ).astype(bf16)
    own_state = lax.dot_general(
        remaining, keys_b, (((0,), (0,)), ((), ())), preferred_element_type=f32
    )
    pair_out[...] = packed(own_state, [jnp.exp(final[:, h : h + 1]) for h in range(heads)])
    pair_copy = pltpu.make_async_remote_copy(
        pair_out, pair_in, pair_s.at[1], pair_r.at[1], device_id=partner
    )
    pair_copy.start()

    scores = lax.dot_general(
        queries_c, keys_b, (((1,), (1,)), ((), ())), preferred_element_type=f32
    )
    inside = []
    for h in range(heads):
        between = running[:, h : h + 1] - running_row[h : h + 1, :]
        decays = jnp.exp(jnp.where(causal, between, -1e30))
        inside.append(
            jnp.dot(
                (scores * decays).astype(bf16), scaled[h].astype(bf16), preferred_element_type=f32
            )
        )

    pair_copy.wait_recv()

    def half_of(ref):
        state, decays = unpacked(ref[...], heads)
        return (
            jnp.where(c == 0, state[:half_rows], state[half_rows:]),
            [jnp.where(c == 0, decays[j], decays[half_heads + j]) for j in range(half_heads)],
        )

    ours, theirs = half_of(pair_out), half_of(pair_in)
    lower, upper = chosen(c == 0, ours, theirs), chosen(c == 0, theirs, ours)
    chip = followed(lower, upper)
    quad_out[...] = packed(*chip)

    def quad_send(k):
        to = quad * QUAD + lax.rem(place + k, QUAD)
        return pltpu.make_async_remote_copy(
            quad_out, quad_in.at[place], quad_s.at[k], quad_r.at[k], device_id={"sp_0": to}
        )

    def quad_arrival(k):
        return pltpu.make_async_remote_copy(
            quad_out,
            quad_in.at[lax.rem(place + QUAD - k, QUAD)],
            quad_s.at[k],
            quad_r.at[k],
            device_id={"sp_0": lax.rem(z + 1, nz)},
        )

    for k in range(1, QUAD):
        quad_send(k).start()
    quad_in[place] = quad_out[...]
    for k in range(1, QUAD):
        quad_arrival(k).wait_recv()
    nothing = (jnp.zeros_like(chip[0]), [jnp.ones_like(d) for d in chip[1]])
    whole, inner = nothing, nothing
    for k in range(QUAD):
        inner = chosen(place == k, whole, inner)
        whole = followed(whole, unpacked(quad_in[k], half_heads))
    far_out[...] = packed(*whole)

    def far_send(k):
        return pltpu.make_async_remote_copy(
            far_out,
            far_in.at[k],
            far_s.at[k],
            far_r.at[k],
            device_id={"sp_0": lax.rem(z + k * QUAD, nz)},
        )

    for k in range(1, quads):

        @pl.when(quad + k < quads)
        def _(k=k):
            far_send(k).start()

    far_in[0] = jnp.zeros_like(far_out)
    for k in range(1, quads):

        @pl.when(quad >= k)
        def _(k=k):
            far_send(k).wait_recv()

        @pl.when(quad < k)
        def _(k=k):
            far_in[k] = jnp.zeros_like(far_out)

    incoming = nothing
    for k in reversed(range(1, quads)):
        incoming = followed(incoming, unpacked(far_in[k], half_heads))
    incoming = followed(incoming, inner)
    incoming_low = incoming[0]
    incoming_high = followed(incoming, lower)[0]
    half_out[...] = jnp.where(c == 0, incoming_high, incoming_low).astype(bf16)
    half_copy = pltpu.make_async_remote_copy(
        half_out, half_in, pair_s.at[2], pair_r.at[2], device_id=partner
    )
    half_copy.start()
    kept = jnp.where(c == 0, incoming_low, incoming_high).astype(bf16)
    modulation = silu(gate_ref[...].astype(f32))
    half_copy.wait_recv()
    sent_in = half_in[...]
    entering = jnp.concatenate(
        [jnp.where(c == 0, kept, sent_in), jnp.where(c == 0, sent_in, kept)], axis=0
    )
    outside = lax.dot_general(
        queries_c, entering, (((1,), (1,)), ((), ())), preferred_element_type=f32
    )
    mixed = jnp.concatenate(
        [
            inside[h]
            + outside[:, h * head_dim : (h + 1) * head_dim] * jnp.exp(running[:, h : h + 1])
            for h in range(heads)
        ],
        axis=1,
    )
    gated_out[...] = (mixed * modulation).astype(bf16).reshape(gated_out.shape)

    def gated_send(k):
        to = lax.rem(x + k, nx)
        return pltpu.make_async_remote_copy(
            gated_out.at[to], gated_in.at[x], gated_s.at[k], gated_r.at[k], device_id={"tp": to}
        )

    for k in range(1, nx):
        gated_send(k).start()
    gated_in[x] = gated_out[x]
    facts_arrival = pltpu.make_async_remote_copy(
        facts.at[1 - c], facts.at[1 - c], pair_s.at[0], pair_r.at[0], device_id=partner
    )
    facts_arrival.wait_recv()
    slot_count = weight_ref.shape[1]
    slot_axis = lax.broadcasted_iota(jnp.int32, (2 * count, slot_count), 1).astype(f32)
    known = jnp.concatenate([facts[0], facts[1]], axis=0)
    picked = jnp.zeros((2 * count, slot_count), f32)
    weight = jnp.zeros((2 * count, slot_count), f32)
    for k in range(picks):
        slot = jnp.where(c == 0, known[:, k : k + 1], known[:, picks + k : picks + k + 1])
        hit = slot == slot_axis
        picked = jnp.where(hit, 1.0, picked)
        weight = jnp.where(hit, known[:, 2 * picks + k : 2 * picks + k + 1], weight)
    weight_ref[...] = weight
    for k in range(1, nx):
        pltpu.make_async_remote_copy(
            gated_out.at[x],
            gated_in.at[lax.rem(x + nx - k, nx)],
            gated_s.at[k],
            gated_r.at[k],
            device_id={"tp": lax.rem(x + k, nx)},
        ).wait_recv()
    own_rows = jnp.concatenate([gated_in[k] for k in range(nx)], axis=1).astype(f32)
    normed = (
        own_rows
        * lax.rsqrt(jnp.mean(own_rows * own_rows, axis=1, keepdims=True) + EPS)
        * gain_ref[...]
    ).astype(bf16)
    load.wait()
    middle = (
        carry_ref[...].astype(f32) + jnp.dot(normed, blend[...], preferred_element_type=f32)
    ).astype(bf16)
    middle_ref[...] = middle
    wide = middle.astype(f32)
    rows[c] = (
        wide
        * lax.rsqrt(jnp.mean(wide * wide, axis=1, keepdims=True) + EPS)
        * gain2_ref[...]
    ).astype(bf16)
    rows_copy = pltpu.make_async_remote_copy(
        rows.at[c], rows.at[c], pair_s.at[3], pair_r.at[3], device_id=partner
    )
    rows_copy.start()
    pltpu.make_async_remote_copy(
        rows.at[1 - c], rows.at[1 - c], pair_s.at[3], pair_r.at[3], device_id=partner
    ).wait_recv()
    outgoing_ref[...] = (
        lax.dot_general(
            picked.astype(bf16),
            jnp.concatenate([rows[0], rows[1]], axis=0),
            (((0,), (0,)), ((), ())),
            preferred_element_type=f32,
        )
        .astype(bf16)
        .reshape(outgoing_ref.shape)
    )

    for edge in edges:
        edge.wait_send()
    facts_copy.wait_send()
    pair_copy.wait_send()
    half_copy.wait_send()
    rows_copy.wait_send()
    for k in range(1, QUAD):
        quad_send(k).wait_send()
    for k in range(1, quads):

        @pl.when(quad + k < quads)
        def _(k=k):
            far_send(k).wait_send()

    for k in range(1, nx):
        gated_send(k).wait_send()


def front(nz, nx, local_experts, capacity, *arrays):
    xs, _, keys, queries, raw = arrays[:5]
    blend, carry = arrays[11:13]
    count, width = carry.shape
    slots = local_experts * nz * 2 * capacity
    channels = xs.shape[1]
    total = channels + keys.shape[1] + queries.shape[1]
    rim = 8
    states = keys.shape[1]
    bf16 = jnp.bfloat16
    vmem = pl.BlockSpec(memory_space=pltpu.VMEM)
    half = channels // 2
    return pl.pallas_call(
        functools.partial(front_kernel, nz, nx, capacity),
        out_shape=(
            jax.ShapeDtypeStruct((local_experts, nz, 2 * capacity, width), bf16),
            jax.ShapeDtypeStruct((count, width), bf16),
            jax.ShapeDtypeStruct((2 * count, slots), jnp.float32),
        ),
        in_specs=[vmem] * 11 + [pl.BlockSpec(memory_space=pl.ANY)] + [vmem] * 5,
        out_specs=(vmem, vmem, vmem),
        scratch_shapes=[
            pltpu.VMEM((rim, total), bf16),
            pltpu.VMEM((rim + xs.shape[0], total), jnp.float32),
            pltpu.VMEM((channels + TAIL, states), bf16),
            pltpu.VMEM((channels + TAIL, states), bf16),
            pltpu.VMEM((half + TAIL, states), bf16),
            pltpu.VMEM((QUAD, half + TAIL, states), bf16),
            pltpu.VMEM((half + TAIL, states), bf16),
            pltpu.VMEM((nz // QUAD, half + TAIL, states), bf16),
            pltpu.VMEM((half, states), bf16),
            pltpu.VMEM((half, states), bf16),
            pltpu.VMEM((nx, count, channels), bf16),
            pltpu.VMEM((nx, count, channels), bf16),
            pltpu.VMEM((2, count, 128), jnp.float32),
            pltpu.VMEM((2, count, width), bf16),
            pltpu.VMEM(blend.shape, bf16),
            pltpu.VMEM((xs.shape[0], 128), jnp.float32),
            pltpu.SemaphoreType.DMA,
            pltpu.SemaphoreType.DMA((3,)),
            pltpu.SemaphoreType.DMA((3,)),
            pltpu.SemaphoreType.DMA((4,)),
            pltpu.SemaphoreType.DMA((4,)),
            pltpu.SemaphoreType.DMA((QUAD,)),
            pltpu.SemaphoreType.DMA((QUAD,)),
            pltpu.SemaphoreType.DMA((nz // QUAD,)),
            pltpu.SemaphoreType.DMA((nz // QUAD,)),
            pltpu.SemaphoreType.DMA((nx,)),
            pltpu.SemaphoreType.DMA((nx,)),
        ],
        compiler_params=pltpu.CompilerParams(collective_id=3, has_side_effects=True),
        name="front",
    )(*arrays)


def per_device(
    carryover_vector,
    channel_source_entries,
    final_modulation_vector,
    entering_basis_matrix,
    readout_basis_matrix,
    raw_stride_amount,
    extra_log_attenuation,
    channel_fading_rate,
    channel_source_kernel,
    entering_basis_kernel,
    readout_basis_kernel,
    modulated_rescaling_vector,
    blender_final_matrix,
    specialist_rescaling_vector,
    specialist_gating_matrices,
    widening_matrices,
    contracting_matrices,
    assigned_specialist_ids,
    specialist_choice_affinity,
    cluster_chance,
):
    nz, cores, nx = lax.axis_size("sp_0"), lax.axis_size("sp_1"), lax.axis_size("tp")
    row_count, model_width = carryover_vector.shape
    local_experts = specialist_gating_matrices.shape[0]
    experts = nz * cores * local_experts
    picks = assigned_specialist_ids.shape[1]
    capacity = 2 * row_count * picks // experts
    outgoing, middle, weight_of = front(
        nz,
        nx,
        local_experts,
        capacity,
        channel_source_entries,
        final_modulation_vector,
        entering_basis_matrix,
        readout_basis_matrix,
        raw_stride_amount.T,
        extra_log_attenuation.T,
        channel_fading_rate[None, :],
        channel_source_kernel,
        entering_basis_kernel,
        readout_basis_kernel,
        modulated_rescaling_vector[None, :],
        blender_final_matrix,
        carryover_vector,
        specialist_rescaling_vector[None, :],
        assigned_specialist_ids.T,
        specialist_choice_affinity.T,
        cluster_chance[None, :],
    )
    return routed(
        outgoing,
        specialist_gating_matrices,
        widening_matrices,
        contracting_matrices,
        middle,
        weight_of,
        nz,
        nx,
    )


def solution(mesh):
    finer = Mesh(
        mesh.devices.reshape(mesh.shape["grp"], mesh.shape["sp"] // 2, 2, mesh.shape["tp"]),
        ("grp", "sp_0", "sp_1", "tp"),
    )
    return jax.shard_map(
        per_device,
        mesh=finer,
        in_specs=(
            P(GRP_SP_TP, None),
            P(GRP_SP, "tp"),
            P(GRP_SP, "tp"),
            P(GRP_SP, "tp"),
            P(GRP_SP, "tp"),
            P(GRP_SP, "tp"),
            P(GRP_SP, "tp"),
            P("tp"),
            P(None, "tp"),
            P(None, "tp"),
            P(None, "tp"),
            P(),
            P(),
            P(),
            P(SP, None, "tp"),
            P(SP, None, "tp"),
            P(SP, "tp", None),
            P(GRP_SP, None),
            P(GRP_SP_TP, None),
            P(GRP_SP_TP),
        ),
        out_specs=P(GRP_SP_TP, None),
        check_vma=False,
    )
```

```python
import functools

import jax
import jax.numpy as jnp
from jax import lax
from jax.experimental import pallas as pl
from jax.experimental.pallas import tpu as pltpu
from jax.sharding import Mesh
from jax.sharding import PartitionSpec as P

SP = ("sp_0", "sp_1")
GRP_SP_TP = ("grp", "sp_0", "sp_1", "tp")
GRP_SP = ("grp", "sp_0", "sp_1")


EPS = 1e-06


NEAR = 4


def hop(step, nz):
    step = jnp.where(step > NEAR, nz + NEAR - step, step)
    half = (step + 1) // 2
    return jnp.where(step % 2 == 1, half, -half)


def experts_kernel(
    nz,
    nx,
    src,
    gates_hbm,
    ups_hbm,
    downs_hbm,
    middle_ref,
    weight_ref,
    out_ref,
    arrived,
    part,
    far,
    near,
    both,
    mine,
    total,
    answers,
    gates,
    ups,
    downs,
    given,
    taken,
    load_sem,
    here,
    zs,
    zr,
    xs,
    xr,
    os_,
    or_,
    fs,
    fr,
    ns,
    nr,
    bs,
    br,
    ts,
    tr,
    ps,
    pr,
):
    z, c, x = lax.axis_index("sp_0"), lax.axis_index("sp_1"), lax.axis_index("tp")
    xp, xm = lax.rem(x + 1, nx), lax.rem(x + nx - 1, nx)
    x2 = lax.rem(x + 2, nx)
    local_experts, _, rows, width = src.shape
    f32, bf16 = jnp.float32, jnp.bfloat16
    loads = [
        pltpu.make_async_copy(a, b, load_sem.at[n])
        for n, (a, b) in enumerate(((gates_hbm, gates), (ups_hbm, ups), (downs_hbm, downs)))
    ]
    for load in loads:
        load.start()

    def goal(i):
        return lax.rem(z + hop(i, nz) + nz, nz)

    def origin(i):
        return lax.rem(z - hop(i, nz) + nz, nz)

    def ahead(i):
        return jnp.where(i % 2 == 0, xp, xm)

    def behind(i):
        return jnp.where(i % 2 == 0, xm, xp)

    def remote(a, b, sent, got, **to):
        return pltpu.make_async_remote_copy(a, b, sent, got, device_id=to)

    def along_z(i):
        return remote(src.at[:, goal(i)], arrived.at[i, :, x], zs.at[i], zr.at[i], sp_0=goal(i))

    def along_x(i, way):
        chunk = arrived.at[i, :, x]
        to = xp if way == 0 else xm
        return remote(chunk, chunk, xs.at[way, i], xr.at[way, i], tp=to)

    def from_x(i, way):
        chunk = arrived.at[i, :, jnp.where(way == 0, xm, xp)]
        return remote(chunk, chunk, xs.at[way, i], xr.at[way, i], tp=xp)

    def onward(i):
        chunk = arrived.at[i, :, behind(i)]
        return remote(chunk, chunk, os_.at[i], or_.at[i], tp=ahead(i))

    def from_far(i):
        chunk = arrived.at[i, :, x2]
        return remote(chunk, chunk, os_.at[i], or_.at[i], tp=xp)

    def send_far(i):
        return remote(part.at[i, :, x2], far.at[i], fs.at[i], fr.at[i], tp=ahead(i))

    def send_near(i):
        return remote(part.at[i, :, behind(i)], near.at[i], ns.at[i], nr.at[i], tp=behind(i))

    def send_both(i):
        return remote(mine.at[i], both.at[i], bs.at[i], br.at[i], tp=ahead(i))

    def send_back(i):
        return remote(total.at[i], answers.at[:, z], ts.at[i], tr.at[i], sp_0=origin(i))

    def send_z(i, carry):
        along_z(i).start()
        return carry

    lax.fori_loop(1, nz, send_z, 0)
    own = pltpu.make_async_copy(src.at[:, z], arrived.at[0, :, x], here.at[0])
    own.start()
    own.wait()

    def spread(i):
        along_x(i, 0).start()
        along_x(i, 1).start()

    def pass_on(i):
        from_x(i, i % 2).wait_recv()
        onward(i).start()

    def complete(i):
        from_x(i, (i + 1) % 2).wait_recv()
        from_far(i).wait_recv()

    def multiply(i):
        for e in range(local_experts):
            tokens = jnp.concatenate(
                [
                    arrived[i + k, e].astype(f32).reshape(nx * rows, width).astype(bf16)
                    for k in range(2)
                ],
                axis=0,
            )
            gate = jnp.dot(tokens, gates[e], preferred_element_type=f32)
            up = jnp.dot(tokens, ups[e], preferred_element_type=f32)
            hidden = (silu(gate) * up).astype(bf16)
            result = jnp.dot(hidden, downs[e], preferred_element_type=f32)
            for k in range(2):
                part[i + k, e] = (
                    result[k * nx * rows : (k + 1) * nx * rows].reshape(nx, rows, width).astype(bf16)
                )

    def first(i):
        send_far(i).start()
        send_near(i).start()

    def second(i):
        send_far(i).wait_recv()
        mine[i] = (part[i, :, ahead(i)].astype(f32) + far[i].astype(f32)).astype(bf16)
        send_both(i).start()

    def third(i):
        send_near(i).wait_recv()
        send_both(i).wait_recv()
        total[i] = (
            part[i, :, x].astype(f32) + near[i].astype(f32) + both[i].astype(f32)
        ).astype(bf16)

    pairs = nz // 2

    def turn(p, carry):
        i = 2 * p

        @pl.when(p == 0)
        def _():
            spread(0)

        @pl.when((p > 0) & (p < pairs))
        def _():
            remote(src.at[:, z], arrived.at[i, :, x], zs.at[i], zr.at[i], tp=xp).wait_recv()
            spread(i)

        @pl.when((p > 0) & (p <= pairs))
        def _():
            pass_on(i - 1)

        @pl.when(p < pairs)
        def _():
            remote(src.at[:, z], arrived.at[i + 1, :, x], zs.at[i + 1], zr.at[i + 1], tp=xp).wait_recv()
            spread(i + 1)
            pass_on(i)

        @pl.when(p == 1)
        def _():
            for load in loads:
                load.wait()

        @pl.when((p > 0) & (p <= pairs))
        def _():
            complete(i - 2)
            complete(i - 1)
            multiply(i - 2)
            first(i - 2)
            first(i - 1)

        @pl.when((p > 1) & (p <= pairs + 1))
        def _():
            second(i - 4)
            second(i - 3)

        @pl.when(p > 2)
        def _():
            third(i - 6)
            third(i - 5)

            @pl.when(p > 3)
            def _():
                send_back(i - 6).start()

            send_back(i - 5).start()

        return carry

    lax.fori_loop(0, pairs + 3, turn, 0)
    own_back = pltpu.make_async_copy(total.at[0], answers.at[:, z], here.at[1])
    own_back.start()
    own_back.wait()

    def sent(i, carry):
        along_x(i, 0).wait_send()
        along_x(i, 1).wait_send()
        onward(i).wait_send()
        send_far(i).wait_send()
        send_near(i).wait_send()
        send_both(i).wait_send()
        return carry

    lax.fori_loop(0, nz, sent, 0)

    def returned(i, carry):
        along_z(i).wait_send()
        send_back(i).wait_send()
        remote(total.at[i], answers.at[:, goal(i)], ts.at[i], tr.at[i], tp=xp).wait_recv()
        return carry

    lax.fori_loop(1, nz, returned, 0)

    count = out_ref.shape[0]
    slots = local_experts * nz * rows
    known = answers[...].astype(f32).reshape(slots, width).astype(bf16)

    def shared(start):
        weight = weight_ref[pl.ds(pl.multiple_of(start * count, count), count), :]
        high = weight.astype(bf16)
        low = (weight - high.astype(f32)).astype(bf16)
        return jnp.dot(high, known, preferred_element_type=f32) + jnp.dot(
            low, known, preferred_element_type=f32
        )

    given[...] = shared(1 - c)
    swap = remote(given, taken, ps, pr, sp_1=1 - c)
    swap.start()
    kept = middle_ref[...].astype(f32) + shared(c)
    swap.wait()
    out_ref[...] = (kept + taken[...]).astype(bf16)


QUAD = 4
TAIL = 16


def announce(nz, nx):
    z, c, x = lax.axis_index("sp_0"), lax.axis_index("sp_1"), lax.axis_index("tp")
    barrier = pltpu.get_barrier_semaphore()

    def along_z(k, carry):
        pl.semaphore_signal(barrier, inc=1, device_id={"sp_0": lax.rem(z + k, nz)})
        return carry

    def along_x(k, carry):
        pl.semaphore_signal(barrier, inc=1, device_id={"tp": lax.rem(x + k, nx)})
        return carry

    lax.fori_loop(1, nz, along_z, 0)
    lax.fori_loop(1, nx, along_x, 0)
    pl.semaphore_signal(barrier, inc=1, device_id={"sp_1": 1 - c})
    pl.semaphore_signal(
        barrier, inc=1, device_id={"sp_0": lax.rem(z + nz - 1 + 2 * c, nz), "sp_1": 1 - c}
    )


def silu(v):
    return v * jax.nn.sigmoid(v)


def exact_dot(a, b):
    return jnp.dot(a, b, preferred_element_type=jnp.float32, precision=lax.Precision.HIGHEST)


def packed(state, decays):
    lanes = state.shape[1]
    row = lax.broadcasted_iota(jnp.int32, (TAIL, lanes), 0)
    tail = jnp.zeros((TAIL, lanes), jnp.float32)
    for h, decay in enumerate(decays):
        wide = jnp.broadcast_to(decay, (TAIL, lanes))
        high = wide.astype(jnp.bfloat16).astype(jnp.float32)
        tail = jnp.where(row == h, high, tail)
        tail = jnp.where(row == TAIL // 2 + h, wide - high, tail)
    return jnp.concatenate([state.astype(jnp.bfloat16), tail.astype(jnp.bfloat16)], axis=0)


def unpacked(message, heads):
    rows = message.shape[0] - TAIL
    state = message[:rows].astype(jnp.float32)
    tail = message[rows:].astype(jnp.float32)
    half = TAIL // 2
    return state, [tail[h : h + 1, 0:1] + tail[half + h : half + h + 1, 0:1] for h in range(heads)]


def per_row(decays, rows, lanes):
    each = rows // len(decays)
    return jnp.concatenate([jnp.broadcast_to(d, (each, lanes)) for d in decays], axis=0)


def followed(earlier, later):
    (state_a, decay_a), (state_b, decay_b) = earlier, later
    state = state_a * per_row(decay_b, *state_a.shape) + state_b
    return state, [a * b for a, b in zip(decay_a, decay_b)]


def chosen(flag, one, other):
    return jnp.where(flag, one[0], other[0]), [
        jnp.where(flag, a, b) for a, b in zip(one[1], other[1])
    ]


def front_kernel(
    nz,
    nx,
    capacity,
    xs_ref,
    gate_ref,
    keys_ref,
    queries_ref,
    raw_ref,
    extra_ref,
    rate_ref,
    taps_x_ref,
    taps_k_ref,
    taps_q_ref,
    gain_ref,
    blend_hbm,
    carry_ref,
    gain2_ref,
    ids_ref,
    affinity_ref,
    chance_ref,
    outgoing_ref,
    middle_ref,
    weight_ref,
    halo,
    joined,
    pair_out,
    pair_in,
    quad_out,
    quad_in,
    far_out,
    far_in,
    half_out,
    half_in,
    gated_out,
    gated_in,
    facts,
    rows,
    blend,
    turned,
    blend_sem,
    halo_s,
    halo_r,
    pair_s,
    pair_r,
    quad_s,
    quad_r,
    far_s,
    far_r,
    gated_s,
    gated_r,
):
    z, c, x = lax.axis_index("sp_0"), lax.axis_index("sp_1"), lax.axis_index("tp")
    length, width_x = xs_ref.shape
    state_width = keys_ref.shape[1]
    heads = raw_ref.shape[0]
    head_dim = width_x // heads
    half_heads = heads // 2
    half_rows = width_x // 2
    place, quad = lax.rem(z, QUAD), z // QUAD
    quads = nz // QUAD
    f32, bf16 = jnp.float32, jnp.bfloat16
    partner = {"sp_1": 1 - c}
    announce(nz, nx)
    load = pltpu.make_async_copy(blend_hbm, blend, blend_sem)
    load.start()

    stride_row = jnp.maximum(raw_ref[...], 0.0) + jnp.log1p(jnp.exp(-jnp.abs(raw_ref[...])))
    diagonal = lax.broadcasted_iota(jnp.int32, (heads, heads), 0) == lax.broadcasted_iota(
        jnp.int32, (heads, heads), 1
    )
    rate = jnp.sum(
        jnp.where(diagonal, jnp.broadcast_to(rate_ref[...], (heads, heads)), 0.0),
        axis=1,
        keepdims=True,
    )
    log_row = extra_ref[...] - rate * stride_row
    t_axis = lax.broadcasted_iota(jnp.int32, (length, length), 0)
    s_axis = lax.broadcasted_iota(jnp.int32, (length, length), 1)
    causal = t_axis >= s_axis
    running_row = exact_dot(
        jnp.concatenate([log_row, jnp.zeros_like(log_row)], axis=0), (t_axis <= s_axis).astype(f32)
    )
    picks = ids_ref.shape[0]
    count = ids_ref.shape[1] // nx
    lanes = 128
    stacked = jnp.concatenate(
        [
            running_row[:heads],
            stride_row,
            ids_ref[...].astype(f32),
            jnp.zeros((lanes - 2 * heads - picks, length), f32),
        ],
        axis=0,
    )
    turned[...] = stacked.T
    running = turned[:, :heads]
    stride = turned[:, heads : 2 * heads]
    final = running[length - 1 : length, :]
    lifted = jnp.exp(affinity_ref[...])
    share_row = chance_ref[...] * lifted / jnp.sum(lifted, axis=0, keepdims=True)
    share_row = jnp.concatenate([share_row, jnp.zeros((lanes - picks, count), f32)], axis=0)
    share_row = jnp.concatenate([share_row, jnp.zeros((lanes, lanes - count), f32)], axis=1)
    shares = share_row.T[:count]
    local_experts = outgoing_ref.shape[0]
    experts = nz * 2 * local_experts
    ids = turned[pl.ds(pl.multiple_of(x * count, count), count), :]
    ids = ids[:, 2 * heads : 2 * heads + picks].astype(jnp.int32)
    expert_axis = lax.broadcasted_iota(jnp.int32, (count, experts), 1)
    member = [(ids[:, k : k + 1] == expert_axis).astype(f32) for k in range(picks)]
    row_axis = lax.broadcasted_iota(jnp.int32, (count, count), 0)
    column_axis = lax.broadcasted_iota(jnp.int32, (count, count), 1)
    earlier = (row_axis > column_axis).astype(bf16)
    before = jnp.dot(earlier, sum(member).astype(bf16), preferred_element_type=f32)
    lane = lax.broadcasted_iota(jnp.int32, (count, facts.shape[2]), 1)
    noted = jnp.zeros((count, facts.shape[2]), f32)
    for k in range(picks):
        position = jnp.sum(before * member[k], axis=1, keepdims=True)
        expert = ids[:, k : k + 1]
        holder = lax.div(expert, local_experts)
        slot = (
            (lax.rem(expert, local_experts) * nz + lax.div(holder, 2)) * 2 + c
        ) * capacity + position.astype(jnp.int32)
        for core in range(2):
            there = jnp.where(lax.rem(holder, 2) == core, slot, -1).astype(f32)
            noted = jnp.where(lane == core * picks + k, there, noted)
        noted = jnp.where(lane == 2 * picks + k, shares[:, k : k + 1], noted)
    facts[c] = noted

    pl.semaphore_wait(pltpu.get_barrier_semaphore(), nz + nx)
    rim = halo.shape[0]
    after = {"sp_0": lax.rem(z + c, nz), "sp_1": 1 - c}
    edges = []
    start = 0
    for n, ref in enumerate((xs_ref, keys_ref, queries_ref)):
        columns = pl.ds(start, ref.shape[1])
        edges.append(
            pltpu.make_async_remote_copy(
                ref.at[pl.ds(length - rim, rim)],
                halo.at[:, columns],
                halo_s.at[n],
                halo_r.at[n],
                device_id=after,
            )
        )
        start += ref.shape[1]
    for edge in edges:
        edge.start()
    facts_copy = pltpu.make_async_remote_copy(
        facts.at[c], facts.at[c], pair_s.at[0], pair_r.at[0], device_id=partner
    )
    facts_copy.start()

    start = 0
    for ref in (xs_ref, keys_ref, queries_ref):
        joined[rim:, start : start + ref.shape[1]] = ref[...].astype(f32)
        start += ref.shape[1]
    for edge in edges:
        edge.wait_recv()
    joined[:rim, :] = jnp.where(z + c > 0, halo[...].astype(f32), 0.0)
    taps = jnp.concatenate([taps_x_ref[...], taps_k_ref[...], taps_q_ref[...]], axis=1)
    kernel_len = taps.shape[0]
    convolved = taps[0:1, :] * joined[rim - kernel_len + 1 : rim - kernel_len + 1 + length, :]
    for tap in range(1, kernel_len):
        first = rim - kernel_len + 1 + tap
        convolved = convolved + taps[tap : tap + 1, :] * joined[first : first + length, :]
    convolved = silu(convolved)
    inputs_x = convolved[:, :width_x]
    keys_b = convolved[:, width_x : width_x + state_width].astype(bf16)
    queries_c = convolved[:, width_x + state_width :].astype(bf16)

    scaled = [
        inputs_x[:, h * head_dim : (h + 1) * head_dim] * stride[:, h : h + 1] for h in range(heads)
    ]
    remaining = jnp.concatenate(
        [scaled[h] * jnp.exp(final[:, h : h + 1] - running[:, h : h + 1]) for h in range(heads)],
        axis=1,
    ).astype(bf16)
    own_state = lax.dot_general(
        remaining, keys_b, (((0,), (0,)), ((), ())), preferred_element_type=f32
    )
    pair_out[...] = packed(own_state, [jnp.exp(final[:, h : h + 1]) for h in range(heads)])
    pair_copy = pltpu.make_async_remote_copy(
        pair_out, pair_in, pair_s.at[1], pair_r.at[1], device_id=partner
    )
    pair_copy.start()

    scores = lax.dot_general(
        queries_c, keys_b, (((1,), (1,)), ((), ())), preferred_element_type=f32
    )
    inside = []
    for h in range(heads):
        between = running[:, h : h + 1] - running_row[h : h + 1, :]
        decays = jnp.exp(jnp.where(causal, between, -1e30))
        inside.append(
            jnp.dot(
                (scores * decays).astype(bf16), scaled[h].astype(bf16), preferred_element_type=f32
            )
        )

    pair_copy.wait_recv()

    def half_of(ref):
        state, decays = unpacked(ref[...], heads)
        return (
            jnp.where(c == 0, state[:half_rows], state[half_rows:]),
            [jnp.where(c == 0, decays[j], decays[half_heads + j]) for j in range(half_heads)],
        )

    ours, theirs = half_of(pair_out), half_of(pair_in)
    lower, upper = chosen(c == 0, ours, theirs), chosen(c == 0, theirs, ours)
    chip = followed(lower, upper)
    quad_out[...] = packed(*chip)

    def quad_send(k):
        to = quad * QUAD + lax.rem(place + k, QUAD)
        return pltpu.make_async_remote_copy(
            quad_out, quad_in.at[place], quad_s.at[k], quad_r.at[k], device_id={"sp_0": to}
        )

    def quad_arrival(k):
        return pltpu.make_async_remote_copy(
            quad_out,
            quad_in.at[lax.rem(place + QUAD - k, QUAD)],
            quad_s.at[k],
            quad_r.at[k],
            device_id={"sp_0": lax.rem(z + 1, nz)},
        )

    for k in range(1, QUAD):
        quad_send(k).start()
    quad_in[place] = quad_out[...]
    for k in range(1, QUAD):
        quad_arrival(k).wait_recv()
    nothing = (jnp.zeros_like(chip[0]), [jnp.ones_like(d) for d in chip[1]])
    whole, inner = nothing, nothing
    for k in range(QUAD):
        inner = chosen(place == k, whole, inner)
        whole = followed(whole, unpacked(quad_in[k], half_heads))
    far_out[...] = packed(*whole)

    def far_send(k):
        return pltpu.make_async_remote_copy(
            far_out,
            far_in.at[k],
            far_s.at[k],
            far_r.at[k],
            device_id={"sp_0": lax.rem(z + k * QUAD, nz)},
        )

    for k in range(1, quads):

        @pl.when(quad + k < quads)
        def _(k=k):
            far_send(k).start()

    far_in[0] = jnp.zeros_like(far_out)
    for k in range(1, quads):

        @pl.when(quad >= k)
        def _(k=k):
            far_send(k).wait_recv()

        @pl.when(quad < k)
        def _(k=k):
            far_in[k] = jnp.zeros_like(far_out)

    incoming = nothing
    for k in reversed(range(1, quads)):
        incoming = followed(incoming, unpacked(far_in[k], half_heads))
    incoming = followed(incoming, inner)
    incoming_low = incoming[0]
    incoming_high = followed(incoming, lower)[0]
    half_out[...] = jnp.where(c == 0, incoming_high, incoming_low).astype(bf16)
    half_copy = pltpu.make_async_remote_copy(
        half_out, half_in, pair_s.at[2], pair_r.at[2], device_id=partner
    )
    half_copy.start()
    kept = jnp.where(c == 0, incoming_low, incoming_high).astype(bf16)
    modulation = silu(gate_ref[...].astype(f32))
    half_copy.wait_recv()
    sent_in = half_in[...]
    entering = jnp.concatenate(
        [jnp.where(c == 0, kept, sent_in), jnp.where(c == 0, sent_in, kept)], axis=0
    )
    outside = lax.dot_general(
        queries_c, entering, (((1,), (1,)), ((), ())), preferred_element_type=f32
    )
    mixed = jnp.concatenate(
        [
            inside[h]
            + outside[:, h * head_dim : (h + 1) * head_dim] * jnp.exp(running[:, h : h + 1])
            for h in range(heads)
        ],
        axis=1,
    )
    gated_out[...] = (mixed * modulation).astype(bf16).reshape(gated_out.shape)

    def gated_send(k):
        to = lax.rem(x + k, nx)
        return pltpu.make_async_remote_copy(
            gated_out.at[to], gated_in.at[x], gated_s.at[k], gated_r.at[k], device_id={"tp": to}
        )

    for k in range(1, nx):
        gated_send(k).start()
    gated_in[x] = gated_out[x]
    facts_arrival = pltpu.make_async_remote_copy(
        facts.at[1 - c], facts.at[1 - c], pair_s.at[0], pair_r.at[0], device_id=partner
    )
    facts_arrival.wait_recv()
    slot_count = weight_ref.shape[1]
    slot_axis = lax.broadcasted_iota(jnp.int32, (2 * count, slot_count), 1).astype(f32)
    known = jnp.concatenate([facts[0], facts[1]], axis=0)
    picked = jnp.zeros((2 * count, slot_count), f32)
    weight = jnp.zeros((2 * count, slot_count), f32)
    for k in range(picks):
        slot = jnp.where(c == 0, known[:, k : k + 1], known[:, picks + k : picks + k + 1])
        hit = slot == slot_axis
        picked = jnp.where(hit, 1.0, picked)
        weight = jnp.where(hit, known[:, 2 * picks + k : 2 * picks + k + 1], weight)
    weight_ref[...] = weight
    for k in range(1, nx):
        pltpu.make_async_remote_copy(
            gated_out.at[x],
            gated_in.at[lax.rem(x + nx - k, nx)],
            gated_s.at[k],
            gated_r.at[k],
            device_id={"tp": lax.rem(x + k, nx)},
        ).wait_recv()
    own_rows = jnp.concatenate([gated_in[k] for k in range(nx)], axis=1).astype(f32)
    normed = (
        own_rows
        * lax.rsqrt(jnp.mean(own_rows * own_rows, axis=1, keepdims=True) + EPS)
        * gain_ref[...]
    ).astype(bf16)
    load.wait()
    middle = (
        carry_ref[...].astype(f32) + jnp.dot(normed, blend[...], preferred_element_type=f32)
    ).astype(bf16)
    middle_ref[...] = middle
    wide = middle.astype(f32)
    rows[c] = (
        wide
        * lax.rsqrt(jnp.mean(wide * wide, axis=1, keepdims=True) + EPS)
        * gain2_ref[...]
    ).astype(bf16)
    rows_copy = pltpu.make_async_remote_copy(
        rows.at[c], rows.at[c], pair_s.at[3], pair_r.at[3], device_id=partner
    )
    rows_copy.start()
    pltpu.make_async_remote_copy(
        rows.at[1 - c], rows.at[1 - c], pair_s.at[3], pair_r.at[3], device_id=partner
    ).wait_recv()
    outgoing_ref[...] = (
        lax.dot_general(
            picked.astype(bf16),
            jnp.concatenate([rows[0], rows[1]], axis=0),
            (((0,), (0,)), ((), ())),
            preferred_element_type=f32,
        )
        .astype(bf16)
        .reshape(outgoing_ref.shape)
    )

    for edge in edges:
        edge.wait_send()
    facts_copy.wait_send()
    pair_copy.wait_send()
    half_copy.wait_send()
    rows_copy.wait_send()
    for k in range(1, QUAD):
        quad_send(k).wait_send()
    for k in range(1, quads):

        @pl.when(quad + k < quads)
        def _(k=k):
            far_send(k).wait_send()

    for k in range(1, nx):
        gated_send(k).wait_send()


FRONT_INPUTS = 17
FRONT_SCRATCH = 27


def layer_kernel(nz, nx, capacity, *refs):
    inputs, refs = refs[:FRONT_INPUTS], refs[FRONT_INPUTS:]
    weights, out_ref, refs = refs[:3], refs[3], refs[4:]
    outgoing, middle, weight, refs = *refs[:3], refs[3:]
    front_kernel(nz, nx, capacity, *inputs, outgoing, middle, weight, *refs[:FRONT_SCRATCH])
    experts_kernel(nz, nx, outgoing, *weights, middle, weight, out_ref, *refs[FRONT_SCRATCH:])


def layer(nz, nx, capacity, *arrays):
    xs, _, keys, queries, raw = arrays[:5]
    blend, carry = arrays[11:13]
    weights = arrays[FRONT_INPUTS:]
    experts = weights[0].shape[0]
    count, width = carry.shape
    rows = 2 * capacity
    channels, states = xs.shape[1], keys.shape[1]
    total = channels + states + queries.shape[1]
    rim = 8
    half = channels // 2
    bf16, f32 = jnp.bfloat16, jnp.float32
    vmem = pl.BlockSpec(memory_space=pltpu.VMEM)
    anywhere = pl.BlockSpec(memory_space=pl.ANY)
    slots = pltpu.VMEM((nz, experts, rows, width), bf16)
    wide = pltpu.VMEM((nz, experts, nx, rows, width), bf16)

    def sems(*shape):
        return pltpu.SemaphoreType.DMA(shape)

    front_scratch = [
        pltpu.VMEM((rim, total), bf16),
        pltpu.VMEM((rim + xs.shape[0], total), f32),
        pltpu.VMEM((channels + TAIL, states), bf16),
        pltpu.VMEM((channels + TAIL, states), bf16),
        pltpu.VMEM((half + TAIL, states), bf16),
        pltpu.VMEM((QUAD, half + TAIL, states), bf16),
        pltpu.VMEM((half + TAIL, states), bf16),
        pltpu.VMEM((nz // QUAD, half + TAIL, states), bf16),
        pltpu.VMEM((half, states), bf16),
        pltpu.VMEM((half, states), bf16),
        pltpu.VMEM((nx, count, channels), bf16),
        pltpu.VMEM((nx, count, channels), bf16),
        pltpu.VMEM((2, count, 128), f32),
        pltpu.VMEM((2, count, width), bf16),
        pltpu.VMEM(blend.shape, bf16),
        pltpu.VMEM((xs.shape[0], 128), f32),
        pltpu.SemaphoreType.DMA,
        sems(3),
        sems(3),
        sems(4),
        sems(4),
        sems(QUAD),
        sems(QUAD),
        sems(nz // QUAD),
        sems(nz // QUAD),
        sems(nx),
        sems(nx),
    ]
    experts_scratch = (
        [wide, wide, slots, slots, slots, slots, slots]
        + [pltpu.VMEM((experts, nz, rows, width), bf16)]
        + [pltpu.VMEM(w.shape, bf16) for w in weights]
        + [pltpu.VMEM((count, width), f32)] * 2
        + [sems(3), sems(2), sems(nz), sems(nz), sems(2, nz), sems(2, nz)]
        + [sems(nz)] * 10
        + [pltpu.SemaphoreType.DMA] * 2
    )
    assert len(front_scratch) == FRONT_SCRATCH
    return pl.pallas_call(
        functools.partial(layer_kernel, nz, nx, capacity),
        out_shape=jax.ShapeDtypeStruct((count, width), bf16),
        in_specs=[vmem] * 11 + [anywhere] + [vmem] * 5 + [anywhere] * 3,
        out_specs=vmem,
        scratch_shapes=[
            pltpu.VMEM((experts, nz, rows, width), bf16),
            pltpu.VMEM((count, width), bf16),
            pltpu.VMEM((2 * count, experts * nz * rows), f32),
        ]
        + front_scratch
        + experts_scratch,
        compiler_params=pltpu.CompilerParams(
            collective_id=1, has_side_effects=True, vmem_limit_bytes=60 << 20
        ),
        name="layer",
    )(*arrays)


def per_device(
    carryover_vector,
    channel_source_entries,
    final_modulation_vector,
    entering_basis_matrix,
    readout_basis_matrix,
    raw_stride_amount,
    extra_log_attenuation,
    channel_fading_rate,
    channel_source_kernel,
    entering_basis_kernel,
    readout_basis_kernel,
    modulated_rescaling_vector,
    blender_final_matrix,
    specialist_rescaling_vector,
    specialist_gating_matrices,
    widening_matrices,
    contracting_matrices,
    assigned_specialist_ids,
    specialist_choice_affinity,
    cluster_chance,
):
    nz, cores, nx = lax.axis_size("sp_0"), lax.axis_size("sp_1"), lax.axis_size("tp")
    row_count = carryover_vector.shape[0]
    local_experts = specialist_gating_matrices.shape[0]
    experts = nz * cores * local_experts
    picks = assigned_specialist_ids.shape[1]
    capacity = 2 * row_count * picks // experts
    return layer(
        nz,
        nx,
        capacity,
        channel_source_entries,
        final_modulation_vector,
        entering_basis_matrix,
        readout_basis_matrix,
        raw_stride_amount.T,
        extra_log_attenuation.T,
        channel_fading_rate[None, :],
        channel_source_kernel,
        entering_basis_kernel,
        readout_basis_kernel,
        modulated_rescaling_vector[None, :],
        blender_final_matrix,
        carryover_vector,
        specialist_rescaling_vector[None, :],
        assigned_specialist_ids.T,
        specialist_choice_affinity.T,
        cluster_chance[None, :],
        specialist_gating_matrices,
        widening_matrices,
        contracting_matrices,
    )


def solution(mesh):
    finer = Mesh(
        mesh.devices.reshape(mesh.shape["grp"], mesh.shape["sp"] // 2, 2, mesh.shape["tp"]),
        ("grp", "sp_0", "sp_1", "tp"),
    )
    return jax.shard_map(
        per_device,
        mesh=finer,
        in_specs=(
            P(GRP_SP_TP, None),
            P(GRP_SP, "tp"),
            P(GRP_SP, "tp"),
            P(GRP_SP, "tp"),
            P(GRP_SP, "tp"),
            P(GRP_SP, "tp"),
            P(GRP_SP, "tp"),
            P("tp"),
            P(None, "tp"),
            P(None, "tp"),
            P(None, "tp"),
            P(),
            P(),
            P(),
            P(SP, None, "tp"),
            P(SP, None, "tp"),
            P(SP, "tp", None),
            P(GRP_SP, None),
            P(GRP_SP_TP, None),
            P(GRP_SP_TP),
        ),
        out_specs=P(GRP_SP_TP, None),
        check_vma=False,
    )
```

```python
import functools

import jax
import jax.numpy as jnp
from jax import lax
from jax.experimental import pallas as pl
from jax.experimental.pallas import tpu as pltpu
from jax.sharding import Mesh
from jax.sharding import PartitionSpec as P

SP = ("sp_0", "sp_1")
GRP_SP_TP = ("grp", "sp_0", "sp_1", "tp")
GRP_SP = ("grp", "sp_0", "sp_1")


EPS = 1e-06


NEAR = 4


def hop(step, nz):
    step = jnp.where(step > NEAR, nz + NEAR - step, step)
    half = (step + 1) // 2
    return jnp.where(step % 2 == 1, half, -half)


def experts_kernel(
    nz,
    nx,
    src,
    gates_hbm,
    ups_hbm,
    downs_hbm,
    middle_ref,
    weight_ref,
    out_ref,
    arrived,
    part,
    far,
    near,
    both,
    mine,
    total,
    answers,
    gates,
    ups,
    downs,
    given,
    taken,
    load_sem,
    here,
    zs,
    zr,
    xs,
    xr,
    os_,
    or_,
    fs,
    fr,
    ns,
    nr,
    bs,
    br,
    ts,
    tr,
    ps,
    pr,
):
    z, c, x = lax.axis_index("sp_0"), lax.axis_index("sp_1"), lax.axis_index("tp")
    xp, xm = lax.rem(x + 1, nx), lax.rem(x + nx - 1, nx)
    x2 = lax.rem(x + 2, nx)
    local_experts, _, rows, width = src.shape
    f32, bf16 = jnp.float32, jnp.bfloat16
    loads = [
        pltpu.make_async_copy(a, b, load_sem.at[n])
        for n, (a, b) in enumerate(((gates_hbm, gates), (ups_hbm, ups), (downs_hbm, downs)))
    ]
    for load in loads:
        load.start()

    def goal(i):
        return lax.rem(z + hop(i, nz) + nz, nz)

    def origin(i):
        return lax.rem(z - hop(i, nz) + nz, nz)

    def ahead(i):
        return jnp.where(i % 2 == 0, xp, xm)

    def behind(i):
        return jnp.where(i % 2 == 0, xm, xp)

    def remote(a, b, sent, got, **to):
        return pltpu.make_async_remote_copy(a, b, sent, got, device_id=to)

    def along_z(i):
        return remote(src.at[:, goal(i)], arrived.at[i, :, x], zs.at[i], zr.at[i], sp_0=goal(i))

    def along_x(i, way):
        chunk = arrived.at[i, :, x]
        to = xp if way == 0 else xm
        return remote(chunk, chunk, xs.at[way, i], xr.at[way, i], tp=to)

    def from_x(i, way):
        chunk = arrived.at[i, :, jnp.where(way == 0, xm, xp)]
        return remote(chunk, chunk, xs.at[way, i], xr.at[way, i], tp=xp)

    def onward(i):
        chunk = arrived.at[i, :, behind(i)]
        return remote(chunk, chunk, os_.at[i], or_.at[i], tp=ahead(i))

    def from_far(i):
        chunk = arrived.at[i, :, x2]
        return remote(chunk, chunk, os_.at[i], or_.at[i], tp=xp)

    def send_far(i):
        return remote(part.at[i, :, x2], far.at[i], fs.at[i], fr.at[i], tp=ahead(i))

    def send_near(i):
        return remote(part.at[i, :, behind(i)], near.at[i], ns.at[i], nr.at[i], tp=behind(i))

    def send_both(i):
        return remote(mine.at[i], both.at[i], bs.at[i], br.at[i], tp=ahead(i))

    def send_back(i):
        return remote(total.at[i], answers.at[:, z], ts.at[i], tr.at[i], sp_0=origin(i))

    def send_z(i, carry):
        along_z(i).start()
        return carry

    lax.fori_loop(1, nz, send_z, 0)
    own = pltpu.make_async_copy(src.at[:, z], arrived.at[0, :, x], here.at[0])
    own.start()
    own.wait()

    def spread(i):
        along_x(i, 0).start()
        along_x(i, 1).start()

    def pass_on(i):
        from_x(i, i % 2).wait_recv()
        onward(i).start()

    def complete(i):
        from_x(i, (i + 1) % 2).wait_recv()
        from_far(i).wait_recv()

    def multiply(i):
        for e in range(local_experts):
            tokens = jnp.concatenate(
                [
                    arrived[i + k, e].astype(f32).reshape(nx * rows, width).astype(bf16)
                    for k in range(2)
                ],
                axis=0,
            )
            gate = jnp.dot(tokens, gates[e], preferred_element_type=f32)
            up = jnp.dot(tokens, ups[e], preferred_element_type=f32)
            hidden = (silu(gate) * up).astype(bf16)
            result = jnp.dot(hidden, downs[e], preferred_element_type=f32)
            for k in range(2):
                part[i + k, e] = (
                    result[k * nx * rows : (k + 1) * nx * rows].reshape(nx, rows, width).astype(bf16)
                )

    def first(i):
        send_far(i).start()
        send_near(i).start()

    def second(i):
        send_far(i).wait_recv()
        mine[i] = (part[i, :, ahead(i)].astype(f32) + far[i].astype(f32)).astype(bf16)
        send_both(i).start()

    def third(i):
        send_near(i).wait_recv()
        send_both(i).wait_recv()
        total[i] = (
            part[i, :, x].astype(f32) + near[i].astype(f32) + both[i].astype(f32)
        ).astype(bf16)

    pairs = nz // 2

    def turn(p, carry):
        i = 2 * p

        @pl.when(p == 0)
        def _():
            spread(0)

        @pl.when((p > 0) & (p < pairs))
        def _():
            remote(src.at[:, z], arrived.at[i, :, x], zs.at[i], zr.at[i], tp=xp).wait_recv()
            spread(i)

        @pl.when((p > 0) & (p <= pairs))
        def _():
            pass_on(i - 1)

        @pl.when(p < pairs)
        def _():
            remote(src.at[:, z], arrived.at[i + 1, :, x], zs.at[i + 1], zr.at[i + 1], tp=xp).wait_recv()
            spread(i + 1)
            pass_on(i)

        @pl.when(p == 1)
        def _():
            for load in loads:
                load.wait()

        @pl.when((p > 0) & (p <= pairs))
        def _():
            complete(i - 2)
            complete(i - 1)
            multiply(i - 2)
            first(i - 2)
            first(i - 1)

        @pl.when((p > 1) & (p <= pairs + 1))
        def _():
            second(i - 4)
            second(i - 3)

        @pl.when(p > 2)
        def _():
            third(i - 6)
            third(i - 5)

            @pl.when(p > 3)
            def _():
                send_back(i - 6).start()

            send_back(i - 5).start()

        return carry

    lax.fori_loop(0, pairs + 3, turn, 0)
    own_back = pltpu.make_async_copy(total.at[0], answers.at[:, z], here.at[1])
    own_back.start()
    own_back.wait()

    def sent(i, carry):
        along_x(i, 0).wait_send()
        along_x(i, 1).wait_send()
        onward(i).wait_send()
        send_far(i).wait_send()
        send_near(i).wait_send()
        send_both(i).wait_send()
        return carry

    lax.fori_loop(0, nz, sent, 0)

    def returned(i, carry):
        along_z(i).wait_send()
        send_back(i).wait_send()
        remote(total.at[i], answers.at[:, goal(i)], ts.at[i], tr.at[i], tp=xp).wait_recv()
        return carry

    lax.fori_loop(1, nz, returned, 0)

    count = out_ref.shape[0]
    slots = local_experts * nz * rows
    known = answers[...].astype(f32).reshape(slots, width).astype(bf16)

    def shared(start):
        weight = weight_ref[pl.ds(pl.multiple_of(start * count, count), count), :]
        high = weight.astype(bf16)
        low = (weight - high.astype(f32)).astype(bf16)
        return jnp.dot(high, known, preferred_element_type=f32) + jnp.dot(
            low, known, preferred_element_type=f32
        )

    given[...] = shared(1 - c)
    swap = remote(given, taken, ps, pr, sp_1=1 - c)
    swap.start()
    kept = middle_ref[...].astype(f32) + shared(c)
    swap.wait()
    out_ref[...] = (kept + taken[...]).astype(bf16)


QUAD = 4
TAIL = 16


def announce(nz, nx):
    z, c, x = lax.axis_index("sp_0"), lax.axis_index("sp_1"), lax.axis_index("tp")
    place, quad = lax.rem(z, QUAD), z // QUAD
    barrier = pltpu.get_barrier_semaphore()
    beyond = z + 2 * c - 1
    has_beyond = (beyond >= 0) & (beyond < nz)
    before = (place == 0) & (quad > 0)
    behind = (place == QUAD - 1) & (quad < nz // QUAD - 1)

    def in_quad(k, carry):
        to = quad * QUAD + lax.rem(place + k, QUAD)
        pl.semaphore_signal(barrier, inc=1, device_id={"sp_0": to})
        return carry

    def along_x(k, carry):
        pl.semaphore_signal(barrier, inc=1, device_id={"tp": lax.rem(x + k, nx)})
        return carry

    pl.semaphore_signal(barrier, inc=1, device_id={"sp_1": 1 - c})
    lax.fori_loop(1, QUAD, in_quad, 0)
    lax.fori_loop(1, nx, along_x, 0)

    @pl.when(has_beyond)
    def _():
        pl.semaphore_signal(barrier, inc=1, device_id={"sp_0": beyond, "sp_1": 1 - c})

    @pl.when(before)
    def _():
        pl.semaphore_signal(barrier, inc=1, device_id={"sp_0": z - 1})

    @pl.when(behind)
    def _():
        pl.semaphore_signal(barrier, inc=1, device_id={"sp_0": z + 1})

    return QUAD + nx - 1 + sum(flag.astype(jnp.int32) for flag in (has_beyond, before, behind))


def pass_word(nz, token, ready):
    z = lax.axis_index("sp_0")
    place, quad = lax.rem(z, QUAD), z // QUAD
    last = nz // QUAD - 1

    @pl.when((place == 0) & (quad > 0))
    def _():
        pl.semaphore_wait(token, 1)

    @pl.when((place == 0) & (quad < last))
    def _():
        pl.semaphore_signal(token, inc=1, device_id={"sp_0": z + QUAD - 1})

    @pl.when((place == QUAD - 1) & (quad < last))
    def _():
        pl.semaphore_wait(token, 1)
        pl.semaphore_signal(token, inc=1, device_id={"sp_0": z + 1})

    @pl.when((place == 0) & (quad == last))
    def _():
        def tell(k, carry):
            pl.semaphore_signal(ready, inc=1, device_id={"sp_0": lax.rem(z + k, nz)})
            return carry

        lax.fori_loop(1, nz, tell, 0)


def silu(v):
    return v * jax.nn.sigmoid(v)


def exact_dot(a, b):
    return jnp.dot(a, b, preferred_element_type=jnp.float32, precision=lax.Precision.HIGHEST)


def packed(state, decays):
    lanes = state.shape[1]
    row = lax.broadcasted_iota(jnp.int32, (TAIL, lanes), 0)
    tail = jnp.zeros((TAIL, lanes), jnp.float32)
    for h, decay in enumerate(decays):
        wide = jnp.broadcast_to(decay, (TAIL, lanes))
        high = wide.astype(jnp.bfloat16).astype(jnp.float32)
        tail = jnp.where(row == h, high, tail)
        tail = jnp.where(row == TAIL // 2 + h, wide - high, tail)
    return jnp.concatenate([state.astype(jnp.bfloat16), tail.astype(jnp.bfloat16)], axis=0)


def unpacked(message, heads):
    rows = message.shape[0] - TAIL
    state = message[:rows].astype(jnp.float32)
    tail = message[rows:].astype(jnp.float32)
    half = TAIL // 2
    return state, [tail[h : h + 1, 0:1] + tail[half + h : half + h + 1, 0:1] for h in range(heads)]


def per_row(decays, rows, lanes):
    each = rows // len(decays)
    return jnp.concatenate([jnp.broadcast_to(d, (each, lanes)) for d in decays], axis=0)


def followed(earlier, later):
    (state_a, decay_a), (state_b, decay_b) = earlier, later
    state = state_a * per_row(decay_b, *state_a.shape) + state_b
    return state, [a * b for a, b in zip(decay_a, decay_b)]


def chosen(flag, one, other):
    return jnp.where(flag, one[0], other[0]), [
        jnp.where(flag, a, b) for a, b in zip(one[1], other[1])
    ]


def front_kernel(
    nz,
    nx,
    capacity,
    xs_ref,
    gate_ref,
    keys_ref,
    queries_ref,
    raw_ref,
    extra_ref,
    rate_ref,
    taps_x_ref,
    taps_k_ref,
    taps_q_ref,
    gain_ref,
    blend_hbm,
    carry_ref,
    gain2_ref,
    ids_ref,
    affinity_ref,
    chance_ref,
    outgoing_ref,
    middle_ref,
    weight_ref,
    halo,
    joined,
    pair_out,
    pair_in,
    quad_out,
    quad_in,
    far_out,
    far_in,
    half_out,
    half_in,
    gated_out,
    gated_in,
    facts,
    rows,
    blend,
    turned,
    smooth,
    fading,
    blend_sem,
    halo_s,
    halo_r,
    pair_s,
    pair_r,
    quad_s,
    quad_r,
    far_s,
    far_r,
    gated_s,
    gated_r,
    token,
    ready,
):
    z, c, x = lax.axis_index("sp_0"), lax.axis_index("sp_1"), lax.axis_index("tp")
    length, width_x = xs_ref.shape
    state_width = keys_ref.shape[1]
    heads = raw_ref.shape[0]
    head_dim = width_x // heads
    half_heads = heads // 2
    half_rows = width_x // 2
    place, quad = lax.rem(z, QUAD), z // QUAD
    quads = nz // QUAD
    f32, bf16 = jnp.float32, jnp.bfloat16
    partner = {"sp_1": 1 - c}
    greeted = announce(nz, nx)
    load = pltpu.make_async_copy(blend_hbm, blend, blend_sem)
    load.start()

    stride_row = jnp.maximum(raw_ref[...], 0.0) + jnp.log1p(jnp.exp(-jnp.abs(raw_ref[...])))
    diagonal = lax.broadcasted_iota(jnp.int32, (heads, heads), 0) == lax.broadcasted_iota(
        jnp.int32, (heads, heads), 1
    )
    rate = jnp.sum(
        jnp.where(diagonal, jnp.broadcast_to(rate_ref[...], (heads, heads)), 0.0),
        axis=1,
        keepdims=True,
    )
    log_row = extra_ref[...] - rate * stride_row
    t_axis = lax.broadcasted_iota(jnp.int32, (length, length), 0)
    s_axis = lax.broadcasted_iota(jnp.int32, (length, length), 1)
    causal = t_axis >= s_axis
    running_row = exact_dot(
        jnp.concatenate([log_row, jnp.zeros_like(log_row)], axis=0), (t_axis <= s_axis).astype(f32)
    )
    picks = ids_ref.shape[0]
    count = ids_ref.shape[1] // nx
    lanes = 128
    stacked = jnp.concatenate(
        [
            running_row[:heads],
            stride_row,
            ids_ref[...].astype(f32),
            jnp.zeros((lanes - 2 * heads - picks, length), f32),
        ],
        axis=0,
    )
    turned[...] = stacked.T
    running = turned[:, :heads]
    stride = turned[:, heads : 2 * heads]
    final = running[length - 1 : length, :]
    lifted = jnp.exp(affinity_ref[...])
    share_row = chance_ref[...] * lifted / jnp.sum(lifted, axis=0, keepdims=True)
    share_row = jnp.concatenate([share_row, jnp.zeros((lanes - picks, count), f32)], axis=0)
    share_row = jnp.concatenate([share_row, jnp.zeros((lanes, lanes - count), f32)], axis=1)
    shares = share_row.T[:count]
    local_experts = outgoing_ref.shape[0]
    experts = nz * 2 * local_experts
    ids = turned[pl.ds(pl.multiple_of(x * count, count), count), :]
    ids = ids[:, 2 * heads : 2 * heads + picks].astype(jnp.int32)
    expert_axis = lax.broadcasted_iota(jnp.int32, (count, experts), 1)
    member = [(ids[:, k : k + 1] == expert_axis).astype(f32) for k in range(picks)]
    row_axis = lax.broadcasted_iota(jnp.int32, (count, count), 0)
    column_axis = lax.broadcasted_iota(jnp.int32, (count, count), 1)
    earlier = (row_axis > column_axis).astype(bf16)
    before = jnp.dot(earlier, sum(member).astype(bf16), preferred_element_type=f32)
    lane = lax.broadcasted_iota(jnp.int32, (count, facts.shape[2]), 1)
    noted = jnp.zeros((count, facts.shape[2]), f32)
    for k in range(picks):
        position = jnp.sum(before * member[k], axis=1, keepdims=True)
        expert = ids[:, k : k + 1]
        holder = lax.div(expert, local_experts)
        slot = (
            (lax.rem(expert, local_experts) * nz + lax.div(holder, 2)) * 2 + c
        ) * capacity + position.astype(jnp.int32)
        for core in range(2):
            there = jnp.where(lax.rem(holder, 2) == core, slot, -1).astype(f32)
            noted = jnp.where(lane == core * picks + k, there, noted)
        noted = jnp.where(lane == 2 * picks + k, shares[:, k : k + 1], noted)
    facts[c] = noted

    rim = halo.shape[0]
    start = 0
    for ref in (xs_ref, keys_ref, queries_ref):
        joined[rim:, start : start + ref.shape[1]] = ref[...].astype(f32)
        start += ref.shape[1]
    taps = jnp.concatenate([taps_x_ref[...], taps_k_ref[...], taps_q_ref[...]], axis=1)
    kernel_len = taps.shape[0]

    def convolve(begin, end):
        start = rim - kernel_len + 1
        total = taps[0:1, :] * joined[start + begin : start + end, :]
        for tap in range(1, kernel_len):
            total = total + taps[tap : tap + 1, :] * joined[start + tap + begin : start + tap + end, :]
        return silu(total)

    smooth[rim:, :] = convolve(rim, length)
    modulation = silu(gate_ref[...].astype(f32))
    for h in range(heads):
        between = running[:, h : h + 1] - running_row[h : h + 1, :]
        fading[h] = jnp.exp(jnp.where(causal, between, -1e30))

    pl.semaphore_wait(pltpu.get_barrier_semaphore(), greeted)
    pass_word(nz, token, ready)
    after = {"sp_0": lax.rem(z + c, nz), "sp_1": 1 - c}
    edges = []
    start = 0
    for n, ref in enumerate((xs_ref, keys_ref, queries_ref)):
        columns = pl.ds(start, ref.shape[1])
        edges.append(
            pltpu.make_async_remote_copy(
                ref.at[pl.ds(length - rim, rim)],
                halo.at[:, columns],
                halo_s.at[n],
                halo_r.at[n],
                device_id=after,
            )
        )
        start += ref.shape[1]

    @pl.when(z + c < nz)
    def _():
        for edge in edges:
            edge.start()

    facts_copy = pltpu.make_async_remote_copy(
        facts.at[c], facts.at[c], pair_s.at[0], pair_r.at[0], device_id=partner
    )
    facts_copy.start()

    @pl.when(z + c > 0)
    def _():
        for edge in edges:
            edge.wait_recv()
        joined[:rim, :] = halo[...].astype(f32)

    @pl.when(z + c == 0)
    def _():
        joined[:rim, :] = jnp.zeros_like(joined[:rim, :])

    smooth[:rim, :] = convolve(0, rim)
    inputs_x = smooth[:, :width_x]
    keys_b = smooth[:, width_x : width_x + state_width].astype(bf16)
    queries_c = smooth[:, width_x + state_width :].astype(bf16)

    scaled = [
        inputs_x[:, h * head_dim : (h + 1) * head_dim] * stride[:, h : h + 1] for h in range(heads)
    ]
    remaining = jnp.concatenate(
        [scaled[h] * jnp.exp(final[:, h : h + 1] - running[:, h : h + 1]) for h in range(heads)],
        axis=1,
    ).astype(bf16)
    own_state = lax.dot_general(
        remaining, keys_b, (((0,), (0,)), ((), ())), preferred_element_type=f32
    )
    pair_out[...] = packed(own_state, [jnp.exp(final[:, h : h + 1]) for h in range(heads)])
    pair_copy = pltpu.make_async_remote_copy(
        pair_out, pair_in, pair_s.at[1], pair_r.at[1], device_id=partner
    )
    pair_copy.start()

    scores = lax.dot_general(
        queries_c, keys_b, (((1,), (1,)), ((), ())), preferred_element_type=f32
    )
    inside = []
    for h in range(heads):
        inside.append(
            jnp.dot(
                (scores * fading[h]).astype(bf16), scaled[h].astype(bf16), preferred_element_type=f32
            )
        )

    pair_copy.wait_recv()

    def half_of(ref):
        state, decays = unpacked(ref[...], heads)
        return (
            jnp.where(c == 0, state[:half_rows], state[half_rows:]),
            [jnp.where(c == 0, decays[j], decays[half_heads + j]) for j in range(half_heads)],
        )

    ours, theirs = half_of(pair_out), half_of(pair_in)
    lower, upper = chosen(c == 0, ours, theirs), chosen(c == 0, theirs, ours)
    chip = followed(lower, upper)
    quad_out[...] = packed(*chip)

    def quad_send(k):
        to = quad * QUAD + lax.rem(place + k, QUAD)
        return pltpu.make_async_remote_copy(
            quad_out, quad_in.at[place], quad_s.at[k], quad_r.at[k], device_id={"sp_0": to}
        )

    def quad_arrival(k):
        return pltpu.make_async_remote_copy(
            quad_out,
            quad_in.at[lax.rem(place + QUAD - k, QUAD)],
            quad_s.at[k],
            quad_r.at[k],
            device_id={"sp_0": lax.rem(z + 1, nz)},
        )

    for k in range(1, QUAD):
        quad_send(k).start()
    quad_in[place] = quad_out[...]
    for k in range(1, QUAD):
        quad_arrival(k).wait_recv()
    nothing = (jnp.zeros_like(chip[0]), [jnp.ones_like(d) for d in chip[1]])
    whole, inner = nothing, nothing
    for k in range(QUAD):
        inner = chosen(place == k, whole, inner)
        whole = followed(whole, unpacked(quad_in[k], half_heads))
    far_out[...] = packed(*whole)

    @pl.when((place > 0) | (quad < quads - 1))
    def _():
        pl.semaphore_wait(ready, 1)


    def far_send(k):
        return pltpu.make_async_remote_copy(
            far_out,
            far_in.at[k],
            far_s.at[k],
            far_r.at[k],
            device_id={"sp_0": lax.rem(z + k * QUAD, nz)},
        )

    for k in range(1, quads):

        @pl.when(quad + k < quads)
        def _(k=k):
            far_send(k).start()

    far_in[0] = jnp.zeros_like(far_out)
    for k in range(1, quads):

        @pl.when(quad >= k)
        def _(k=k):
            far_send(k).wait_recv()

        @pl.when(quad < k)
        def _(k=k):
            far_in[k] = jnp.zeros_like(far_out)

    incoming = nothing
    for k in reversed(range(1, quads)):
        incoming = followed(incoming, unpacked(far_in[k], half_heads))
    incoming = followed(incoming, inner)
    incoming_low = incoming[0]
    incoming_high = followed(incoming, lower)[0]
    half_out[...] = jnp.where(c == 0, incoming_high, incoming_low).astype(bf16)
    half_copy = pltpu.make_async_remote_copy(
        half_out, half_in, pair_s.at[2], pair_r.at[2], device_id=partner
    )
    half_copy.start()
    kept = jnp.where(c == 0, incoming_low, incoming_high).astype(bf16)
    half_copy.wait_recv()
    sent_in = half_in[...]
    entering = jnp.concatenate(
        [jnp.where(c == 0, kept, sent_in), jnp.where(c == 0, sent_in, kept)], axis=0
    )
    outside = lax.dot_general(
        queries_c, entering, (((1,), (1,)), ((), ())), preferred_element_type=f32
    )
    mixed = jnp.concatenate(
        [
            inside[h]
            + outside[:, h * head_dim : (h + 1) * head_dim] * jnp.exp(running[:, h : h + 1])
            for h in range(heads)
        ],
        axis=1,
    )
    gated_out[...] = (mixed * modulation).astype(bf16).reshape(gated_out.shape)

    def gated_send(k):
        to = lax.rem(x + k, nx)
        return pltpu.make_async_remote_copy(
            gated_out.at[to], gated_in.at[x], gated_s.at[k], gated_r.at[k], device_id={"tp": to}
        )

    for k in range(1, nx):
        gated_send(k).start()
    gated_in[x] = gated_out[x]
    facts_arrival = pltpu.make_async_remote_copy(
        facts.at[1 - c], facts.at[1 - c], pair_s.at[0], pair_r.at[0], device_id=partner
    )
    facts_arrival.wait_recv()
    slot_count = weight_ref.shape[1]
    slot_axis = lax.broadcasted_iota(jnp.int32, (2 * count, slot_count), 1).astype(f32)
    known = jnp.concatenate([facts[0], facts[1]], axis=0)
    picked = jnp.zeros((2 * count, slot_count), f32)
    weight = jnp.zeros((2 * count, slot_count), f32)
    for k in range(picks):
        slot = jnp.where(c == 0, known[:, k : k + 1], known[:, picks + k : picks + k + 1])
        hit = slot == slot_axis
        picked = jnp.where(hit, 1.0, picked)
        weight = jnp.where(hit, known[:, 2 * picks + k : 2 * picks + k + 1], weight)
    weight_ref[...] = weight
    for k in range(1, nx):
        pltpu.make_async_remote_copy(
            gated_out.at[x],
            gated_in.at[lax.rem(x + nx - k, nx)],
            gated_s.at[k],
            gated_r.at[k],
            device_id={"tp": lax.rem(x + k, nx)},
        ).wait_recv()
    own_rows = jnp.concatenate([gated_in[k] for k in range(nx)], axis=1).astype(f32)
    normed = (
        own_rows
        * lax.rsqrt(jnp.mean(own_rows * own_rows, axis=1, keepdims=True) + EPS)
        * gain_ref[...]
    ).astype(bf16)
    load.wait()
    middle = (
        carry_ref[...].astype(f32) + jnp.dot(normed, blend[...], preferred_element_type=f32)
    ).astype(bf16)
    middle_ref[...] = middle
    wide = middle.astype(f32)
    rows[c] = (
        wide
        * lax.rsqrt(jnp.mean(wide * wide, axis=1, keepdims=True) + EPS)
        * gain2_ref[...]
    ).astype(bf16)
    rows_copy = pltpu.make_async_remote_copy(
        rows.at[c], rows.at[c], pair_s.at[3], pair_r.at[3], device_id=partner
    )
    rows_copy.start()
    pltpu.make_async_remote_copy(
        rows.at[1 - c], rows.at[1 - c], pair_s.at[3], pair_r.at[3], device_id=partner
    ).wait_recv()
    outgoing_ref[...] = (
        lax.dot_general(
            picked.astype(bf16),
            jnp.concatenate([rows[0], rows[1]], axis=0),
            (((0,), (0,)), ((), ())),
            preferred_element_type=f32,
        )
        .astype(bf16)
        .reshape(outgoing_ref.shape)
    )


    @pl.when(z + c < nz)
    def _():
        for edge in edges:
            edge.wait_send()

    facts_copy.wait_send()
    pair_copy.wait_send()
    half_copy.wait_send()
    rows_copy.wait_send()
    for k in range(1, QUAD):
        quad_send(k).wait_send()
    for k in range(1, quads):

        @pl.when(quad + k < quads)
        def _(k=k):
            far_send(k).wait_send()

    for k in range(1, nx):
        gated_send(k).wait_send()


FRONT_INPUTS = 17
FRONT_SCRATCH = 31


def layer_kernel(nz, nx, capacity, *refs):
    inputs, refs = refs[:FRONT_INPUTS], refs[FRONT_INPUTS:]
    weights, out_ref, refs = refs[:3], refs[3], refs[4:]
    outgoing, middle, weight, refs = *refs[:3], refs[3:]
    front_kernel(nz, nx, capacity, *inputs, outgoing, middle, weight, *refs[:FRONT_SCRATCH])
    experts_kernel(nz, nx, outgoing, *weights, middle, weight, out_ref, *refs[FRONT_SCRATCH:])


def layer(nz, nx, capacity, *arrays):
    xs, _, keys, queries, raw = arrays[:5]
    blend, carry = arrays[11:13]
    weights = arrays[FRONT_INPUTS:]
    experts = weights[0].shape[0]
    count, width = carry.shape
    rows = 2 * capacity
    channels, states = xs.shape[1], keys.shape[1]
    total = channels + states + queries.shape[1]
    rim = 8
    half = channels // 2
    bf16, f32 = jnp.bfloat16, jnp.float32
    vmem = pl.BlockSpec(memory_space=pltpu.VMEM)
    anywhere = pl.BlockSpec(memory_space=pl.ANY)
    slots = pltpu.VMEM((nz, experts, rows, width), bf16)
    wide = pltpu.VMEM((nz, experts, nx, rows, width), bf16)

    def sems(*shape):
        return pltpu.SemaphoreType.DMA(shape)

    front_scratch = [
        pltpu.VMEM((rim, total), bf16),
        pltpu.VMEM((rim + xs.shape[0], total), f32),
        pltpu.VMEM((channels + TAIL, states), bf16),
        pltpu.VMEM((channels + TAIL, states), bf16),
        pltpu.VMEM((half + TAIL, states), bf16),
        pltpu.VMEM((QUAD, half + TAIL, states), bf16),
        pltpu.VMEM((half + TAIL, states), bf16),
        pltpu.VMEM((nz // QUAD, half + TAIL, states), bf16),
        pltpu.VMEM((half, states), bf16),
        pltpu.VMEM((half, states), bf16),
        pltpu.VMEM((nx, count, channels), bf16),
        pltpu.VMEM((nx, count, channels), bf16),
        pltpu.VMEM((2, count, 128), f32),
        pltpu.VMEM((2, count, width), bf16),
        pltpu.VMEM(blend.shape, bf16),
        pltpu.VMEM((xs.shape[0], 128), f32),
        pltpu.VMEM((xs.shape[0], total), f32),
        pltpu.VMEM((raw.shape[0], xs.shape[0], xs.shape[0]), f32),
        pltpu.SemaphoreType.DMA,
        sems(3),
        sems(3),
        sems(4),
        sems(4),
        sems(QUAD),
        sems(QUAD),
        sems(nz // QUAD),
        sems(nz // QUAD),
        sems(nx),
        sems(nx),
        pltpu.SemaphoreType.REGULAR,
        pltpu.SemaphoreType.REGULAR,
    ]
    experts_scratch = (
        [wide, wide, slots, slots, slots, slots, slots]
        + [pltpu.VMEM((experts, nz, rows, width), bf16)]
        + [pltpu.VMEM(w.shape, bf16) for w in weights]
        + [pltpu.VMEM((count, width), f32)] * 2
        + [sems(3), sems(2), sems(nz), sems(nz), sems(2, nz), sems(2, nz)]
        + [sems(nz)] * 10
        + [pltpu.SemaphoreType.DMA] * 2
    )
    assert len(front_scratch) == FRONT_SCRATCH
    return pl.pallas_call(
        functools.partial(layer_kernel, nz, nx, capacity),
        out_shape=jax.ShapeDtypeStruct((count, width), bf16),
        in_specs=[vmem] * 11 + [anywhere] + [vmem] * 5 + [anywhere] * 3,
        out_specs=vmem,
        scratch_shapes=[
            pltpu.VMEM((experts, nz, rows, width), bf16),
            pltpu.VMEM((count, width), bf16),
            pltpu.VMEM((2 * count, experts * nz * rows), f32),
        ]
        + front_scratch
        + experts_scratch,
        compiler_params=pltpu.CompilerParams(
            collective_id=1, has_side_effects=True, vmem_limit_bytes=60 << 20
        ),
        name="layer",
    )(*arrays)


def per_device(
    carryover_vector,
    channel_source_entries,
    final_modulation_vector,
    entering_basis_matrix,
    readout_basis_matrix,
    raw_stride_amount,
    extra_log_attenuation,
    channel_fading_rate,
    channel_source_kernel,
    entering_basis_kernel,
    readout_basis_kernel,
    modulated_rescaling_vector,
    blender_final_matrix,
    specialist_rescaling_vector,
    specialist_gating_matrices,
    widening_matrices,
    contracting_matrices,
    assigned_specialist_ids,
    specialist_choice_affinity,
    cluster_chance,
):
    nz, cores, nx = lax.axis_size("sp_0"), lax.axis_size("sp_1"), lax.axis_size("tp")
    row_count = carryover_vector.shape[0]
    local_experts = specialist_gating_matrices.shape[0]
    experts = nz * cores * local_experts
    picks = assigned_specialist_ids.shape[1]
    capacity = 2 * row_count * picks // experts
    return layer(
        nz,
        nx,
        capacity,
        channel_source_entries,
        final_modulation_vector,
        entering_basis_matrix,
        readout_basis_matrix,
        raw_stride_amount.T,
        extra_log_attenuation.T,
        channel_fading_rate[None, :],
        channel_source_kernel,
        entering_basis_kernel,
        readout_basis_kernel,
        modulated_rescaling_vector[None, :],
        blender_final_matrix,
        carryover_vector,
        specialist_rescaling_vector[None, :],
        assigned_specialist_ids.T,
        specialist_choice_affinity.T,
        cluster_chance[None, :],
        specialist_gating_matrices,
        widening_matrices,
        contracting_matrices,
    )


def solution(mesh):
    finer = Mesh(
        mesh.devices.reshape(mesh.shape["grp"], mesh.shape["sp"] // 2, 2, mesh.shape["tp"]),
        ("grp", "sp_0", "sp_1", "tp"),
    )
    return jax.shard_map(
        per_device,
        mesh=finer,
        in_specs=(
            P(GRP_SP_TP, None),
            P(GRP_SP, "tp"),
            P(GRP_SP, "tp"),
            P(GRP_SP, "tp"),
            P(GRP_SP, "tp"),
            P(GRP_SP, "tp"),
            P(GRP_SP, "tp"),
            P("tp"),
            P(None, "tp"),
            P(None, "tp"),
            P(None, "tp"),
            P(),
            P(),
            P(),
            P(SP, None, "tp"),
            P(SP, None, "tp"),
            P(SP, "tp", None),
            P(GRP_SP, None),
            P(GRP_SP_TP, None),
            P(GRP_SP_TP),
        ),
        out_specs=P(GRP_SP_TP, None),
        check_vma=False,
    )
```

```python
import functools

import jax
import jax.numpy as jnp
from jax import lax
from jax.experimental import pallas as pl
from jax.experimental.pallas import tpu as pltpu
from jax.sharding import Mesh
from jax.sharding import PartitionSpec as P

SP = ("sp_0", "sp_1")
GRP_SP_TP = ("grp", "sp_0", "sp_1", "tp")
GRP_SP = ("grp", "sp_0", "sp_1")


EPS = 1e-06


NEAR = 4


def hop(step, nz):
    step = jnp.where(step > NEAR, nz + NEAR - step, step)
    half = (step + 1) // 2
    return jnp.where(step % 2 == 1, half, -half)


def experts_kernel(
    nz,
    nx,
    src,
    gates_hbm,
    ups_hbm,
    downs_hbm,
    middle_ref,
    weight_ref,
    out_ref,
    arrived,
    part,
    far,
    near,
    both,
    mine,
    total,
    answers,
    gates,
    ups,
    downs,
    given,
    taken,
    load_sem,
    here,
    zs,
    zr,
    xs,
    xr,
    os_,
    or_,
    fs,
    fr,
    ns,
    nr,
    bs,
    br,
    ts,
    tr,
    ps,
    pr,
):
    z, c, x = lax.axis_index("sp_0"), lax.axis_index("sp_1"), lax.axis_index("tp")
    xp, xm = lax.rem(x + 1, nx), lax.rem(x + nx - 1, nx)
    x2 = lax.rem(x + 2, nx)
    local_experts, _, rows, width = src.shape
    f32, bf16 = jnp.float32, jnp.bfloat16
    loads = [
        pltpu.make_async_copy(a, b, load_sem.at[n])
        for n, (a, b) in enumerate(((gates_hbm, gates), (ups_hbm, ups), (downs_hbm, downs)))
    ]
    for load in loads:
        load.start()

    def goal(i):
        return lax.rem(z + hop(i, nz) + nz, nz)

    def origin(i):
        return lax.rem(z - hop(i, nz) + nz, nz)

    def ahead(i):
        return jnp.where(i % 2 == 0, xp, xm)

    def behind(i):
        return jnp.where(i % 2 == 0, xm, xp)

    def remote(a, b, sent, got, **to):
        return pltpu.make_async_remote_copy(a, b, sent, got, device_id=to)

    def along_z(i):
        return remote(src.at[:, goal(i)], arrived.at[i, :, x], zs.at[i], zr.at[i], sp_0=goal(i))

    def along_x(i, way):
        chunk = arrived.at[i, :, x]
        to = xp if way == 0 else xm
        return remote(chunk, chunk, xs.at[way, i], xr.at[way, i], tp=to)

    def from_x(i, way):
        chunk = arrived.at[i, :, jnp.where(way == 0, xm, xp)]
        return remote(chunk, chunk, xs.at[way, i], xr.at[way, i], tp=xp)

    def onward(i):
        chunk = arrived.at[i, :, behind(i)]
        return remote(chunk, chunk, os_.at[i], or_.at[i], tp=ahead(i))

    def from_far(i):
        chunk = arrived.at[i, :, x2]
        return remote(chunk, chunk, os_.at[i], or_.at[i], tp=xp)

    def send_far(i):
        return remote(part.at[i, :, x2], far.at[i], fs.at[i], fr.at[i], tp=ahead(i))

    def send_near(i):
        return remote(part.at[i, :, behind(i)], near.at[i], ns.at[i], nr.at[i], tp=behind(i))

    def send_both(i):
        return remote(mine.at[i], both.at[i], bs.at[i], br.at[i], tp=ahead(i))

    def send_back(i):
        return remote(total.at[i], answers.at[:, z], ts.at[i], tr.at[i], sp_0=origin(i))

    def send_z(i, carry):
        along_z(i).start()
        return carry

    lax.fori_loop(1, nz, send_z, 0)
    own = pltpu.make_async_copy(src.at[:, z], arrived.at[0, :, x], here.at[0])
    own.start()
    own.wait()

    def spread(i):
        along_x(i, 0).start()
        along_x(i, 1).start()

    def pass_on(i):
        from_x(i, i % 2).wait_recv()
        onward(i).start()

    def complete(i):
        from_x(i, (i + 1) % 2).wait_recv()
        from_far(i).wait_recv()

    def multiply(i):
        for e in range(local_experts):
            tokens = jnp.concatenate(
                [
                    arrived[i + k, e].astype(f32).reshape(nx * rows, width).astype(bf16)
                    for k in range(2)
                ],
                axis=0,
            )
            gate = jnp.dot(tokens, gates[e], preferred_element_type=f32)
            up = jnp.dot(tokens, ups[e], preferred_element_type=f32)
            hidden = (silu(gate) * up).astype(bf16)
            result = jnp.dot(hidden, downs[e], preferred_element_type=f32)
            for k in range(2):
                part[i + k, e] = (
                    result[k * nx * rows : (k + 1) * nx * rows].reshape(nx, rows, width).astype(bf16)
                )

    def first(i):
        send_far(i).start()
        send_near(i).start()

    def second(i):
        send_far(i).wait_recv()
        mine[i] = (part[i, :, ahead(i)].astype(f32) + far[i].astype(f32)).astype(bf16)
        send_both(i).start()

    def third(i):
        send_near(i).wait_recv()
        send_both(i).wait_recv()
        total[i] = (
            part[i, :, x].astype(f32) + near[i].astype(f32) + both[i].astype(f32)
        ).astype(bf16)

    pairs = nz // 2

    def turn(p, carry):
        i = 2 * p

        @pl.when(p == 0)
        def _():
            spread(0)

        @pl.when((p > 0) & (p < pairs))
        def _():
            remote(src.at[:, z], arrived.at[i, :, x], zs.at[i], zr.at[i], tp=xp).wait_recv()
            spread(i)

        @pl.when((p > 0) & (p <= pairs))
        def _():
            pass_on(i - 1)

        @pl.when(p < pairs)
        def _():
            remote(src.at[:, z], arrived.at[i + 1, :, x], zs.at[i + 1], zr.at[i + 1], tp=xp).wait_recv()
            spread(i + 1)
            pass_on(i)

        @pl.when(p == 1)
        def _():
            for load in loads:
                load.wait()

        @pl.when((p > 0) & (p <= pairs))
        def _():
            complete(i - 2)
            complete(i - 1)
            multiply(i - 2)
            first(i - 2)
            first(i - 1)

        @pl.when((p > 1) & (p <= pairs + 1))
        def _():
            second(i - 4)
            second(i - 3)

        @pl.when(p > 2)
        def _():
            third(i - 6)
            third(i - 5)

            @pl.when(p > 3)
            def _():
                send_back(i - 6).start()

            send_back(i - 5).start()

        return carry

    lax.fori_loop(0, pairs + 3, turn, 0)
    own_back = pltpu.make_async_copy(total.at[0], answers.at[:, z], here.at[1])
    own_back.start()
    own_back.wait()

    def sent(i, carry):
        along_x(i, 0).wait_send()
        along_x(i, 1).wait_send()
        onward(i).wait_send()
        send_far(i).wait_send()
        send_near(i).wait_send()
        send_both(i).wait_send()
        return carry

    lax.fori_loop(0, nz, sent, 0)

    def returned(i, carry):
        along_z(i).wait_send()
        send_back(i).wait_send()
        remote(total.at[i], answers.at[:, goal(i)], ts.at[i], tr.at[i], tp=xp).wait_recv()
        return carry

    lax.fori_loop(1, nz, returned, 0)

    count = out_ref.shape[0]
    slots = local_experts * nz * rows
    known = answers[...].astype(f32).reshape(slots, width).astype(bf16)

    def shared(start):
        weight = weight_ref[pl.ds(pl.multiple_of(start * count, count), count), :]
        high = weight.astype(bf16)
        low = (weight - high.astype(f32)).astype(bf16)
        return jnp.dot(high, known, preferred_element_type=f32) + jnp.dot(
            low, known, preferred_element_type=f32
        )

    given[...] = shared(1 - c)
    swap = remote(given, taken, ps, pr, sp_1=1 - c)
    swap.start()
    kept = middle_ref[...].astype(f32) + shared(c)
    swap.wait()
    out_ref[...] = (kept + taken[...]).astype(bf16)


QUAD = 4
TAIL = 16


def announce(nz, nx):
    z, c, x = lax.axis_index("sp_0"), lax.axis_index("sp_1"), lax.axis_index("tp")
    place, quad = lax.rem(z, QUAD), z // QUAD
    barrier = pltpu.get_barrier_semaphore()
    beyond = z + 2 * c - 1
    has_beyond = (beyond >= 0) & (beyond < nz)
    before = (place == 0) & (quad > 0)
    behind = (place == QUAD - 1) & (quad < nz // QUAD - 1)

    def in_quad(k, carry):
        to = quad * QUAD + lax.rem(place + k, QUAD)
        pl.semaphore_signal(barrier, inc=1, device_id={"sp_0": to})
        return carry

    def along_x(k, carry):
        pl.semaphore_signal(barrier, inc=1, device_id={"tp": lax.rem(x + k, nx)})
        return carry

    pl.semaphore_signal(barrier, inc=1, device_id={"sp_1": 1 - c})
    lax.fori_loop(1, QUAD, in_quad, 0)
    lax.fori_loop(1, nx, along_x, 0)

    @pl.when(has_beyond)
    def _():
        pl.semaphore_signal(barrier, inc=1, device_id={"sp_0": beyond, "sp_1": 1 - c})

    @pl.when(before)
    def _():
        pl.semaphore_signal(barrier, inc=1, device_id={"sp_0": z - 1})

    @pl.when(behind)
    def _():
        pl.semaphore_signal(barrier, inc=1, device_id={"sp_0": z + 1})

    return QUAD + nx - 1 + sum(flag.astype(jnp.int32) for flag in (has_beyond, before, behind))


def pass_word(nz, token, ready):
    z = lax.axis_index("sp_0")
    place, quad = lax.rem(z, QUAD), z // QUAD
    last = nz // QUAD - 1

    @pl.when((place == 0) & (quad > 0))
    def _():
        pl.semaphore_wait(token, 1)

    @pl.when((place == 0) & (quad < last))
    def _():
        pl.semaphore_signal(token, inc=1, device_id={"sp_0": z + QUAD - 1})

    @pl.when((place == QUAD - 1) & (quad < last))
    def _():
        pl.semaphore_wait(token, 1)
        pl.semaphore_signal(token, inc=1, device_id={"sp_0": z + 1})

    @pl.when((place == 0) & (quad == last))
    def _():
        def tell(k, carry):
            pl.semaphore_signal(ready, inc=1, device_id={"sp_0": lax.rem(z + k, nz)})
            return carry

        lax.fori_loop(1, nz, tell, 0)


def silu(v):
    return v * jax.nn.sigmoid(v)


def exact_dot(a, b):
    return jnp.dot(a, b, preferred_element_type=jnp.float32, precision=lax.Precision.HIGHEST)


def packed(state, decays):
    lanes = state.shape[1]
    row = lax.broadcasted_iota(jnp.int32, (TAIL, lanes), 0)
    tail = jnp.zeros((TAIL, lanes), jnp.float32)
    for h, decay in enumerate(decays):
        wide = jnp.broadcast_to(decay, (TAIL, lanes))
        high = wide.astype(jnp.bfloat16).astype(jnp.float32)
        tail = jnp.where(row == h, high, tail)
        tail = jnp.where(row == TAIL // 2 + h, wide - high, tail)
    return jnp.concatenate([state.astype(jnp.bfloat16), tail.astype(jnp.bfloat16)], axis=0)


def unpacked(message, heads):
    rows = message.shape[0] - TAIL
    state = message[:rows].astype(jnp.float32)
    tail = message[rows:].astype(jnp.float32)
    half = TAIL // 2
    return state, [tail[h : h + 1, 0:1] + tail[half + h : half + h + 1, 0:1] for h in range(heads)]


def per_row(decays, rows, lanes):
    each = rows // len(decays)
    return jnp.concatenate([jnp.broadcast_to(d, (each, lanes)) for d in decays], axis=0)


def followed(earlier, later):
    (state_a, decay_a), (state_b, decay_b) = earlier, later
    state = state_a * per_row(decay_b, *state_a.shape) + state_b
    return state, [a * b for a, b in zip(decay_a, decay_b)]


def chosen(flag, one, other):
    return jnp.where(flag, one[0], other[0]), [
        jnp.where(flag, a, b) for a, b in zip(one[1], other[1])
    ]


def front_kernel(
    nz,
    nx,
    capacity,
    xs_ref,
    gate_ref,
    keys_ref,
    queries_ref,
    raw_ref,
    extra_ref,
    rate_ref,
    taps_x_ref,
    taps_k_ref,
    taps_q_ref,
    gain_ref,
    blend_hbm,
    carry_ref,
    gain2_ref,
    ids_ref,
    affinity_ref,
    chance_ref,
    outgoing_ref,
    middle_ref,
    weight_ref,
    halo,
    joined,
    pair_out,
    pair_in,
    quad_out,
    quad_in,
    far_out,
    far_in,
    half_out,
    half_in,
    gated_out,
    gated_in,
    facts,
    rows,
    blend,
    turned,
    smooth,
    fading,
    blend_sem,
    halo_s,
    halo_r,
    pair_s,
    pair_r,
    quad_s,
    quad_r,
    far_s,
    far_r,
    gated_s,
    gated_r,
    token,
    following,
    ready,
):
    z, c, x = lax.axis_index("sp_0"), lax.axis_index("sp_1"), lax.axis_index("tp")
    length, width_x = xs_ref.shape
    state_width = keys_ref.shape[1]
    heads = raw_ref.shape[0]
    head_dim = width_x // heads
    half_heads = heads // 2
    half_rows = width_x // 2
    place, quad = lax.rem(z, QUAD), z // QUAD
    quads = nz // QUAD
    f32, bf16 = jnp.float32, jnp.bfloat16
    partner = {"sp_1": 1 - c}
    greeted = announce(nz, nx)
    load = pltpu.make_async_copy(blend_hbm, blend, blend_sem)
    load.start()

    stride_row = jnp.maximum(raw_ref[...], 0.0) + jnp.log1p(jnp.exp(-jnp.abs(raw_ref[...])))
    diagonal = lax.broadcasted_iota(jnp.int32, (heads, heads), 0) == lax.broadcasted_iota(
        jnp.int32, (heads, heads), 1
    )
    rate = jnp.sum(
        jnp.where(diagonal, jnp.broadcast_to(rate_ref[...], (heads, heads)), 0.0),
        axis=1,
        keepdims=True,
    )
    log_row = extra_ref[...] - rate * stride_row
    t_axis = lax.broadcasted_iota(jnp.int32, (length, length), 0)
    s_axis = lax.broadcasted_iota(jnp.int32, (length, length), 1)
    causal = t_axis >= s_axis
    running_row = exact_dot(
        jnp.concatenate([log_row, jnp.zeros_like(log_row)], axis=0), (t_axis <= s_axis).astype(f32)
    )
    picks = ids_ref.shape[0]
    count = ids_ref.shape[1] // nx
    lanes = 128
    stacked = jnp.concatenate(
        [
            running_row[:heads],
            stride_row,
            ids_ref[...].astype(f32),
            jnp.zeros((lanes - 2 * heads - picks, length), f32),
        ],
        axis=0,
    )
    turned[...] = stacked.T
    running = turned[:, :heads]
    stride = turned[:, heads : 2 * heads]
    final = running[length - 1 : length, :]
    lifted = jnp.exp(affinity_ref[...])
    share_row = chance_ref[...] * lifted / jnp.sum(lifted, axis=0, keepdims=True)
    share_row = jnp.concatenate([share_row, jnp.zeros((lanes - picks, count), f32)], axis=0)
    share_row = jnp.concatenate([share_row, jnp.zeros((lanes, lanes - count), f32)], axis=1)
    shares = share_row.T[:count]
    local_experts = outgoing_ref.shape[0]
    experts = nz * 2 * local_experts
    ids = turned[pl.ds(pl.multiple_of(x * count, count), count), :]
    ids = ids[:, 2 * heads : 2 * heads + picks].astype(jnp.int32)
    expert_axis = lax.broadcasted_iota(jnp.int32, (count, experts), 1)
    member = [(ids[:, k : k + 1] == expert_axis).astype(f32) for k in range(picks)]
    row_axis = lax.broadcasted_iota(jnp.int32, (count, count), 0)
    column_axis = lax.broadcasted_iota(jnp.int32, (count, count), 1)
    earlier = (row_axis > column_axis).astype(bf16)
    before = jnp.dot(earlier, sum(member).astype(bf16), preferred_element_type=f32)
    lane = lax.broadcasted_iota(jnp.int32, (count, facts.shape[2]), 1)
    noted = jnp.zeros((count, facts.shape[2]), f32)
    for k in range(picks):
        position = jnp.sum(before * member[k], axis=1, keepdims=True)
        expert = ids[:, k : k + 1]
        holder = lax.div(expert, local_experts)
        slot = (
            (lax.rem(expert, local_experts) * nz + lax.div(holder, 2)) * 2 + c
        ) * capacity + position.astype(jnp.int32)
        for core in range(2):
            there = jnp.where(lax.rem(holder, 2) == core, slot, -1).astype(f32)
            noted = jnp.where(lane == core * picks + k, there, noted)
        noted = jnp.where(lane == 2 * picks + k, shares[:, k : k + 1], noted)
    facts[c] = noted

    rim = halo.shape[0]
    start = 0
    for ref in (xs_ref, keys_ref, queries_ref):
        joined[rim:, start : start + ref.shape[1]] = ref[...].astype(f32)
        start += ref.shape[1]
    taps = jnp.concatenate([taps_x_ref[...], taps_k_ref[...], taps_q_ref[...]], axis=1)
    kernel_len = taps.shape[0]

    def convolve(begin, end):
        start = rim - kernel_len + 1
        total = taps[0:1, :] * joined[start + begin : start + end, :]
        for tap in range(1, kernel_len):
            total = total + taps[tap : tap + 1, :] * joined[start + tap + begin : start + tap + end, :]
        return silu(total)

    smooth[rim:, :] = convolve(rim, length)
    modulation = silu(gate_ref[...].astype(f32))
    for h in range(heads):
        between = running[:, h : h + 1] - running_row[h : h + 1, :]
        fading[h] = jnp.exp(jnp.where(causal, between, -1e30))

    pl.semaphore_wait(pltpu.get_barrier_semaphore(), greeted)

    @pl.when((place == 0) & (quad > 0))
    def _():
        pl.semaphore_signal(following, inc=1, device_id={"sp_0": z - 1})

    after = {"sp_0": lax.rem(z + c, nz), "sp_1": 1 - c}
    edges = []
    start = 0
    for n, ref in enumerate((xs_ref, keys_ref, queries_ref)):
        columns = pl.ds(start, ref.shape[1])
        edges.append(
            pltpu.make_async_remote_copy(
                ref.at[pl.ds(length - rim, rim)],
                halo.at[:, columns],
                halo_s.at[n],
                halo_r.at[n],
                device_id=after,
            )
        )
        start += ref.shape[1]

    @pl.when(z + c < nz)
    def _():
        for edge in edges:
            edge.start()

    facts_copy = pltpu.make_async_remote_copy(
        facts.at[c], facts.at[c], pair_s.at[0], pair_r.at[0], device_id=partner
    )
    facts_copy.start()

    @pl.when(z + c > 0)
    def _():
        for edge in edges:
            edge.wait_recv()
        joined[:rim, :] = halo[...].astype(f32)

    @pl.when(z + c == 0)
    def _():
        joined[:rim, :] = jnp.zeros_like(joined[:rim, :])

    smooth[:rim, :] = convolve(0, rim)
    inputs_x = smooth[:, :width_x]
    keys_b = smooth[:, width_x : width_x + state_width].astype(bf16)
    queries_c = smooth[:, width_x + state_width :].astype(bf16)

    scaled = [
        inputs_x[:, h * head_dim : (h + 1) * head_dim] * stride[:, h : h + 1] for h in range(heads)
    ]
    remaining = jnp.concatenate(
        [scaled[h] * jnp.exp(final[:, h : h + 1] - running[:, h : h + 1]) for h in range(heads)],
        axis=1,
    ).astype(bf16)
    own_state = lax.dot_general(
        remaining, keys_b, (((0,), (0,)), ((), ())), preferred_element_type=f32
    )
    pair_out[...] = packed(own_state, [jnp.exp(final[:, h : h + 1]) for h in range(heads)])
    pair_copy = pltpu.make_async_remote_copy(
        pair_out, pair_in, pair_s.at[1], pair_r.at[1], device_id=partner
    )
    pair_copy.start()

    scores = lax.dot_general(
        queries_c, keys_b, (((1,), (1,)), ((), ())), preferred_element_type=f32
    )
    inside = []
    for h in range(heads):
        inside.append(
            jnp.dot(
                (scores * fading[h]).astype(bf16), scaled[h].astype(bf16), preferred_element_type=f32
            )
        )

    pair_copy.wait_recv()

    def half_of(ref):
        state, decays = unpacked(ref[...], heads)
        return (
            jnp.where(c == 0, state[:half_rows], state[half_rows:]),
            [jnp.where(c == 0, decays[j], decays[half_heads + j]) for j in range(half_heads)],
        )

    ours, theirs = half_of(pair_out), half_of(pair_in)
    lower, upper = chosen(c == 0, ours, theirs), chosen(c == 0, theirs, ours)
    chip = followed(lower, upper)
    quad_out[...] = packed(*chip)

    def quad_send(k):
        to = quad * QUAD + lax.rem(place + k, QUAD)
        return pltpu.make_async_remote_copy(
            quad_out, quad_in.at[place], quad_s.at[k], quad_r.at[k], device_id={"sp_0": to}
        )

    def quad_arrival(k):
        return pltpu.make_async_remote_copy(
            quad_out,
            quad_in.at[lax.rem(place + QUAD - k, QUAD)],
            quad_s.at[k],
            quad_r.at[k],
            device_id={"sp_0": lax.rem(z + 1, nz)},
        )

    for k in range(1, QUAD):

        @pl.when(place + k < QUAD)
        def _(k=k):
            quad_send(k).start()

    pass_word(nz, token, ready)
    for k in range(1, QUAD):

        @pl.when(place >= k)
        def _(k=k):
            quad_arrival(k).wait_recv()

        @pl.when(place < k)
        def _(k=k):
            quad_in[k - 1] = jnp.zeros_like(quad_out)

    nothing = (jnp.zeros_like(chip[0]), [jnp.ones_like(d) for d in chip[1]])
    inner = nothing
    for k in range(QUAD - 1):
        inner = chosen(k < place, followed(inner, unpacked(quad_in[k], half_heads)), inner)

    def far_send(k):
        return pltpu.make_async_remote_copy(
            far_out,
            far_in,
            far_s.at[k],
            far_r,
            device_id={"sp_0": lax.rem(z + 1 + k, nz)},
        )

    @pl.when(quad > 0)
    def _():
        far_send(0).wait_recv()

    @pl.when(quad == 0)
    def _():
        far_in[...] = jnp.zeros_like(far_in)

    incoming = followed((far_in[...].astype(f32), nothing[1]), inner)
    incoming_low = incoming[0]
    leads_on = (place == QUAD - 1) & (quad < quads - 1)

    @pl.when(leads_on)
    def _():
        far_out[...] = followed(incoming, chip)[0].astype(bf16)
        pl.semaphore_wait(following, 1)
        for k in range(QUAD):
            far_send(k).start()

    incoming_high = followed(incoming, lower)[0]
    half_out[...] = jnp.where(c == 0, incoming_high, incoming_low).astype(bf16)
    half_copy = pltpu.make_async_remote_copy(
        half_out, half_in, pair_s.at[2], pair_r.at[2], device_id=partner
    )
    half_copy.start()
    kept = jnp.where(c == 0, incoming_low, incoming_high).astype(bf16)
    half_copy.wait_recv()
    sent_in = half_in[...]
    entering = jnp.concatenate(
        [jnp.where(c == 0, kept, sent_in), jnp.where(c == 0, sent_in, kept)], axis=0
    )
    outside = lax.dot_general(
        queries_c, entering, (((1,), (1,)), ((), ())), preferred_element_type=f32
    )
    mixed = jnp.concatenate(
        [
            inside[h]
            + outside[:, h * head_dim : (h + 1) * head_dim] * jnp.exp(running[:, h : h + 1])
            for h in range(heads)
        ],
        axis=1,
    )
    gated_out[...] = (mixed * modulation).astype(bf16).reshape(gated_out.shape)

    def gated_send(k):
        to = lax.rem(x + k, nx)
        return pltpu.make_async_remote_copy(
            gated_out.at[to], gated_in.at[x], gated_s.at[k], gated_r.at[k], device_id={"tp": to}
        )

    for k in range(1, nx):
        gated_send(k).start()
    gated_in[x] = gated_out[x]
    facts_arrival = pltpu.make_async_remote_copy(
        facts.at[1 - c], facts.at[1 - c], pair_s.at[0], pair_r.at[0], device_id=partner
    )
    facts_arrival.wait_recv()
    slot_count = weight_ref.shape[1]
    slot_axis = lax.broadcasted_iota(jnp.int32, (2 * count, slot_count), 1).astype(f32)
    known = jnp.concatenate([facts[0], facts[1]], axis=0)
    picked = jnp.zeros((2 * count, slot_count), f32)
    weight = jnp.zeros((2 * count, slot_count), f32)
    for k in range(picks):
        slot = jnp.where(c == 0, known[:, k : k + 1], known[:, picks + k : picks + k + 1])
        hit = slot == slot_axis
        picked = jnp.where(hit, 1.0, picked)
        weight = jnp.where(hit, known[:, 2 * picks + k : 2 * picks + k + 1], weight)
    weight_ref[...] = weight
    for k in range(1, nx):
        pltpu.make_async_remote_copy(
            gated_out.at[x],
            gated_in.at[lax.rem(x + nx - k, nx)],
            gated_s.at[k],
            gated_r.at[k],
            device_id={"tp": lax.rem(x + k, nx)},
        ).wait_recv()
    own_rows = jnp.concatenate([gated_in[k] for k in range(nx)], axis=1).astype(f32)
    normed = (
        own_rows
        * lax.rsqrt(jnp.mean(own_rows * own_rows, axis=1, keepdims=True) + EPS)
        * gain_ref[...]
    ).astype(bf16)
    load.wait()
    middle = (
        carry_ref[...].astype(f32) + jnp.dot(normed, blend[...], preferred_element_type=f32)
    ).astype(bf16)
    middle_ref[...] = middle
    wide = middle.astype(f32)
    rows[c] = (
        wide
        * lax.rsqrt(jnp.mean(wide * wide, axis=1, keepdims=True) + EPS)
        * gain2_ref[...]
    ).astype(bf16)
    rows_copy = pltpu.make_async_remote_copy(
        rows.at[c], rows.at[c], pair_s.at[3], pair_r.at[3], device_id=partner
    )
    rows_copy.start()
    pltpu.make_async_remote_copy(
        rows.at[1 - c], rows.at[1 - c], pair_s.at[3], pair_r.at[3], device_id=partner
    ).wait_recv()
    outgoing_ref[...] = (
        lax.dot_general(
            picked.astype(bf16),
            jnp.concatenate([rows[0], rows[1]], axis=0),
            (((0,), (0,)), ((), ())),
            preferred_element_type=f32,
        )
        .astype(bf16)
        .reshape(outgoing_ref.shape)
    )


    @pl.when(z + c < nz)
    def _():
        for edge in edges:
            edge.wait_send()

    facts_copy.wait_send()
    pair_copy.wait_send()
    half_copy.wait_send()
    rows_copy.wait_send()
    for k in range(1, QUAD):

        @pl.when(place + k < QUAD)
        def _(k=k):
            quad_send(k).wait_send()

    @pl.when(leads_on)
    def _():
        for k in range(QUAD):
            far_send(k).wait_send()

    for k in range(1, nx):
        gated_send(k).wait_send()

    @pl.when((place > 0) | (quad < quads - 1))
    def _():
        pl.semaphore_wait(ready, 1)


FRONT_INPUTS = 17
FRONT_SCRATCH = 32


def layer_kernel(nz, nx, capacity, *refs):
    inputs, refs = refs[:FRONT_INPUTS], refs[FRONT_INPUTS:]
    weights, out_ref, refs = refs[:3], refs[3], refs[4:]
    outgoing, middle, weight, refs = *refs[:3], refs[3:]
    front_kernel(nz, nx, capacity, *inputs, outgoing, middle, weight, *refs[:FRONT_SCRATCH])
    experts_kernel(nz, nx, outgoing, *weights, middle, weight, out_ref, *refs[FRONT_SCRATCH:])


def layer(nz, nx, capacity, *arrays):
    xs, _, keys, queries, raw = arrays[:5]
    blend, carry = arrays[11:13]
    weights = arrays[FRONT_INPUTS:]
    experts = weights[0].shape[0]
    count, width = carry.shape
    rows = 2 * capacity
    channels, states = xs.shape[1], keys.shape[1]
    total = channels + states + queries.shape[1]
    rim = 8
    half = channels // 2
    bf16, f32 = jnp.bfloat16, jnp.float32
    vmem = pl.BlockSpec(memory_space=pltpu.VMEM)
    anywhere = pl.BlockSpec(memory_space=pl.ANY)
    slots = pltpu.VMEM((nz, experts, rows, width), bf16)
    wide = pltpu.VMEM((nz, experts, nx, rows, width), bf16)

    def sems(*shape):
        return pltpu.SemaphoreType.DMA(shape)

    front_scratch = [
        pltpu.VMEM((rim, total), bf16),
        pltpu.VMEM((rim + xs.shape[0], total), f32),
        pltpu.VMEM((channels + TAIL, states), bf16),
        pltpu.VMEM((channels + TAIL, states), bf16),
        pltpu.VMEM((half + TAIL, states), bf16),
        pltpu.VMEM((QUAD, half + TAIL, states), bf16),
        pltpu.VMEM((half, states), bf16),
        pltpu.VMEM((half, states), bf16),
        pltpu.VMEM((half, states), bf16),
        pltpu.VMEM((half, states), bf16),
        pltpu.VMEM((nx, count, channels), bf16),
        pltpu.VMEM((nx, count, channels), bf16),
        pltpu.VMEM((2, count, 128), f32),
        pltpu.VMEM((2, count, width), bf16),
        pltpu.VMEM(blend.shape, bf16),
        pltpu.VMEM((xs.shape[0], 128), f32),
        pltpu.VMEM((xs.shape[0], total), f32),
        pltpu.VMEM((raw.shape[0], xs.shape[0], xs.shape[0]), f32),
        pltpu.SemaphoreType.DMA,
        sems(3),
        sems(3),
        sems(4),
        sems(4),
        sems(QUAD),
        sems(QUAD),
        sems(QUAD),
        pltpu.SemaphoreType.DMA,
        sems(nx),
        sems(nx),
        pltpu.SemaphoreType.REGULAR,
        pltpu.SemaphoreType.REGULAR,
        pltpu.SemaphoreType.REGULAR,
    ]
    experts_scratch = (
        [wide, wide, slots, slots, slots, slots, slots]
        + [pltpu.VMEM((experts, nz, rows, width), bf16)]
        + [pltpu.VMEM(w.shape, bf16) for w in weights]
        + [pltpu.VMEM((count, width), f32)] * 2
        + [sems(3), sems(2), sems(nz), sems(nz), sems(2, nz), sems(2, nz)]
        + [sems(nz)] * 10
        + [pltpu.SemaphoreType.DMA] * 2
    )
    assert len(front_scratch) == FRONT_SCRATCH
    return pl.pallas_call(
        functools.partial(layer_kernel, nz, nx, capacity),
        out_shape=jax.ShapeDtypeStruct((count, width), bf16),
        in_specs=[vmem] * 11 + [anywhere] + [vmem] * 5 + [anywhere] * 3,
        out_specs=vmem,
        scratch_shapes=[
            pltpu.VMEM((experts, nz, rows, width), bf16),
            pltpu.VMEM((count, width), bf16),
            pltpu.VMEM((2 * count, experts * nz * rows), f32),
        ]
        + front_scratch
        + experts_scratch,
        compiler_params=pltpu.CompilerParams(
            collective_id=1, has_side_effects=True, vmem_limit_bytes=60 << 20
        ),
        name="layer",
    )(*arrays)


def per_device(
    carryover_vector,
    channel_source_entries,
    final_modulation_vector,
    entering_basis_matrix,
    readout_basis_matrix,
    raw_stride_amount,
    extra_log_attenuation,
    channel_fading_rate,
    channel_source_kernel,
    entering_basis_kernel,
    readout_basis_kernel,
    modulated_rescaling_vector,
    blender_final_matrix,
    specialist_rescaling_vector,
    specialist_gating_matrices,
    widening_matrices,
    contracting_matrices,
    assigned_specialist_ids,
    specialist_choice_affinity,
    cluster_chance,
):
    nz, cores, nx = lax.axis_size("sp_0"), lax.axis_size("sp_1"), lax.axis_size("tp")
    row_count = carryover_vector.shape[0]
    local_experts = specialist_gating_matrices.shape[0]
    experts = nz * cores * local_experts
    picks = assigned_specialist_ids.shape[1]
    capacity = 2 * row_count * picks // experts
    return layer(
        nz,
        nx,
        capacity,
        channel_source_entries,
        final_modulation_vector,
        entering_basis_matrix,
        readout_basis_matrix,
        raw_stride_amount.T,
        extra_log_attenuation.T,
        channel_fading_rate[None, :],
        channel_source_kernel,
        entering_basis_kernel,
        readout_basis_kernel,
        modulated_rescaling_vector[None, :],
        blender_final_matrix,
        carryover_vector,
        specialist_rescaling_vector[None, :],
        assigned_specialist_ids.T,
        specialist_choice_affinity.T,
        cluster_chance[None, :],
        specialist_gating_matrices,
        widening_matrices,
        contracting_matrices,
    )


def solution(mesh):
    finer = Mesh(
        mesh.devices.reshape(mesh.shape["grp"], mesh.shape["sp"] // 2, 2, mesh.shape["tp"]),
        ("grp", "sp_0", "sp_1", "tp"),
    )
    return jax.shard_map(
        per_device,
        mesh=finer,
        in_specs=(
            P(GRP_SP_TP, None),
            P(GRP_SP, "tp"),
            P(GRP_SP, "tp"),
            P(GRP_SP, "tp"),
            P(GRP_SP, "tp"),
            P(GRP_SP, "tp"),
            P(GRP_SP, "tp"),
            P("tp"),
            P(None, "tp"),
            P(None, "tp"),
            P(None, "tp"),
            P(),
            P(),
            P(),
            P(SP, None, "tp"),
            P(SP, None, "tp"),
            P(SP, "tp", None),
            P(GRP_SP, None),
            P(GRP_SP_TP, None),
            P(GRP_SP_TP),
        ),
        out_specs=P(GRP_SP_TP, None),
        check_vma=False,
    )
```

```python
import functools

import jax
import jax.numpy as jnp
from jax import lax
from jax.experimental import pallas as pl
from jax.experimental.pallas import tpu as pltpu
from jax.sharding import Mesh
from jax.sharding import PartitionSpec as P

SP = ("sp_0", "sp_1")
GRP_SP_TP = ("grp", "sp_0", "sp_1", "tp")
GRP_SP = ("grp", "sp_0", "sp_1")


EPS = 1e-06


NEAR = 4


def hop(step, nz):
    step = jnp.where(step > NEAR, nz + NEAR - step, step)
    half = (step + 1) // 2
    return jnp.where(step % 2 == 1, half, -half)


def experts_kernel(
    nz,
    nx,
    src,
    gates_hbm,
    ups_hbm,
    downs_hbm,
    middle_ref,
    weight_ref,
    out_ref,
    arrived,
    part,
    far,
    near,
    both,
    mine,
    total,
    answers,
    gates,
    ups,
    downs,
    given,
    taken,
    load_sem,
    here,
    zs,
    zr,
    xs,
    xr,
    os_,
    or_,
    fs,
    fr,
    ns,
    nr,
    bs,
    br,
    ts,
    tr,
    ps,
    pr,
):
    z, c, x = lax.axis_index("sp_0"), lax.axis_index("sp_1"), lax.axis_index("tp")
    xp, xm = lax.rem(x + 1, nx), lax.rem(x + nx - 1, nx)
    x2 = lax.rem(x + 2, nx)
    local_experts, _, rows, width = src.shape
    f32, bf16 = jnp.float32, jnp.bfloat16
    loads = [
        pltpu.make_async_copy(a, b, load_sem.at[n])
        for n, (a, b) in enumerate(((gates_hbm, gates), (ups_hbm, ups), (downs_hbm, downs)))
    ]
    for load in loads:
        load.start()

    def goal(i):
        return lax.rem(z + hop(i, nz) + nz, nz)

    def origin(i):
        return lax.rem(z - hop(i, nz) + nz, nz)

    def ahead(i):
        return jnp.where(i % 2 == 0, xp, xm)

    def behind(i):
        return jnp.where(i % 2 == 0, xm, xp)

    def remote(a, b, sent, got, **to):
        return pltpu.make_async_remote_copy(a, b, sent, got, device_id=to)

    def along_z(i):
        return remote(src.at[:, goal(i)], arrived.at[i, :, x], zs.at[i], zr.at[i], sp_0=goal(i))

    def along_x(i, way):
        chunk = arrived.at[i, :, x]
        to = xp if way == 0 else xm
        return remote(chunk, chunk, xs.at[way, i], xr.at[way, i], tp=to)

    def from_x(i, way):
        chunk = arrived.at[i, :, jnp.where(way == 0, xm, xp)]
        return remote(chunk, chunk, xs.at[way, i], xr.at[way, i], tp=xp)

    def onward(i):
        chunk = arrived.at[i, :, behind(i)]
        return remote(chunk, chunk, os_.at[i], or_.at[i], tp=ahead(i))

    def from_far(i):
        chunk = arrived.at[i, :, x2]
        return remote(chunk, chunk, os_.at[i], or_.at[i], tp=xp)

    def send_far(i):
        return remote(part.at[i, :, x2], far.at[i], fs.at[i], fr.at[i], tp=ahead(i))

    def send_near(i):
        return remote(part.at[i, :, behind(i)], near.at[i], ns.at[i], nr.at[i], tp=behind(i))

    def send_both(i):
        return remote(mine.at[i], both.at[i], bs.at[i], br.at[i], tp=ahead(i))

    def send_back(i):
        return remote(total.at[i], answers.at[:, z], ts.at[i], tr.at[i], sp_0=origin(i))

    def send_z(i, carry):
        along_z(i).start()
        return carry

    lax.fori_loop(1, nz, send_z, 0)
    own = pltpu.make_async_copy(src.at[:, z], arrived.at[0, :, x], here.at[0])
    own.start()
    own.wait()

    def spread(i):
        along_x(i, 0).start()
        along_x(i, 1).start()

    def pass_on(i):
        from_x(i, i % 2).wait_recv()
        onward(i).start()

    def complete(i):
        from_x(i, (i + 1) % 2).wait_recv()
        from_far(i).wait_recv()

    def multiply(i):
        for e in range(local_experts):
            tokens = jnp.concatenate(
                [
                    arrived[i + k, e].astype(f32).reshape(nx * rows, width).astype(bf16)
                    for k in range(2)
                ],
                axis=0,
            )
            gate = jnp.dot(tokens, gates[e], preferred_element_type=f32)
            up = jnp.dot(tokens, ups[e], preferred_element_type=f32)
            hidden = (silu(gate) * up).astype(bf16)
            result = jnp.dot(hidden, downs[e], preferred_element_type=f32)
            for k in range(2):
                part[i + k, e] = (
                    result[k * nx * rows : (k + 1) * nx * rows].reshape(nx, rows, width).astype(bf16)
                )

    def first(i):
        send_far(i).start()
        send_near(i).start()

    def second(i):
        send_far(i).wait_recv()
        mine[i] = (part[i, :, ahead(i)].astype(f32) + far[i].astype(f32)).astype(bf16)
        send_both(i).start()

    def third(i):
        send_near(i).wait_recv()
        send_both(i).wait_recv()
        total[i] = (
            part[i, :, x].astype(f32) + near[i].astype(f32) + both[i].astype(f32)
        ).astype(bf16)

    pairs = nz // 2

    def turn(p, carry):
        i = 2 * p

        @pl.when(p == 0)
        def _():
            spread(0)

        @pl.when((p > 0) & (p < pairs))
        def _():
            remote(src.at[:, z], arrived.at[i, :, x], zs.at[i], zr.at[i], tp=xp).wait_recv()
            spread(i)

        @pl.when((p > 0) & (p <= pairs))
        def _():
            pass_on(i - 1)

        @pl.when(p < pairs)
        def _():
            remote(src.at[:, z], arrived.at[i + 1, :, x], zs.at[i + 1], zr.at[i + 1], tp=xp).wait_recv()
            spread(i + 1)
            pass_on(i)

        @pl.when(p == 1)
        def _():
            for load in loads:
                load.wait()

        @pl.when(p > 1)
        def _():
            second(i - 4)
            second(i - 3)

        @pl.when((p > 0) & (p <= pairs))
        def _():
            complete(i - 2)
            complete(i - 1)
            multiply(i - 2)
            first(i - 2)
            first(i - 1)

        @pl.when(p > 1)
        def _():
            third(i - 4)
            third(i - 3)

            @pl.when(p > 2)
            def _():
                send_back(i - 4).start()

            send_back(i - 3).start()

        return carry

    lax.fori_loop(0, pairs + 2, turn, 0)
    own_back = pltpu.make_async_copy(total.at[0], answers.at[:, z], here.at[1])
    own_back.start()
    own_back.wait()

    def sent(i, carry):
        along_x(i, 0).wait_send()
        along_x(i, 1).wait_send()
        onward(i).wait_send()
        send_far(i).wait_send()
        send_near(i).wait_send()
        send_both(i).wait_send()
        return carry

    lax.fori_loop(0, nz, sent, 0)

    def returned(i, carry):
        along_z(i).wait_send()
        send_back(i).wait_send()
        remote(total.at[i], answers.at[:, goal(i)], ts.at[i], tr.at[i], tp=xp).wait_recv()
        return carry

    lax.fori_loop(1, nz, returned, 0)

    count = out_ref.shape[0]
    slots = local_experts * nz * rows
    known = answers[...].astype(f32).reshape(slots, width).astype(bf16)

    def shared(start):
        weight = weight_ref[pl.ds(pl.multiple_of(start * count, count), count), :]
        high = weight.astype(bf16)
        low = (weight - high.astype(f32)).astype(bf16)
        return jnp.dot(high, known, preferred_element_type=f32) + jnp.dot(
            low, known, preferred_element_type=f32
        )

    given[...] = shared(1 - c)
    swap = remote(given, taken, ps, pr, sp_1=1 - c)
    swap.start()
    kept = middle_ref[...].astype(f32) + shared(c)
    swap.wait()
    out_ref[...] = (kept + taken[...]).astype(bf16)


QUAD = 4
TAIL = 16


def announce(nz, nx):
    z, c, x = lax.axis_index("sp_0"), lax.axis_index("sp_1"), lax.axis_index("tp")
    place, quad = lax.rem(z, QUAD), z // QUAD
    barrier = pltpu.get_barrier_semaphore()
    beyond = z + 2 * c - 1
    has_beyond = (beyond >= 0) & (beyond < nz)
    before = (place == 0) & (quad > 0)
    behind = (place == QUAD - 1) & (quad < nz // QUAD - 1)

    def in_quad(k, carry):
        to = quad * QUAD + lax.rem(place + k, QUAD)
        pl.semaphore_signal(barrier, inc=1, device_id={"sp_0": to})
        return carry

    def along_x(k, carry):
        pl.semaphore_signal(barrier, inc=1, device_id={"tp": lax.rem(x + k, nx)})
        return carry

    pl.semaphore_signal(barrier, inc=1, device_id={"sp_1": 1 - c})
    lax.fori_loop(1, QUAD, in_quad, 0)
    lax.fori_loop(1, nx, along_x, 0)

    @pl.when(has_beyond)
    def _():
        pl.semaphore_signal(barrier, inc=1, device_id={"sp_0": beyond, "sp_1": 1 - c})

    @pl.when(before)
    def _():
        pl.semaphore_signal(barrier, inc=1, device_id={"sp_0": z - 1})

    @pl.when(behind)
    def _():
        pl.semaphore_signal(barrier, inc=1, device_id={"sp_0": z + 1})

    return QUAD + nx - 1 + sum(flag.astype(jnp.int32) for flag in (has_beyond, before, behind))


def pass_word(nz, token, ready):
    z = lax.axis_index("sp_0")
    place, quad = lax.rem(z, QUAD), z // QUAD
    last = nz // QUAD - 1

    @pl.when((place == 0) & (quad > 0))
    def _():
        pl.semaphore_wait(token, 1)

    @pl.when((place == 0) & (quad < last))
    def _():
        pl.semaphore_signal(token, inc=1, device_id={"sp_0": z + QUAD - 1})

    @pl.when((place == QUAD - 1) & (quad < last))
    def _():
        pl.semaphore_wait(token, 1)
        pl.semaphore_signal(token, inc=1, device_id={"sp_0": z + 1})

    @pl.when((place == 0) & (quad == last))
    def _():
        def tell(k, carry):
            pl.semaphore_signal(ready, inc=1, device_id={"sp_0": lax.rem(z + k, nz)})
            return carry

        lax.fori_loop(1, nz, tell, 0)


def silu(v):
    return v * jax.nn.sigmoid(v)


def exact_dot(a, b):
    return jnp.dot(a, b, preferred_element_type=jnp.float32, precision=lax.Precision.HIGHEST)


def packed(state, decays):
    lanes = state.shape[1]
    row = lax.broadcasted_iota(jnp.int32, (TAIL, lanes), 0)
    tail = jnp.zeros((TAIL, lanes), jnp.float32)
    for h, decay in enumerate(decays):
        wide = jnp.broadcast_to(decay, (TAIL, lanes))
        high = wide.astype(jnp.bfloat16).astype(jnp.float32)
        tail = jnp.where(row == h, high, tail)
        tail = jnp.where(row == TAIL // 2 + h, wide - high, tail)
    return jnp.concatenate([state.astype(jnp.bfloat16), tail.astype(jnp.bfloat16)], axis=0)


def unpacked(message, heads):
    rows = message.shape[0] - TAIL
    state = message[:rows].astype(jnp.float32)
    tail = message[rows:].astype(jnp.float32)
    half = TAIL // 2
    return state, [tail[h : h + 1, 0:1] + tail[half + h : half + h + 1, 0:1] for h in range(heads)]


def per_row(decays, rows, lanes):
    each = rows // len(decays)
    return jnp.concatenate([jnp.broadcast_to(d, (each, lanes)) for d in decays], axis=0)


def followed(earlier, later):
    (state_a, decay_a), (state_b, decay_b) = earlier, later
    state = state_a * per_row(decay_b, *state_a.shape) + state_b
    return state, [a * b for a, b in zip(decay_a, decay_b)]


def chosen(flag, one, other):
    return jnp.where(flag, one[0], other[0]), [
        jnp.where(flag, a, b) for a, b in zip(one[1], other[1])
    ]


def front_kernel(
    nz,
    nx,
    capacity,
    xs_ref,
    gate_ref,
    keys_ref,
    queries_ref,
    raw_ref,
    extra_ref,
    rate_ref,
    taps_x_ref,
    taps_k_ref,
    taps_q_ref,
    gain_ref,
    blend_hbm,
    carry_ref,
    gain2_ref,
    ids_ref,
    affinity_ref,
    chance_ref,
    outgoing_ref,
    middle_ref,
    weight_ref,
    halo,
    joined,
    pair_out,
    pair_in,
    quad_out,
    quad_in,
    far_out,
    far_in,
    half_out,
    half_in,
    gated_out,
    gated_in,
    facts,
    rows,
    blend,
    turned,
    smooth,
    fading,
    blend_sem,
    halo_s,
    halo_r,
    pair_s,
    pair_r,
    quad_s,
    quad_r,
    far_s,
    far_r,
    gated_s,
    gated_r,
    token,
    following,
    ready,
):
    z, c, x = lax.axis_index("sp_0"), lax.axis_index("sp_1"), lax.axis_index("tp")
    length, width_x = xs_ref.shape
    state_width = keys_ref.shape[1]
    heads = raw_ref.shape[0]
    head_dim = width_x // heads
    half_heads = heads // 2
    half_rows = width_x // 2
    place, quad = lax.rem(z, QUAD), z // QUAD
    quads = nz // QUAD
    f32, bf16 = jnp.float32, jnp.bfloat16
    partner = {"sp_1": 1 - c}
    greeted = announce(nz, nx)
    load = pltpu.make_async_copy(blend_hbm, blend, blend_sem)
    load.start()

    stride_row = jnp.maximum(raw_ref[...], 0.0) + jnp.log1p(jnp.exp(-jnp.abs(raw_ref[...])))
    diagonal = lax.broadcasted_iota(jnp.int32, (heads, heads), 0) == lax.broadcasted_iota(
        jnp.int32, (heads, heads), 1
    )
    rate = jnp.sum(
        jnp.where(diagonal, jnp.broadcast_to(rate_ref[...], (heads, heads)), 0.0),
        axis=1,
        keepdims=True,
    )
    log_row = extra_ref[...] - rate * stride_row
    t_axis = lax.broadcasted_iota(jnp.int32, (length, length), 0)
    s_axis = lax.broadcasted_iota(jnp.int32, (length, length), 1)
    causal = t_axis >= s_axis
    running_row = exact_dot(
        jnp.concatenate([log_row, jnp.zeros_like(log_row)], axis=0), (t_axis <= s_axis).astype(f32)
    )
    picks = ids_ref.shape[0]
    count = ids_ref.shape[1] // nx
    lanes = 128
    stacked = jnp.concatenate(
        [
            running_row[:heads],
            stride_row,
            ids_ref[...].astype(f32),
            jnp.zeros((lanes - 2 * heads - picks, length), f32),
        ],
        axis=0,
    )
    turned[...] = stacked.T
    running = turned[:, :heads]
    stride = turned[:, heads : 2 * heads]
    final = running[length - 1 : length, :]
    lifted = jnp.exp(affinity_ref[...])
    share_row = chance_ref[...] * lifted / jnp.sum(lifted, axis=0, keepdims=True)
    share_row = jnp.concatenate([share_row, jnp.zeros((lanes - picks, count), f32)], axis=0)
    share_row = jnp.concatenate([share_row, jnp.zeros((lanes, lanes - count), f32)], axis=1)
    shares = share_row.T[:count]
    local_experts = outgoing_ref.shape[0]
    experts = nz * 2 * local_experts
    ids = turned[pl.ds(pl.multiple_of(x * count, count), count), :]
    ids = ids[:, 2 * heads : 2 * heads + picks].astype(jnp.int32)
    expert_axis = lax.broadcasted_iota(jnp.int32, (count, experts), 1)
    member = [(ids[:, k : k + 1] == expert_axis).astype(f32) for k in range(picks)]
    row_axis = lax.broadcasted_iota(jnp.int32, (count, count), 0)
    column_axis = lax.broadcasted_iota(jnp.int32, (count, count), 1)
    earlier = (row_axis > column_axis).astype(bf16)
    before = jnp.dot(earlier, sum(member).astype(bf16), preferred_element_type=f32)
    lane = lax.broadcasted_iota(jnp.int32, (count, facts.shape[2]), 1)
    noted = jnp.zeros((count, facts.shape[2]), f32)
    for k in range(picks):
        position = jnp.sum(before * member[k], axis=1, keepdims=True)
        expert = ids[:, k : k + 1]
        holder = lax.div(expert, local_experts)
        slot = (
            (lax.rem(expert, local_experts) * nz + lax.div(holder, 2)) * 2 + c
        ) * capacity + position.astype(jnp.int32)
        for core in range(2):
            there = jnp.where(lax.rem(holder, 2) == core, slot, -1).astype(f32)
            noted = jnp.where(lane == core * picks + k, there, noted)
        noted = jnp.where(lane == 2 * picks + k, shares[:, k : k + 1], noted)
    facts[c] = noted

    rim = halo.shape[0]
    start = 0
    for ref in (xs_ref, keys_ref, queries_ref):
        joined[rim:, start : start + ref.shape[1]] = ref[...].astype(f32)
        start += ref.shape[1]
    taps = jnp.concatenate([taps_x_ref[...], taps_k_ref[...], taps_q_ref[...]], axis=1)
    kernel_len = taps.shape[0]

    def convolve(begin, end):
        start = rim - kernel_len + 1
        total = taps[0:1, :] * joined[start + begin : start + end, :]
        for tap in range(1, kernel_len):
            total = total + taps[tap : tap + 1, :] * joined[start + tap + begin : start + tap + end, :]
        return silu(total)

    smooth[rim:, :] = convolve(rim, length)
    modulation = silu(gate_ref[...].astype(f32))
    for h in range(heads):
        between = running[:, h : h + 1] - running_row[h : h + 1, :]
        fading[h] = jnp.exp(jnp.where(causal, between, -1e30))

    pl.semaphore_wait(pltpu.get_barrier_semaphore(), greeted)

    @pl.when((place == 0) & (quad > 0))
    def _():
        pl.semaphore_signal(following, inc=1, device_id={"sp_0": z - 1})

    after = {"sp_0": lax.rem(z + c, nz), "sp_1": 1 - c}
    edges = []
    start = 0
    for n, ref in enumerate((xs_ref, keys_ref, queries_ref)):
        columns = pl.ds(start, ref.shape[1])
        edges.append(
            pltpu.make_async_remote_copy(
                ref.at[pl.ds(length - rim, rim)],
                halo.at[:, columns],
                halo_s.at[n],
                halo_r.at[n],
                device_id=after,
            )
        )
        start += ref.shape[1]

    @pl.when(z + c < nz)
    def _():
        for edge in edges:
            edge.start()

    facts_copy = pltpu.make_async_remote_copy(
        facts.at[c], facts.at[c], pair_s.at[0], pair_r.at[0], device_id=partner
    )
    facts_copy.start()

    @pl.when(z + c > 0)
    def _():
        for edge in edges:
            edge.wait_recv()
        joined[:rim, :] = halo[...].astype(f32)

    @pl.when(z + c == 0)
    def _():
        joined[:rim, :] = jnp.zeros_like(joined[:rim, :])

    smooth[:rim, :] = convolve(0, rim)
    inputs_x = smooth[:, :width_x]
    keys_b = smooth[:, width_x : width_x + state_width].astype(bf16)
    queries_c = smooth[:, width_x + state_width :].astype(bf16)

    scaled = [
        inputs_x[:, h * head_dim : (h + 1) * head_dim] * stride[:, h : h + 1] for h in range(heads)
    ]
    remaining = jnp.concatenate(
        [scaled[h] * jnp.exp(final[:, h : h + 1] - running[:, h : h + 1]) for h in range(heads)],
        axis=1,
    ).astype(bf16)
    own_state = lax.dot_general(
        remaining, keys_b, (((0,), (0,)), ((), ())), preferred_element_type=f32
    )
    pair_out[...] = packed(own_state, [jnp.exp(final[:, h : h + 1]) for h in range(heads)])
    pair_copy = pltpu.make_async_remote_copy(
        pair_out, pair_in, pair_s.at[1], pair_r.at[1], device_id=partner
    )
    pair_copy.start()

    scores = lax.dot_general(
        queries_c, keys_b, (((1,), (1,)), ((), ())), preferred_element_type=f32
    )
    inside = []
    for h in range(heads):
        inside.append(
            jnp.dot(
                (scores * fading[h]).astype(bf16), scaled[h].astype(bf16), preferred_element_type=f32
            )
        )

    pair_copy.wait_recv()

    def half_of(ref):
        state, decays = unpacked(ref[...], heads)
        return (
            jnp.where(c == 0, state[:half_rows], state[half_rows:]),
            [jnp.where(c == 0, decays[j], decays[half_heads + j]) for j in range(half_heads)],
        )

    ours, theirs = half_of(pair_out), half_of(pair_in)
    lower, upper = chosen(c == 0, ours, theirs), chosen(c == 0, theirs, ours)
    chip = followed(lower, upper)
    quad_out[...] = packed(*chip)

    def quad_send(k):
        to = quad * QUAD + lax.rem(place + k, QUAD)
        return pltpu.make_async_remote_copy(
            quad_out, quad_in.at[place], quad_s.at[k], quad_r.at[k], device_id={"sp_0": to}
        )

    def quad_arrival(k):
        return pltpu.make_async_remote_copy(
            quad_out,
            quad_in.at[lax.rem(place + QUAD - k, QUAD)],
            quad_s.at[k],
            quad_r.at[k],
            device_id={"sp_0": lax.rem(z + 1, nz)},
        )

    for k in range(1, QUAD):

        @pl.when(place + k < QUAD)
        def _(k=k):
            quad_send(k).start()

    pass_word(nz, token, ready)
    for k in range(1, QUAD):

        @pl.when(place >= k)
        def _(k=k):
            quad_arrival(k).wait_recv()

        @pl.when(place < k)
        def _(k=k):
            quad_in[k - 1] = jnp.zeros_like(quad_out)

    nothing = (jnp.zeros_like(chip[0]), [jnp.ones_like(d) for d in chip[1]])
    inner = nothing
    for k in range(QUAD - 1):
        inner = chosen(k < place, followed(inner, unpacked(quad_in[k], half_heads)), inner)

    def far_send(k):
        return pltpu.make_async_remote_copy(
            far_out,
            far_in,
            far_s.at[k],
            far_r,
            device_id={"sp_0": lax.rem(z + 1 + k, nz)},
        )

    @pl.when(quad > 0)
    def _():
        far_send(0).wait_recv()

    @pl.when(quad == 0)
    def _():
        far_in[...] = jnp.zeros_like(far_in)

    incoming = followed((far_in[...].astype(f32), nothing[1]), inner)
    incoming_low = incoming[0]
    leads_on = (place == QUAD - 1) & (quad < quads - 1)

    @pl.when(leads_on)
    def _():
        far_out[...] = followed(incoming, chip)[0].astype(bf16)
        pl.semaphore_wait(following, 1)
        for k in range(QUAD):
            far_send(k).start()

    incoming_high = followed(incoming, lower)[0]
    half_out[...] = jnp.where(c == 0, incoming_high, incoming_low).astype(bf16)
    half_copy = pltpu.make_async_remote_copy(
        half_out, half_in, pair_s.at[2], pair_r.at[2], device_id=partner
    )
    half_copy.start()
    kept = jnp.where(c == 0, incoming_low, incoming_high).astype(bf16)
    half_copy.wait_recv()
    sent_in = half_in[...]
    entering = jnp.concatenate(
        [jnp.where(c == 0, kept, sent_in), jnp.where(c == 0, sent_in, kept)], axis=0
    )
    outside = lax.dot_general(
        queries_c, entering, (((1,), (1,)), ((), ())), preferred_element_type=f32
    )
    mixed = jnp.concatenate(
        [
            inside[h]
            + outside[:, h * head_dim : (h + 1) * head_dim] * jnp.exp(running[:, h : h + 1])
            for h in range(heads)
        ],
        axis=1,
    )
    gated_out[...] = (mixed * modulation).astype(bf16).reshape(gated_out.shape)

    def gated_send(k):
        to = lax.rem(x + k, nx)
        return pltpu.make_async_remote_copy(
            gated_out.at[to], gated_in.at[x], gated_s.at[k], gated_r.at[k], device_id={"tp": to}
        )

    for k in range(1, nx):
        gated_send(k).start()
    gated_in[x] = gated_out[x]
    facts_arrival = pltpu.make_async_remote_copy(
        facts.at[1 - c], facts.at[1 - c], pair_s.at[0], pair_r.at[0], device_id=partner
    )
    facts_arrival.wait_recv()
    slot_count = weight_ref.shape[1]
    slot_axis = lax.broadcasted_iota(jnp.int32, (2 * count, slot_count), 1).astype(f32)
    known = jnp.concatenate([facts[0], facts[1]], axis=0)
    picked = jnp.zeros((2 * count, slot_count), f32)
    weight = jnp.zeros((2 * count, slot_count), f32)
    for k in range(picks):
        slot = jnp.where(c == 0, known[:, k : k + 1], known[:, picks + k : picks + k + 1])
        hit = slot == slot_axis
        picked = jnp.where(hit, 1.0, picked)
        weight = jnp.where(hit, known[:, 2 * picks + k : 2 * picks + k + 1], weight)
    weight_ref[...] = weight
    for k in range(1, nx):
        pltpu.make_async_remote_copy(
            gated_out.at[x],
            gated_in.at[lax.rem(x + nx - k, nx)],
            gated_s.at[k],
            gated_r.at[k],
            device_id={"tp": lax.rem(x + k, nx)},
        ).wait_recv()
    own_rows = jnp.concatenate([gated_in[k] for k in range(nx)], axis=1).astype(f32)
    normed = (
        own_rows
        * lax.rsqrt(jnp.mean(own_rows * own_rows, axis=1, keepdims=True) + EPS)
        * gain_ref[...]
    ).astype(bf16)
    load.wait()
    middle = (
        carry_ref[...].astype(f32) + jnp.dot(normed, blend[...], preferred_element_type=f32)
    ).astype(bf16)
    middle_ref[...] = middle
    wide = middle.astype(f32)
    rows[c] = (
        wide
        * lax.rsqrt(jnp.mean(wide * wide, axis=1, keepdims=True) + EPS)
        * gain2_ref[...]
    ).astype(bf16)
    rows_copy = pltpu.make_async_remote_copy(
        rows.at[c], rows.at[c], pair_s.at[3], pair_r.at[3], device_id=partner
    )
    rows_copy.start()
    pltpu.make_async_remote_copy(
        rows.at[1 - c], rows.at[1 - c], pair_s.at[3], pair_r.at[3], device_id=partner
    ).wait_recv()
    outgoing_ref[...] = (
        lax.dot_general(
            picked.astype(bf16),
            jnp.concatenate([rows[0], rows[1]], axis=0),
            (((0,), (0,)), ((), ())),
            preferred_element_type=f32,
        )
        .astype(bf16)
        .reshape(outgoing_ref.shape)
    )


    @pl.when(z + c < nz)
    def _():
        for edge in edges:
            edge.wait_send()

    facts_copy.wait_send()
    pair_copy.wait_send()
    half_copy.wait_send()
    rows_copy.wait_send()
    for k in range(1, QUAD):

        @pl.when(place + k < QUAD)
        def _(k=k):
            quad_send(k).wait_send()

    @pl.when(leads_on)
    def _():
        for k in range(QUAD):
            far_send(k).wait_send()

    for k in range(1, nx):
        gated_send(k).wait_send()

    @pl.when((place > 0) | (quad < quads - 1))
    def _():
        pl.semaphore_wait(ready, 1)


FRONT_INPUTS = 17
FRONT_SCRATCH = 32


def layer_kernel(nz, nx, capacity, *refs):
    inputs, refs = refs[:FRONT_INPUTS], refs[FRONT_INPUTS:]
    weights, out_ref, refs = refs[:3], refs[3], refs[4:]
    outgoing, middle, weight, refs = *refs[:3], refs[3:]
    front_kernel(nz, nx, capacity, *inputs, outgoing, middle, weight, *refs[:FRONT_SCRATCH])
    experts_kernel(nz, nx, outgoing, *weights, middle, weight, out_ref, *refs[FRONT_SCRATCH:])


def layer(nz, nx, capacity, *arrays):
    xs, _, keys, queries, raw = arrays[:5]
    blend, carry = arrays[11:13]
    weights = arrays[FRONT_INPUTS:]
    experts = weights[0].shape[0]
    count, width = carry.shape
    rows = 2 * capacity
    channels, states = xs.shape[1], keys.shape[1]
    total = channels + states + queries.shape[1]
    rim = 8
    half = channels // 2
    bf16, f32 = jnp.bfloat16, jnp.float32
    vmem = pl.BlockSpec(memory_space=pltpu.VMEM)
    anywhere = pl.BlockSpec(memory_space=pl.ANY)
    slots = pltpu.VMEM((nz, experts, rows, width), bf16)
    wide = pltpu.VMEM((nz, experts, nx, rows, width), bf16)

    def sems(*shape):
        return pltpu.SemaphoreType.DMA(shape)

    front_scratch = [
        pltpu.VMEM((rim, total), bf16),
        pltpu.VMEM((rim + xs.shape[0], total), f32),
        pltpu.VMEM((channels + TAIL, states), bf16),
        pltpu.VMEM((channels + TAIL, states), bf16),
        pltpu.VMEM((half + TAIL, states), bf16),
        pltpu.VMEM((QUAD, half + TAIL, states), bf16),
        pltpu.VMEM((half, states), bf16),
        pltpu.VMEM((half, states), bf16),
        pltpu.VMEM((half, states), bf16),
        pltpu.VMEM((half, states), bf16),
        pltpu.VMEM((nx, count, channels), bf16),
        pltpu.VMEM((nx, count, channels), bf16),
        pltpu.VMEM((2, count, 128), f32),
        pltpu.VMEM((2, count, width), bf16),
        pltpu.VMEM(blend.shape, bf16),
        pltpu.VMEM((xs.shape[0], 128), f32),
        pltpu.VMEM((xs.shape[0], total), f32),
        pltpu.VMEM((raw.shape[0], xs.shape[0], xs.shape[0]), f32),
        pltpu.SemaphoreType.DMA,
        sems(3),
        sems(3),
        sems(4),
        sems(4),
        sems(QUAD),
        sems(QUAD),
        sems(QUAD),
        pltpu.SemaphoreType.DMA,
        sems(nx),
        sems(nx),
        pltpu.SemaphoreType.REGULAR,
        pltpu.SemaphoreType.REGULAR,
        pltpu.SemaphoreType.REGULAR,
    ]
    experts_scratch = (
        [wide, wide, slots, slots, slots, slots, slots]
        + [pltpu.VMEM((experts, nz, rows, width), bf16)]
        + [pltpu.VMEM(w.shape, bf16) for w in weights]
        + [pltpu.VMEM((count, width), f32)] * 2
        + [sems(3), sems(2), sems(nz), sems(nz), sems(2, nz), sems(2, nz)]
        + [sems(nz)] * 10
        + [pltpu.SemaphoreType.DMA] * 2
    )
    assert len(front_scratch) == FRONT_SCRATCH
    return pl.pallas_call(
        functools.partial(layer_kernel, nz, nx, capacity),
        out_shape=jax.ShapeDtypeStruct((count, width), bf16),
        in_specs=[vmem] * 11 + [anywhere] + [vmem] * 5 + [anywhere] * 3,
        out_specs=vmem,
        scratch_shapes=[
            pltpu.VMEM((experts, nz, rows, width), bf16),
            pltpu.VMEM((count, width), bf16),
            pltpu.VMEM((2 * count, experts * nz * rows), f32),
        ]
        + front_scratch
        + experts_scratch,
        compiler_params=pltpu.CompilerParams(
            collective_id=1, has_side_effects=True, vmem_limit_bytes=60 << 20
        ),
        name="layer",
    )(*arrays)


def per_device(
    carryover_vector,
    channel_source_entries,
    final_modulation_vector,
    entering_basis_matrix,
    readout_basis_matrix,
    raw_stride_amount,
    extra_log_attenuation,
    channel_fading_rate,
    channel_source_kernel,
    entering_basis_kernel,
    readout_basis_kernel,
    modulated_rescaling_vector,
    blender_final_matrix,
    specialist_rescaling_vector,
    specialist_gating_matrices,
    widening_matrices,
    contracting_matrices,
    assigned_specialist_ids,
    specialist_choice_affinity,
    cluster_chance,
):
    nz, cores, nx = lax.axis_size("sp_0"), lax.axis_size("sp_1"), lax.axis_size("tp")
    row_count = carryover_vector.shape[0]
    local_experts = specialist_gating_matrices.shape[0]
    experts = nz * cores * local_experts
    picks = assigned_specialist_ids.shape[1]
    capacity = 2 * row_count * picks // experts
    return layer(
        nz,
        nx,
        capacity,
        channel_source_entries,
        final_modulation_vector,
        entering_basis_matrix,
        readout_basis_matrix,
        raw_stride_amount.T,
        extra_log_attenuation.T,
        channel_fading_rate[None, :],
        channel_source_kernel,
        entering_basis_kernel,
        readout_basis_kernel,
        modulated_rescaling_vector[None, :],
        blender_final_matrix,
        carryover_vector,
        specialist_rescaling_vector[None, :],
        assigned_specialist_ids.T,
        specialist_choice_affinity.T,
        cluster_chance[None, :],
        specialist_gating_matrices,
        widening_matrices,
        contracting_matrices,
    )


def solution(mesh):
    finer = Mesh(
        mesh.devices.reshape(mesh.shape["grp"], mesh.shape["sp"] // 2, 2, mesh.shape["tp"]),
        ("grp", "sp_0", "sp_1", "tp"),
    )
    return jax.shard_map(
        per_device,
        mesh=finer,
        in_specs=(
            P(GRP_SP_TP, None),
            P(GRP_SP, "tp"),
            P(GRP_SP, "tp"),
            P(GRP_SP, "tp"),
            P(GRP_SP, "tp"),
            P(GRP_SP, "tp"),
            P(GRP_SP, "tp"),
            P("tp"),
            P(None, "tp"),
            P(None, "tp"),
            P(None, "tp"),
            P(),
            P(),
            P(),
            P(SP, None, "tp"),
            P(SP, None, "tp"),
            P(SP, "tp", None),
            P(GRP_SP, None),
            P(GRP_SP_TP, None),
            P(GRP_SP_TP),
        ),
        out_specs=P(GRP_SP_TP, None),
        check_vma=False,
    )
```
